128 devices in a mesh: sp: 16 (over z, y), tp: 8 (over x, core).
Axes of the slice: x: 4, y: 4, z: 4, core: 2. Of those that a mesh axis runs over, the one named last changes fastest.
Arguments:
- latents: bfloat16 [4096, 4096], P('sp'), may hold values from -0.4375 to 0.4375
- query_heads: bfloat16 [4096, 16, 128], P('sp', 'tp'), may hold values from -8 to 8
- key_heads: bfloat16 [4096, 16, 128], P('sp', 'tp'), may hold values from -8 to 8
- value_heads: bfloat16 [4096, 16, 128], P('sp', 'tp'), may hold values from -6 to 6
- map_outputs: bfloat16 [4096, 2, 16, 128], P('sp', None, 'tp'), may hold values from -6 to 6
- log_sums: float32 [4096, 16, 2], P('sp', 'tp'), may hold values from -600 to 600, as said below
- out_grad: bfloat16 [4096, 16, 128], P('sp', 'tp'), may hold values from -6 to 6
- mix_lambda: float32 [16], P('tp'), may hold values from 0.3 to 0.8
- norm_gain: float32 [128], replicated, may hold values from 0.1 to 1.9
Outputs:
- query_grad: bfloat16 [4096, 16, 128], P('sp', 'tp')
- key_grad: bfloat16 [4096, 16, 128], P('sp', 'tp')
- value_grad: bfloat16 [4096, 16, 128], P('sp', 'tp')
- weight_grad: float32 [4096, 2048], P('sp', 'tp')
The draws below stay inside these ranges and needn't reach their ends.
Inputs may be any that keep to these rules, and one draw needn't show every extreme that they name: query_heads, key_heads and value_heads together with map_outputs and log_sums are one consistent causal forward pass: log_sums is the row's log-sum of exp(score_m) over keys at or before the row, and map_outputs[:, m] is prob_m times value_heads rounded to bfloat16.
All inputs are finite; a program needn't handle non-finite values.
Results may differ from the reference program's by a relative error of at most 0.019.
Values may be sent and summed in bfloat16 or wider, within the bound.
No kernel may reach another device: no remote copies, remote signals or barrier semaphores. Data moves between devices by JAX's collectives and lax.ppermute only.
A program may use at most 64 MiB of HBM per device.

```python
import math
import jax
import jax.numpy as jnp
from jax import lax

D = 4096
HEADS = 16
DH = 64
TOKENS = 4096


def attention_forward(key):
    shape = (TOKENS, HEADS, 2 * DH)
    query_f = jnp.clip(1.3 * jax.random.normal(jax.random.fold_in(key, 101), shape, jnp.float32), -8.0, 8.0)
    key_f = jnp.clip(1.3 * jax.random.normal(jax.random.fold_in(key, 102), shape, jnp.float32), -8.0, 8.0)
    value_f = jnp.clip(jax.random.normal(jax.random.fold_in(key, 103), shape, jnp.float32), -6.0, 6.0)
    query_low = query_f.astype(jnp.bfloat16)
    key_low = key_f.astype(jnp.bfloat16)
    value_low = value_f.astype(jnp.bfloat16)
    length = TOKENS
    span = math.gcd(length, 512)
    score_scale = DH ** (-0.5)

    def per_head(inputs):
        query_one, key_one, value_one = inputs
        query_split = query_one.astype(jnp.float32).reshape(length, 2, DH)
        key_split = key_one.astype(jnp.float32).reshape(length, 2, DH)
        value_wide = value_one.astype(jnp.float32)
        key_pos = jnp.arange(length, dtype=jnp.int32)

        def visit(block_index):
            anchor = (block_index * span).astype(jnp.int32)
            query_blk = lax.dynamic_slice_in_dim(query_split, anchor, span, 0)
            scores = jnp.einsum('qmd,kmd->mqk', query_blk, key_split) * score_scale
            query_pos = anchor + jnp.arange(span, dtype=jnp.int32)
            causal = key_pos[None, :] <= query_pos[:, None]
            masked = jnp.where(causal[None], scores, -jnp.inf)
            highest = jnp.max(masked, axis=-1, keepdims=True)
            log_total = highest + jnp.log(jnp.sum(jnp.exp(masked - highest), axis=-1, keepdims=True))
            probs = jnp.exp(masked - log_total)
            outputs = jnp.einsum('mqk,ke->mqe', probs, value_wide)
            return (log_total[..., 0].T, outputs)
        lse_blocks, out_blocks = lax.map(visit, jnp.arange(length // span, dtype=jnp.int32))
        lse_head = lse_blocks.reshape(length, 2)
        out_head = jnp.transpose(out_blocks, (1, 0, 2, 3)).reshape(2, length, 2 * DH)
        return (lse_head, out_head)
    lse_all, out_all = lax.map(per_head, (jnp.transpose(query_low, (1, 0, 2)), jnp.transpose(key_low, (1, 0, 2)), jnp.transpose(value_low, (1, 0, 2))))
    log_table = jnp.transpose(lse_all, (1, 0, 2))
    out_table = jnp.transpose(out_all, (2, 1, 0, 3)).astype(jnp.bfloat16)
    return (query_low, key_low, value_low, out_table, log_table)


def draw_query_heads(key, part):
    return attention_forward(key)[0]


def draw_key_heads(key, part):
    return attention_forward(key)[1]


def draw_value_heads(key, part):
    return attention_forward(key)[2]


def draw_map_outputs(key, part):
    return attention_forward(key)[3]


def draw_log_sums(key, part):
    return attention_forward(key)[4]


def raised(values, stream_key, source, target, parts, factor):
    def block_of(position):
        return (jnp.arange(values.shape[position]) // (values.shape[position] // parts)).reshape((-1,) + (1,) * (values.ndim - 1 - position))

    near = jax.random.permutation(stream_key, parts)[block_of(target)]
    far = (block_of(target) + parts // 2) % parts
    return jnp.where((block_of(source) == near) | (block_of(source) == far), factor * values, values)


def level_of(key, extent, split, least, top_value):
    factor_of, own = 1.0, jax.random.fold_in(key, 6)
    for position, shards_of in split:
        steps = jnp.exp(jax.random.uniform(jax.random.fold_in(own, position), (shards_of,), jnp.float32, least / len(split), top_value / len(split)))
        factor_of = factor_of * jnp.repeat(steps, extent[position] // shards_of).reshape([-1 if axis == position else 1 for axis in range(len(extent))])
    return factor_of


def noise(key, dims, scale, most, pieces=(), kind=jnp.bfloat16):
    level = level_of(key, dims, pieces, -0.22, 0.18) if pieces else 1.0
    values = jax.random.normal(key, dims, jnp.float32) * scale * level
    return jnp.minimum(jnp.maximum(values, -most), most).astype(kind)


def gaussian_with(stream_key, shape, deviation, reach, shards, heavy, kind=jnp.bfloat16):
    entries = deviation * jax.random.normal(stream_key, shape, jnp.float32)
    if shards:
        entries = entries * level_of(stream_key, shape, shards, -0.22, 0.18)
    return jnp.clip(raised(entries, jax.random.fold_in(stream_key, 3), *heavy), -reach, reach).astype(kind)


def setup_inputs(seed: int = 0) -> dict:
    seeds = jax.random.split(jax.random.key(seed), 10)
    return {
        "latents": gaussian_with(seeds[0], (TOKENS, D), 0.02, 0.4375, ((0, 16),), (0, 1, 16, 2.0)),
        "query_heads": draw_query_heads(jax.random.fold_in(seeds[9], 71), 0),
        "key_heads": draw_key_heads(jax.random.fold_in(seeds[9], 71), 0),
        "value_heads": draw_value_heads(jax.random.fold_in(seeds[9], 71), 0),
        "map_outputs": draw_map_outputs(jax.random.fold_in(seeds[9], 71), 0),
        "log_sums": draw_log_sums(jax.random.fold_in(seeds[9], 71), 0),
        "out_grad": noise(seeds[6], (TOKENS, HEADS, 2 * DH), 1.0, 6.0, ((0, 16), (1, 8))),
        "mix_lambda": jnp.clip(0.3 + 0.5 * jax.random.uniform(seeds[7], (HEADS,), jnp.float32) ** level_of(seeds[7], (HEADS,), ((0, 8),), -0.2, 0.2), 0.3, 0.8),
        "norm_gain": jnp.clip(1.0 + 0.18 * jax.random.normal(seeds[8], (2 * DH,), jnp.float32), 0.1, 1.9),
    }


EPSILON = 1e-05

def reference(latents, query_heads, key_heads, value_heads, map_outputs, log_sums, out_grad, mix_lambda, norm_gain):
    highest = lax.Precision.HIGHEST
    score_scale = DH ** (-0.5)
    first_map = map_outputs[:, 0].astype(jnp.float32)
    second_map = map_outputs[:, 1].astype(jnp.float32)
    lambda_col = mix_lambda[None, :, None]
    combined = first_map - lambda_col * second_map
    inverse = lax.rsqrt(lax.optimization_barrier(jnp.mean(combined * combined, axis=-1, keepdims=True)) + EPSILON)
    weighted = norm_gain[None, None, :] * out_grad.astype(jnp.float32)
    grad_out = (inverse * weighted - inverse ** 3 * combined * lax.optimization_barrier(jnp.mean(combined * weighted, axis=-1, keepdims=True))).astype(jnp.bfloat16)
    grad_wide = lax.optimization_barrier(grad_out).astype(jnp.float32)
    row_terms = jnp.stack([lax.optimization_barrier(jnp.sum(grad_wide * first_map, axis=-1)), lax.optimization_barrier(jnp.sum(grad_wide * second_map, axis=-1))], axis=-1)
    length = query_heads.shape[0]
    span = math.gcd(length, 512)

    def per_head(inputs):
        query_one, key_one, value_one, grad_one, lse_one, term_one, lam = inputs
        query_split = query_one.astype(jnp.float32).reshape(length, 2, DH)
        key_split = key_one.astype(jnp.float32).reshape(length, 2, DH)
        value_wide = value_one.astype(jnp.float32)
        grad_full = grad_one.astype(jnp.float32)
        key_pos = jnp.arange(length, dtype=jnp.int32)
        map_signs = jnp.stack([jnp.ones((), jnp.float32), -lam])

        def visit(running, block_index):
            key_acc, value_acc = running
            anchor = (block_index * span).astype(jnp.int32)
            query_blk = lax.dynamic_slice_in_dim(query_split, anchor, span, 0)
            grad_blk = lax.dynamic_slice_in_dim(grad_full, anchor, span, 0)
            lse_blk = lax.dynamic_slice_in_dim(lse_one, anchor, span, 0)
            term_blk = lax.dynamic_slice_in_dim(term_one, anchor, span, 0)
            scores = jnp.einsum('qmd,kmd->mqk', query_blk, key_split, precision=highest) * score_scale
            query_pos = anchor + jnp.arange(span, dtype=jnp.int32)
            causal = key_pos[None, :] <= query_pos[:, None]
            softmax_maps = jnp.exp(jnp.where(causal[None], scores - lse_blk.T[:, :, None], -jnp.inf))
            mixed_grad = jnp.dot(grad_blk, value_wide.T, precision=highest)
            score_grad = map_signs[:, None, None] * softmax_maps * (mixed_grad[None] - term_blk.T[:, :, None])
            score_low = lax.optimization_barrier(score_grad.astype(jnp.bfloat16)).astype(jnp.float32)
            diff_weights = lax.optimization_barrier((softmax_maps[0] - lam * softmax_maps[1]).astype(jnp.bfloat16)).astype(jnp.float32)
            value_acc = value_acc + jnp.dot(diff_weights.T, grad_blk, precision=highest)
            query_part = score_scale * jnp.einsum('mqk,kmd->qmd', score_low, key_split, precision=highest)
            key_acc = key_acc + score_scale * jnp.einsum('mqk,qmd->kmd', score_low, query_blk, precision=highest)
            return ((key_acc, value_acc), query_part)
        start_state = (jnp.zeros((length, 2, DH), jnp.float32), jnp.zeros((length, 2 * DH), jnp.float32))
        (key_acc, value_acc), query_parts = lax.scan(visit, start_state, jnp.arange(length // span, dtype=jnp.int32))
        return (query_parts.reshape(length, 2 * DH), key_acc.reshape(length, 2 * DH), value_acc)

    def head_major(array):
        return jnp.transpose(array, (1, 0, 2))
    query_all, key_all, value_all = lax.map(per_head, (head_major(query_heads), head_major(key_heads), head_major(value_heads), head_major(grad_out), head_major(log_sums), head_major(row_terms), mix_lambda))
    query_grad = head_major(query_all).astype(jnp.bfloat16)
    key_grad = head_major(key_all).astype(jnp.bfloat16)
    value_grad = head_major(value_all).astype(jnp.bfloat16)
    weight_grad = jnp.dot(latents.T, query_grad.reshape(length, -1), preferred_element_type=jnp.float32)
    return (query_grad, key_grad, value_grad, weight_grad)
```

```python
import functools

import jax
import jax.numpy as jnp
from jax import lax
from jax.experimental import pallas as pl
from jax.experimental.pallas import tpu as pltpu
from jax.sharding import PartitionSpec as P

DH = 64
EPSILON = 1e-05
SIDE = 4
ROWS = 256
STAT_ROWS = 32
QG = 2 * ROWS + STAT_ROWS
SLOT = QG + 2 * ROWS
LOG2E = 1.4426950408889634
NT = (((1,), (1,)), ((), ()))
BF = jnp.bfloat16
F32 = jnp.float32


def in_vmem(count):
    return [pl.BlockSpec(memory_space=pltpu.VMEM)] * count


def in_smem(count):
    return [pl.BlockSpec(memory_space=pltpu.SMEM)] * count


def prepare_kernel(
    place, lam, q_ref, k_ref, v_ref, maps_ref, lse_ref, out_ref, gain_ref, ysend, plus, minus, far, own
):
    z = place[0]
    gain = gain_ref[...]
    grads = []
    stats = []
    for head in range(2):
        first = maps_ref[0, head].astype(F32)
        second = maps_ref[1, head].astype(F32)
        combined = first - lam[head] * second
        inverse = lax.rsqrt(jnp.mean(combined * combined, axis=-1, keepdims=True) + EPSILON)
        weighted = gain * out_ref[head].astype(F32)
        dot = jnp.mean(combined * weighted, axis=-1, keepdims=True)
        grad = (inverse * weighted - inverse * inverse * inverse * combined * dot).astype(BF)
        wide = grad.astype(F32)
        term1 = jnp.sum((wide * first).T, axis=0, keepdims=True)
        term2 = jnp.sum((wide * second).T, axis=0, keepdims=True)
        lse = lse_ref[head]
        rows = jnp.concatenate([lse[0:1], lse[1:2], term1, term2], axis=0)
        high = rows.astype(BF)
        rest = rows - high.astype(F32)
        middle = rest.astype(BF)
        low = (rest - middle.astype(F32)).astype(F32)
        packed = jnp.concatenate(
            [high.astype(F32), middle.astype(F32), low, jnp.zeros_like(rows)], axis=0
        ).astype(BF)
        grads.append(grad)
        stats.append(packed)
    for copy in range(SIDE):
        ysend[copy, 0:ROWS] = q_ref[1]
        ysend[copy, ROWS : 2 * ROWS] = grads[1]
        ysend[copy, 2 * ROWS : 2 * ROWS + 16] = stats[1][:, 0:128]
        ysend[copy, 2 * ROWS + 16 : QG] = stats[1][:, 128:256]
        ysend[copy, QG : QG + ROWS] = k_ref[0]
        ysend[copy, QG + ROWS : SLOT] = v_ref[0]
    own[0:ROWS] = q_ref[0]
    own[ROWS : 2 * ROWS] = grads[0]
    own[2 * ROWS : 2 * ROWS + 16] = stats[0][:, 0:128]
    own[2 * ROWS + 16 : QG] = stats[0][:, 128:256]
    own[QG : QG + ROWS] = k_ref[1]
    own[QG + ROWS : SLOT] = v_ref[1]

    def send(ref, keys):
        @pl.when(keys)
        def _():
            ref[0:ROWS] = k_ref[1]
            ref[ROWS : 2 * ROWS] = v_ref[1]
            ref[2 * ROWS : QG] = jnp.zeros((STAT_ROWS, 128), BF)

        @pl.when(jnp.logical_not(keys))
        def _():
            ref[...] = own[0:QG]

    send(plus, z < SIDE - 1)
    send(minus, z == 0)
    send(far, z < SIDE // 2)


def attend_kernel(
    place, lam, ybuf, own, plus, minus, far, yret, ret_plus, ret_minus, ret_far, own_q, own_k, own_v,
    buf, stat, kpad, kturn, qpad, dq, dk, dv,
):
    z = place[0]
    y = place[1]
    buf[0:SIDE] = ybuf[...]
    buf[SIDE] = own[...]
    keys_plus = (z > 0).astype(jnp.int32)
    keys_minus = (z == SIDE - 1).astype(jnp.int32)
    keys_far = (z >= SIDE // 2).astype(jnp.int32)
    for slot, (ref, keys) in enumerate(((plus, keys_plus), (minus, keys_minus), (far, keys_far))):
        @pl.when(keys == 1)
        def _():
            buf[SIDE + 1 + slot, QG:SLOT] = ref[0 : 2 * ROWS]

        @pl.when(keys == 0)
        def _():
            buf[SIDE + 1 + slot, 0:QG] = ref[...]

    def ready(slot, carry):
        lane = lax.broadcasted_iota(jnp.int32, (ROWS, 128), 1)
        q = buf[slot, 0:ROWS]
        k = buf[slot, QG : QG + ROWS]
        zero = jnp.zeros_like(q)
        qpad[slot, 0:ROWS] = jnp.where(lane < DH, q, zero)
        qpad[slot, ROWS:] = jnp.where(lane < DH, zero, q)
        kpad[slot, 0:ROWS] = jnp.where(lane < DH, k, zero)
        kpad[slot, ROWS:] = jnp.where(lane < DH, zero, k)
        turned = k.astype(F32).T.astype(BF)
        row = lax.broadcasted_iota(jnp.int32, (128, ROWS), 0)
        none = jnp.zeros_like(turned)
        kturn[slot, :, 0:ROWS] = jnp.where(row < DH, turned, none)
        kturn[slot, :, ROWS:] = jnp.where(row < DH, none, turned)
        left = buf[slot, 2 * ROWS : 2 * ROWS + 16].astype(F32)
        right = buf[slot, 2 * ROWS + 16 : QG].astype(F32)
        pieces = jnp.concatenate([left, right], axis=1)
        rows = pieces[0:4] + pieces[4:8] + pieces[8:12]
        stat[slot, 0:2] = rows[0:2] * LOG2E
        stat[slot, 2:4] = rows[2:4]
        dq[slot] = jnp.zeros((128, ROWS), F32)
        dk[slot] = jnp.zeros((ROWS, 128), F32)
        dv[slot] = jnp.zeros((ROWS, 128), F32)
        return carry

    lax.fori_loop(0, 2 * SIDE, ready, 0)

    def step(item, carry):
        is_own = item < SIDE + 1
        after = item > y
        slot = jnp.where(is_own, SIDE, SIDE + 1 + (item - SIDE - 1) // SIDE)
        other = jnp.where(
            is_own, item - after.astype(jnp.int32), (item - SIDE - 1) % SIDE
        )
        kind = jnp.where(
            is_own,
            after.astype(jnp.int32),
            jnp.where(
                slot == SIDE + 1, keys_plus, jnp.where(slot == SIDE + 2, keys_minus, keys_far)
            ),
        )
        diagonal = jnp.logical_and(is_own, other == y)
        qs = jnp.where(kind == 0, slot, other)
        ks = jnp.where(kind == 0, other, slot)
        shift = jnp.where(diagonal, 0, 2 * ROWS)
        factor = lam[kind]
        q = buf[qs, 0:ROWS]
        g = buf[qs, ROWS : 2 * ROWS]
        v = buf[ks, QG + ROWS : SLOT]
        rows = stat[qs]
        scores = lax.dot_general(kpad[ks], q, NT, preferred_element_type=F32)
        mixed = lax.dot_general(v, g, NT, preferred_element_type=F32)
        key_pos = lax.broadcasted_iota(jnp.int32, (ROWS, ROWS), 0)
        query_pos = lax.broadcasted_iota(jnp.int32, (ROWS, ROWS), 1)
        seen = key_pos <= query_pos + shift
        gone = jnp.full((ROWS, ROWS), -1e30, F32)
        scale = DH ** (-0.5) * LOG2E
        prob1 = jnp.exp2(jnp.where(seen, scores[0:ROWS] * scale - rows[0:1], gone))
        prob2 = factor * jnp.exp2(jnp.where(seen, scores[ROWS:] * scale - rows[1:2], gone))
        weights = (prob1 - prob2).astype(BF)
        score1 = (prob1 * (mixed - rows[2:3])).astype(BF)
        score2 = (prob2 * (rows[3:4] - mixed)).astype(BF)
        dv[ks] += jnp.dot(weights, g, preferred_element_type=F32)
        dk[ks] += jnp.dot(
            jnp.concatenate([score1, score2], axis=1), qpad[qs], preferred_element_type=F32
        )
        dq[qs] += jnp.dot(
            kturn[ks], jnp.concatenate([score1, score2], axis=0), preferred_element_type=F32
        )
        return carry

    lax.fori_loop(0, SIDE * SIDE + 1, step, 0)

    scale = DH ** (-0.5)
    for j in range(SIDE):
        yret[j, 0:ROWS] = (dq[j].T * scale).astype(BF)
        yret[j, ROWS : 2 * ROWS] = (dk[j] * scale).astype(BF)
        yret[j, 2 * ROWS :] = dv[j].astype(BF)
    for slot, (ref, keys) in enumerate(
        ((ret_plus, keys_plus), (ret_minus, keys_minus), (ret_far, keys_far))
    ):
        @pl.when(keys == 1)
        def _():
            ref[0:ROWS] = (dk[SIDE + 1 + slot] * scale).astype(BF)
            ref[ROWS:] = dv[SIDE + 1 + slot].astype(BF)

        @pl.when(keys == 0)
        def _():
            ref[0:ROWS] = (dq[SIDE + 1 + slot].T * scale).astype(BF)
            ref[ROWS:] = jnp.zeros((ROWS, 128), BF)

    own_q[...] = dq[SIDE].T * scale
    own_k[...] = dk[SIDE] * scale
    own_v[...] = dv[SIDE]


def finish_kernel(
    place, yin, back_plus, back_minus, back_far, own_q, own_k, own_v, qg, kg, vg, acc_q, acc_k, acc_v
):
    z = place[0]
    total = yin[0].astype(F32)
    for j in range(1, SIDE):
        total += yin[j].astype(F32)
    qg[1] = total[0:ROWS].astype(BF)
    kg[0] = total[ROWS : 2 * ROWS].astype(BF)
    vg[0] = total[2 * ROWS :].astype(BF)
    acc_q[...] = own_q[...]
    acc_k[...] = own_k[...]
    acc_v[...] = own_v[...]

    def add(ref, keys):
        @pl.when(keys)
        def _():
            acc_k[...] += ref[0:ROWS].astype(F32)
            acc_v[...] += ref[ROWS:].astype(F32)

        @pl.when(jnp.logical_not(keys))
        def _():
            acc_q[...] += ref[0:ROWS].astype(F32)

    add(back_plus, z < SIDE - 1)
    add(back_minus, z == 0)
    add(back_far, z < SIDE // 2)
    qg[0] = acc_q[...].astype(BF)
    kg[1] = acc_k[...].astype(BF)
    vg[1] = acc_v[...].astype(BF)


def shifted(x, steps):
    pairs = []
    for z in range(SIDE):
        for y in range(SIDE):
            pairs.append((z * SIDE + y, (z + steps) % SIDE * SIDE + y))
    return lax.ppermute(x, "sp", pairs)


def along_y(x):
    groups = [[z * SIDE + y for y in range(SIDE)] for z in range(SIDE)]
    return lax.all_to_all(x, "sp", 0, 0, axis_index_groups=groups, tiled=True)


def heads_first(x):
    return jnp.swapaxes(x, -3, -2)


def body(
    latents,
    query_heads,
    key_heads,
    value_heads,
    map_outputs,
    log_sums,
    out_grad,
    mix_lambda,
    norm_gain,
):
    index = lax.axis_index("sp")
    place = jnp.stack([index // SIDE, index % SIDE]).astype(jnp.int32)
    maps = jnp.transpose(map_outputs, (1, 2, 0, 3))
    sums = jnp.transpose(log_sums, (1, 2, 0))
    block = jax.ShapeDtypeStruct((QG, 128), BF)
    ysend, plus, minus, far, own = pl.pallas_call(
        prepare_kernel,
        out_shape=(
            jax.ShapeDtypeStruct((SIDE, SLOT, 128), BF),
            block,
            block,
            block,
            jax.ShapeDtypeStruct((SLOT, 128), BF),
        ),
        in_specs=in_smem(2) + in_vmem(7),
        out_specs=tuple(in_vmem(5)),
        cost_estimate=pl.CostEstimate(flops=10**6, bytes_accessed=3 * 10**6, transcendentals=0),
        compiler_params=pltpu.CompilerParams(vmem_limit_bytes=8 * 2**20),
        name="prepare",
    )(
        place,
        mix_lambda,
        heads_first(query_heads),
        heads_first(key_heads),
        heads_first(value_heads),
        maps,
        sums,
        heads_first(out_grad),
        norm_gain.reshape(1, 128),
    )
    from_plus = shifted(plus, 1)
    from_minus = shifted(minus, -1)
    from_far = shifted(far, 2)
    ybuf = along_y(ysend)

    back = jax.ShapeDtypeStruct((2 * ROWS, 128), BF)
    wide = jax.ShapeDtypeStruct((ROWS, 128), F32)
    slots = 2 * SIDE
    yret, ret_plus, ret_minus, ret_far, own_q, own_k, own_v = pl.pallas_call(
        attend_kernel,
        out_shape=(
            jax.ShapeDtypeStruct((SIDE, 3 * ROWS, 128), BF),
            back,
            back,
            back,
            wide,
            wide,
            wide,
        ),
        in_specs=in_smem(2) + in_vmem(5),
        out_specs=tuple(in_vmem(7)),
        scratch_shapes=[
            pltpu.VMEM((slots, SLOT, 128), BF),
            pltpu.VMEM((slots, 8, ROWS), F32),
            pltpu.VMEM((slots, 2 * ROWS, 128), BF),
            pltpu.VMEM((slots, 128, 2 * ROWS), BF),
            pltpu.VMEM((slots, 2 * ROWS, 128), BF),
            pltpu.VMEM((slots, 128, ROWS), F32),
            pltpu.VMEM((slots, ROWS, 128), F32),
            pltpu.VMEM((slots, ROWS, 128), F32),
        ],
        cost_estimate=pl.CostEstimate(
            flops=17 * 10 * ROWS * ROWS * 128, bytes_accessed=4 * 10**6, transcendentals=0
        ),
        compiler_params=pltpu.CompilerParams(vmem_limit_bytes=20 * 2**20),
        name="attend",
    )(place, mix_lambda, ybuf, own, from_plus, from_minus, from_far)
    back_plus = shifted(ret_plus, -1)
    back_minus = shifted(ret_minus, 1)
    back_far = shifted(ret_far, 2)
    yin = along_y(yret)
    pair = jax.ShapeDtypeStruct((2, ROWS, 128), BF)
    qg, kg, vg = pl.pallas_call(
        finish_kernel,
        out_shape=(pair, pair, pair),
        in_specs=in_smem(1) + in_vmem(7),
        out_specs=tuple(in_vmem(3)),
        scratch_shapes=[pltpu.VMEM((ROWS, 128), F32)] * 3,
        cost_estimate=pl.CostEstimate(flops=10**6, bytes_accessed=2 * 10**6, transcendentals=0),
        compiler_params=pltpu.CompilerParams(vmem_limit_bytes=8 * 2**20),
        name="finish",
    )(place, yin, back_plus, back_minus, back_far, own_q, own_k, own_v)
    query_grad = heads_first(qg)
    parts = lax.dot_general(
        latents,
        jnp.concatenate([qg[0], qg[1]], axis=1),
        (((0,), (0,)), ((), ())),
        preferred_element_type=F32,
    ).astype(BF)
    arrived = lax.all_to_all(
        parts.reshape(SIDE * SIDE, ROWS, 2 * 128), "sp", 0, 0, tiled=True
    )
    weight_grad = arrived.astype(F32).sum(axis=0)
    return (query_grad, heads_first(kg), heads_first(vg), weight_grad)


def solution(mesh):
    placed = (
        P("sp", None),
        P("sp", "tp", None),
        P("sp", "tp", None),
        P("sp", "tp", None),
        P("sp", None, "tp", None),
        P("sp", "tp", None),
        P("sp", "tp", None),
        P("tp"),
        P(),
    )
    return jax.shard_map(
        body,
        mesh=mesh,
        in_specs=placed,
        out_specs=(P("sp", "tp", None), P("sp", "tp", None), P("sp", "tp", None), P("sp", "tp")),
        check_vma=False,
    )
```

```python
import jax
import jax.numpy as jnp
from jax import lax
from jax.experimental import pallas as pl
from jax.experimental.pallas import tpu as pltpu
from jax.sharding import PartitionSpec as P


DH = 64
EPSILON = 1e-05
SIDE = 4
ROWS = 256
HALF = ROWS // 2
WIDE = 1024
STAT_ROWS = 32
QG = 2 * ROWS + STAT_ROWS
SLOT = QG + 2 * ROWS
LOG2E = 1.4426950408889634
NT = (((1,), (1,)), ((), ()))
BF = jnp.bfloat16
F32 = jnp.float32


def iota(shape, dim):
    return lax.broadcasted_iota(jnp.int32, shape, dim)


def one_hot(hit):
    return jnp.where(hit, 1.0, 0.0).astype(BF)


def exact(a, b):
    return jnp.dot(a, b, preferred_element_type=F32)


def turned(eye, x):
    return lax.dot_general(eye, x, NT, preferred_element_type=F32)


def two_heads(spread, first, second):
    parts = []
    for half in range(2):
        rows = pl.ds(half * ROWS, ROWS)
        parts.append(exact(spread, jnp.concatenate([first[rows], second[rows]], axis=1)))
    found = []
    for lanes in (slice(0, 128), slice(128, 256)):
        for head in range(2):
            keep = slice(head * HALF, (head + 1) * HALF)
            found.append(jnp.concatenate([part[keep, lanes] for part in parts], axis=0))
    return found


def prepare_kernel(
    place, lam, q_hbm, k_hbm, v_hbm, maps_hbm, lse_hbm, out_hbm, gain_hbm, lat_hbm,
    yown, zown, plus, minus, far, lat_own, lat_plus, lat_minus, lat_far,
    q_in, k_in, v_in, maps_in, lse_in, out_in, gain_in, sems,
):
    z = place[0]
    core = place[2]
    pairs = [
        (maps_hbm, maps_in), (out_hbm, out_in), (gain_hbm, gain_in), (lse_hbm, lse_in),
        (q_hbm, q_in), (k_hbm, k_in), (v_hbm, v_in),
    ]
    copies = [pltpu.make_async_copy(a, b, sems.at[n]) for n, (a, b) in enumerate(pairs)]
    tokens = pl.ds(pl.multiple_of(core * HALF, HALF), HALF)
    for ref, step in ((lat_plus, 1), (lat_minus, SIDE - 1), (lat_far, 2)):
        columns = pl.ds(pl.multiple_of((z + step) % SIDE * WIDE, WIDE), WIDE)
        copies.append(
            pltpu.make_async_copy(lat_hbm.at[tokens, columns], ref, sems.at[len(copies)])
        )
    columns = pl.ds(pl.multiple_of(z * WIDE, WIDE), WIDE)
    copies.append(pltpu.make_async_copy(lat_hbm.at[:, columns], lat_own, sems.at[len(copies)]))
    for copy in copies:
        copy.start()
    row = iota((ROWS, ROWS), 0)
    col = iota((ROWS, ROWS), 1)
    spread = one_hot(col == 2 * (row % HALF) + row // HALF)
    deal = one_hot(col == 4 * (row % DH) + row // DH)
    for copy in copies[:4]:
        copy.wait()
    left = exact(deal, jnp.concatenate([maps_in[0:256], maps_in[256:512]], axis=1))
    right = exact(deal, jnp.concatenate([maps_in[512:768], maps_in[768:1024]], axis=1))

    def map_rows(which, head):
        rows = slice((which * 2 + head) * DH, (which * 2 + head + 1) * DH)
        return jnp.concatenate(
            [left[rows, 0:128], left[rows, 128:], right[rows, 0:128], right[rows, 128:]], axis=0
        )

    outs = []
    for half in range(2):
        outs.append(exact(spread, out_in[half * ROWS : (half + 1) * ROWS]))
    gain = gain_in[...]
    for head, ref in ((1, yown), (0, zown)):
        first = map_rows(0, head)
        second = map_rows(1, head)
        rows = slice(head * HALF, (head + 1) * HALF)
        cotangent = jnp.concatenate([outs[0][rows], outs[1][rows]], axis=0)
        combined = first - lam[head] * second
        inverse = lax.rsqrt(jnp.mean(combined * combined, axis=-1, keepdims=True) + EPSILON)
        weighted = gain * cotangent
        dot = jnp.mean(combined * weighted, axis=-1, keepdims=True)
        grad = (inverse * weighted - inverse * inverse * inverse * combined * dot).astype(BF)
        wide = grad.astype(F32)
        term1 = jnp.sum((wide * first).T, axis=0, keepdims=True)
        term2 = jnp.sum((wide * second).T, axis=0, keepdims=True)
        lse = lse_in[head]
        table = jnp.concatenate([lse[0:1], lse[1:2], term1, term2], axis=0)
        high = table.astype(BF).astype(F32)
        middle = (table - high).astype(BF).astype(F32)
        low = table - high - middle
        packed = jnp.concatenate([high, middle, low, jnp.zeros_like(table)], axis=0).astype(BF)
        ref[ROWS : 2 * ROWS] = grad
        ref[2 * ROWS : 2 * ROWS + 16] = packed[:, 0:128]
        ref[2 * ROWS + 16 : QG] = packed[:, 128:256]
    for copy in copies[4:7]:
        copy.wait()
    q0, q1, k0, k1 = two_heads(spread, q_in, k_in)
    v0, v1, _, _ = two_heads(spread, v_in, v_in)
    yown[0:ROWS] = q1.astype(BF)
    yown[QG : QG + ROWS] = k0.astype(BF)
    yown[QG + ROWS : SLOT] = v0.astype(BF)
    zown[0:ROWS] = q0.astype(BF)
    zown[QG : QG + ROWS] = k1.astype(BF)
    zown[QG + ROWS : SLOT] = v1.astype(BF)

    def send(ref, keys):
        @pl.when(keys)
        def _():
            ref[0 : 2 * ROWS] = zown[QG:SLOT]
            ref[2 * ROWS : QG] = jnp.zeros((STAT_ROWS, 128), BF)

        @pl.when(jnp.logical_not(keys))
        def _():
            ref[...] = zown[0:QG]

    send(plus, z < SIDE - 1)
    send(minus, z == 0)
    send(far, z < SIDE // 2)
    for copy in copies[7:]:
        copy.wait()


def attend_kernel(
    place, lam, yown, yleft, yright, ytop, ybottom, zown, plus, minus, far,
    q_left, q_right, q_far, q_plus, q_minus, q_zfar,
    kv_left, kv_right, kv_far, v_plus, v_minus, v_zfar, own_q, own_k, own_v,
    buf, stat, kpad, kturn, qpad, dq, dk, dv,
):
    z = place[0]
    y = place[1]
    buf[0] = yown[...]
    buf[1] = yleft[...]
    buf[2] = yright[...]
    buf[3, 0 : SLOT // 2] = ytop[...]
    buf[3, SLOT // 2 :] = ybottom[...]
    buf[SIDE] = zown[...]
    keys_plus = (z > 0).astype(jnp.int32)
    keys_minus = (z == SIDE - 1).astype(jnp.int32)
    keys_far = (z >= SIDE // 2).astype(jnp.int32)
    for slot, (ref, keys) in enumerate(((plus, keys_plus), (minus, keys_minus), (far, keys_far))):
        @pl.when(keys == 1)
        def _():
            buf[SIDE + 1 + slot, QG:SLOT] = ref[0 : 2 * ROWS]

        @pl.when(keys == 0)
        def _():
            buf[SIDE + 1 + slot, 0:QG] = ref[...]

    row = iota((128, 128), 0)
    col = iota((128, 128), 1)
    eye_first = one_hot(jnp.logical_and(row == col, row < DH))
    eye_second = one_hot(jnp.logical_and(row == col, row >= DH))

    def ready(slot, carry):
        lane = iota((ROWS, 128), 1)
        q = buf[slot, 0:ROWS]
        k = buf[slot, QG : QG + ROWS]
        zero = jnp.zeros_like(q)
        qpad[slot, 0:ROWS] = jnp.where(lane < DH, q, zero)
        qpad[slot, ROWS:] = jnp.where(lane < DH, zero, q)
        kpad[slot, 0:ROWS] = jnp.where(lane < DH, k, zero)
        kpad[slot, ROWS:] = jnp.where(lane < DH, zero, k)
        kturn[slot, :, 0:ROWS] = turned(eye_first, k).astype(BF)
        kturn[slot, :, ROWS:] = turned(eye_second, k).astype(BF)
        left = buf[slot, 2 * ROWS : 2 * ROWS + 16].astype(F32)
        right = buf[slot, 2 * ROWS + 16 : QG].astype(F32)
        pieces = jnp.concatenate([left, right], axis=1)
        rows = pieces[0:4] + pieces[4:8] + pieces[8:12]
        stat[slot, 0:2] = rows[0:2] * LOG2E
        stat[slot, 2:4] = rows[2:4]
        dq[slot] = jnp.zeros((128, ROWS), F32)
        dk[slot] = jnp.zeros((ROWS, 128), F32)
        dv[slot] = jnp.zeros((ROWS, 128), F32)
        return carry

    lax.fori_loop(0, 2 * SIDE, ready, 0)

    def pair(zslot, yslot, kind, shift):
        qs = jnp.where(kind == 0, zslot, yslot)
        ks = jnp.where(kind == 0, yslot, zslot)
        factor = lam[kind]
        q = buf[qs, 0:ROWS]
        g = buf[qs, ROWS : 2 * ROWS]
        v = buf[ks, QG + ROWS : SLOT]
        rows = stat[qs]
        scores = lax.dot_general(kpad[ks], q, NT, preferred_element_type=F32)
        mixed = lax.dot_general(v, g, NT, preferred_element_type=F32)
        scale = DH ** (-0.5) * LOG2E
        power1 = scores[0:ROWS] * scale - rows[0:1]
        power2 = scores[ROWS:] * scale - rows[1:2]
        seen = iota((ROWS, ROWS), 0) <= iota((ROWS, ROWS), 1) + shift
        gone = jnp.full((ROWS, ROWS), -1e30, F32)
        prob1 = jnp.exp2(jnp.where(seen, power1, gone))
        prob2 = factor * jnp.exp2(jnp.where(seen, power2, gone))
        weights = (prob1 - prob2).astype(BF)
        score1 = (prob1 * (mixed - rows[2:3])).astype(BF)
        score2 = (prob2 * (rows[3:4] - mixed)).astype(BF)
        dv[ks] += exact(weights, g)
        dk[ks] += exact(jnp.concatenate([score1, score2], axis=1), qpad[qs])
        dq[qs] += exact(kturn[ks], jnp.concatenate([score1, score2], axis=0))

    def step(item, carry):
        own = item < SIDE + 1
        rest = item - SIDE - 1
        zslot = jnp.where(own, SIDE, SIDE + 1 + rest // SIDE)
        yslot = jnp.where(own, jnp.maximum(item - 1, 0), rest % SIDE)
        offset = jnp.where(yslot == 1, SIDE - 1, jnp.where(yslot == 2, 1, yslot - 1))
        behind = jnp.where(
            yslot == 0, item == 0, (y + offset) % SIDE < y
        )
        kind = jnp.where(
            own,
            1 - behind.astype(jnp.int32),
            jnp.where(
                zslot == SIDE + 1, keys_plus, jnp.where(zslot == SIDE + 2, keys_minus, keys_far)
            ),
        )
        shift = jnp.where(item < 2, 0, 2 * ROWS)
        pair(zslot, yslot, kind, shift)
        return carry

    lax.fori_loop(0, SIDE * SIDE + 1, step, 0)

    scale = DH ** (-0.5)

    def put_q(ref, slot):
        value = (dq[slot] * scale).astype(BF)
        ref[0:HALF] = value[:, 0:128]
        ref[HALF:] = value[:, 128:]

    for slot, (ref, kv) in enumerate(((q_left, kv_left), (q_right, kv_right), (q_far, kv_far))):
        put_q(ref, slot + 1)
        kv[0:ROWS] = (dk[slot + 1] * scale).astype(BF)
        kv[ROWS:] = dv[slot + 1].astype(BF)
    for slot, (ref, ref_v, keys) in enumerate(
        ((q_plus, v_plus, keys_plus), (q_minus, v_minus, keys_minus), (q_zfar, v_zfar, keys_far))
    ):
        @pl.when(keys == 1)
        def _():
            ref[...] = (dk[SIDE + 1 + slot] * scale).astype(BF)

        @pl.when(keys == 0)
        def _():
            put_q(ref, SIDE + 1 + slot)

        ref_v[...] = dv[SIDE + 1 + slot].astype(BF)

    own_q[0] = dq[SIDE] * scale
    own_q[1] = dq[0] * scale
    own_k[0] = dk[0] * scale
    own_k[1] = dk[SIDE] * scale
    own_v[0] = dv[0]
    own_v[1] = dv[SIDE]


def queries_kernel(place, own_q, y1, y2, y3, z1, z2, z3, turned_out, rows_out, acc):
    z = place[0]

    def lanes(ref):
        return jnp.concatenate([ref[0:HALF].astype(F32), ref[HALF:].astype(F32)], axis=1)

    acc[...] = own_q[0]
    for ref, keys in ((z1, z < SIDE - 1), (z2, z == 0), (z3, z < SIDE // 2)):
        @pl.when(jnp.logical_not(keys))
        def _():
            acc[...] += lanes(ref)

    first = acc[...].astype(BF)
    second = (own_q[1] + lanes(y1) + lanes(y2) + lanes(y3)).astype(BF)
    turned_out[0:128] = first
    turned_out[128:256] = second
    row = iota((ROWS, ROWS), 0)
    col = iota((ROWS, ROWS), 1)
    weave = one_hot(col == row % 2 * HALF + row // 2)
    for half in range(2):
        keep = slice(half * HALF, (half + 1) * HALF)
        both = jnp.concatenate([first[:, keep], second[:, keep]], axis=1)
        rows_out[half * ROWS : (half + 1) * ROWS] = turned(weave, both).astype(BF)


def keys_kernel(
    place, own_k, own_v, y1, y2, y3, a1, a2, a3, b1, b2, b3, k_out, v_out, acc_k, acc_v
):
    z = place[0]
    acc_k[...] = own_k[1]
    acc_v[...] = own_v[1]
    for ref, ref_v, keys in (
        (a1, b1, z < SIDE - 1), (a2, b2, z == 0), (a3, b3, z < SIDE // 2)
    ):
        @pl.when(keys)
        def _():
            acc_k[...] += ref[...].astype(F32)
            acc_v[...] += ref_v[...].astype(F32)

    row = iota((ROWS, ROWS), 0)
    col = iota((ROWS, ROWS), 1)
    weave = one_hot(col == row % 2 * HALF + row // 2)
    k0 = own_k[0]
    v0 = own_v[0]
    for ref in (y1, y2, y3):
        k0 += ref[0:ROWS].astype(F32)
        v0 += ref[ROWS:].astype(F32)
    k1 = acc_k[...].astype(BF)
    v1 = acc_v[...].astype(BF)
    zero = jnp.concatenate([k0.astype(BF), v0.astype(BF)], axis=1)
    one = jnp.concatenate([k1, v1], axis=1)
    for half in range(2):
        keep = slice(half * HALF, (half + 1) * HALF)
        woven = exact(weave, jnp.concatenate([zero[keep], one[keep]], axis=0)).astype(BF)
        k_out[half * ROWS : (half + 1) * ROWS] = woven[:, 0:128]
        v_out[half * ROWS : (half + 1) * ROWS] = woven[:, 128:256]


def project_kernel(
    place, g0, g1, g2, g3, lat0, m1, m2, m3, s1, s2, s3, own, to_plus, to_minus, to_far, lat
):
    y = place[1]
    core = place[2]
    lat[0:ROWS] = lat0[...]
    for n, (mine, swap) in enumerate(((m1, s1), (m2, s2), (m3, s3))):
        base = (n + 1) * ROWS
        for part in range(2):
            rows = slice(base + part * HALF, base + (part + 1) * HALF)

            @pl.when(core == part)
            def _():
                lat[rows] = mine[...]

            @pl.when(core != part)
            def _():
                lat[rows] = swap[...]

    grads = jnp.concatenate([g0[...], g1[...], g2[...], g3[...]], axis=1)
    for ref, step in ((to_plus, 1), (to_minus, SIDE - 1), (to_far, 2), (own, 0)):
        columns = pl.ds(pl.multiple_of((y + step) % SIDE * ROWS, ROWS), ROWS)
        ref[...] = exact(grads, lat[:, columns]).astype(ref.dtype)


def total_kernel(own, t1, t2, t3, out):
    whole = own[...] + t1[...].astype(F32) + t2[...].astype(F32) + t3[...].astype(F32)
    out[...] = whole.T


def moved(x, dz, dy):
    pairs = []
    for z in range(SIDE):
        for y in range(SIDE):
            pairs.append((z * SIDE + y, (z + dz) % SIDE * SIDE + (y + dy) % SIDE))
    return lax.ppermute(x, "sp", pairs)


def partner(x):
    return lax.ppermute(x, "tp", [(t, t ^ 1) for t in range(lax.axis_size("tp"))])


def shape(*dims, dtype=BF):
    return jax.ShapeDtypeStruct(dims, dtype)


def call(kernel, outs, scalars, hbm, vmem, scratch, flops, mib=16):
    return pl.pallas_call(
        kernel,
        out_shape=outs,
        in_specs=[pl.BlockSpec(memory_space=pltpu.SMEM)] * scalars
        + [pl.BlockSpec(memory_space=pltpu.HBM)] * hbm
        + [pl.BlockSpec(memory_space=pltpu.VMEM)] * vmem,
        out_specs=jax.tree.map(lambda _: pl.BlockSpec(memory_space=pltpu.VMEM), outs),
        scratch_shapes=scratch,
        compiler_params=pltpu.CompilerParams(vmem_limit_bytes=mib * 2**20),
        cost_estimate=pl.CostEstimate(flops=flops, bytes_accessed=10**6, transcendentals=0),
    )


def body(
    latents,
    query_heads,
    key_heads,
    value_heads,
    map_outputs,
    log_sums,
    out_grad,
    mix_lambda,
    norm_gain,
):
    index = lax.axis_index("sp")
    place = jnp.stack([index // SIDE, index % SIDE, lax.axis_index("tp") % 2]).astype(jnp.int32)
    part = shape(HALF, WIDE)
    yown, zown, plus, minus, far, lat_own, lat_plus, lat_minus, lat_far = call(
        prepare_kernel,
        (shape(SLOT, 128),) * 2 + (shape(QG, 128),) * 3 + (shape(ROWS, WIDE), part, part, part),
        2,
        8,
        0,
        [pltpu.VMEM((2 * ROWS, 128), BF)] * 3
        + [
            pltpu.VMEM((4 * ROWS, 128), BF),
            pltpu.VMEM((2, 2, ROWS), F32),
            pltpu.VMEM((2 * ROWS, 128), BF),
            pltpu.VMEM((1, 128), F32),
            pltpu.SemaphoreType.DMA((11,)),
        ],
        10**8,
        54,
    )(
        place,
        mix_lambda,
        query_heads.reshape(2 * ROWS, 128),
        key_heads.reshape(2 * ROWS, 128),
        value_heads.reshape(2 * ROWS, 128),
        map_outputs.reshape(4 * ROWS, 128),
        jnp.transpose(log_sums, (1, 2, 0)),
        out_grad.reshape(2 * ROWS, 128),
        norm_gain.reshape(1, 128),
        latents,
    )
    yleft = moved(yown, 0, 1)
    yright = moved(yown, 0, -1)
    zplus = moved(plus, 1, 0)
    zminus = moved(minus, -1, 0)
    zfar = moved(far, 2, 0)
    ytop = moved(yleft[0 : SLOT // 2], 0, 1)
    ybottom = moved(yright[SLOT // 2 :], 0, -1)
    mine = (moved(lat_plus, 1, 0), moved(lat_minus, -1, 0), moved(lat_far, 2, 0))
    swap = tuple(partner(x) for x in mine)

    slots = 2 * SIDE
    small = shape(ROWS, 128)
    both = shape(2 * ROWS, 128)
    results = call(
        attend_kernel,
        (small,) * 6
        + (both,) * 3
        + (small,) * 3
        + (shape(2, 128, ROWS, dtype=F32),)
        + (shape(2, ROWS, 128, dtype=F32),) * 2,
        2,
        0,
        9,
        [
            pltpu.VMEM((slots, SLOT, 128), BF),
            pltpu.VMEM((slots, 8, ROWS), F32),
            pltpu.VMEM((slots, 2 * ROWS, 128), BF),
            pltpu.VMEM((slots, 128, 2 * ROWS), BF),
            pltpu.VMEM((slots, 2 * ROWS, 128), BF),
            pltpu.VMEM((slots, 128, ROWS), F32),
            pltpu.VMEM((slots, ROWS, 128), F32),
            pltpu.VMEM((slots, ROWS, 128), F32),
        ],
        17 * 10 * ROWS * ROWS * 128,
        24,
    )(place, mix_lambda, yown, yleft, yright, ytop, ybottom, zown, zplus, zminus, zfar)
    q_left, q_right, q_far, q_plus, q_minus, q_zfar = results[0:6]
    kv_left, kv_right, kv_far, v_plus, v_minus, v_zfar = results[6:12]
    own_q, own_k, own_v = results[12:15]
    q_back = (
        moved(q_left, 0, -1),
        moved(q_right, 0, 1),
        moved(q_far, 0, 2),
        moved(q_plus, -1, 0),
        moved(q_minus, 1, 0),
        moved(q_zfar, 2, 0),
    )
    turned_grad, query_rows = call(
        queries_kernel,
        (shape(ROWS, ROWS), shape(2 * ROWS, 128)),
        1,
        0,
        7,
        [pltpu.VMEM((128, ROWS), F32)],
        10**7,
    )(place, own_q, *q_back)
    grads = (
        turned_grad, moved(turned_grad, 1, 0), moved(turned_grad, -1, 0), moved(turned_grad, 2, 0)
    )
    kv_back = (moved(kv_left, 0, -1), moved(kv_right, 0, 1), moved(kv_far, 0, 2))
    v_back = (moved(v_plus, -1, 0), moved(v_minus, 1, 0), moved(v_zfar, 2, 0))
    key_rows, value_rows = call(
        keys_kernel,
        (shape(2 * ROWS, 128),) * 2,
        1,
        0,
        11,
        [pltpu.VMEM((ROWS, 128), F32)] * 2,
        10**7,
    )(place, own_k, own_v, *kv_back, *q_back[3:], *v_back)
    square = shape(ROWS, ROWS)
    own, to_plus, to_minus, to_far = call(
        project_kernel,
        (shape(ROWS, ROWS, dtype=F32), square, square, square),
        1,
        0,
        11,
        [pltpu.VMEM((WIDE, WIDE), BF)],
        2 * WIDE * WIDE * ROWS,
    )(place, *grads, lat_own, *mine, *swap)
    weight_grad = call(total_kernel, shape(ROWS, ROWS, dtype=F32), 0, 0, 4, [], 10**6)(
        own, moved(to_plus, 0, 1), moved(to_minus, 0, -1), moved(to_far, 0, 2)
    )
    whole = (ROWS, 2, 128)
    return (
        query_rows.reshape(whole),
        key_rows.reshape(whole),
        value_rows.reshape(whole),
        weight_grad,
    )


def solution(mesh):
    placed = (
        P("sp", None),
        P("sp", "tp", None),
        P("sp", "tp", None),
        P("sp", "tp", None),
        P("sp", None, "tp", None),
        P("sp", "tp", None),
        P("sp", "tp", None),
        P("tp"),
        P(),
    )
    return jax.shard_map(
        body,
        mesh=mesh,
        in_specs=placed,
        out_specs=(P("sp", "tp", None), P("sp", "tp", None), P("sp", "tp", None), P("sp", "tp")),
        check_vma=False,
    )
```

```python
import jax
import jax.numpy as jnp
from jax import lax
from jax.experimental import pallas as pl
from jax.experimental.pallas import tpu as pltpu
from jax.sharding import PartitionSpec as P


DH = 64
EPSILON = 1e-05
SIDE = 4
ROWS = 256
HALF = ROWS // 2
WIDE = 1024
STAT_ROWS = 32
QG = 2 * ROWS + STAT_ROWS
SLOT = QG + 2 * ROWS
LOG2E = 1.4426950408889634
NT = (((1,), (1,)), ((), ()))
BF = jnp.bfloat16
F32 = jnp.float32


def iota(shape, dim):
    return lax.broadcasted_iota(jnp.int32, shape, dim)


def one_hot(hit):
    return jnp.where(hit, 1.0, 0.0).astype(BF)


def exact(a, b):
    return jnp.dot(a, b, preferred_element_type=F32)


def turned(eye, x):
    return lax.dot_general(eye, x, NT, preferred_element_type=F32)


def two_heads(spread, first, second):
    parts = []
    for half in range(2):
        rows = pl.ds(half * ROWS, ROWS)
        parts.append(exact(spread, jnp.concatenate([first[rows], second[rows]], axis=1)))
    found = []
    for lanes in (slice(0, 128), slice(128, 256)):
        for head in range(2):
            keep = slice(head * HALF, (head + 1) * HALF)
            found.append(jnp.concatenate([part[keep, lanes] for part in parts], axis=0))
    return found


def position():
    index = lax.axis_index("sp")
    return index // SIDE, lax.rem(index, SIDE), lax.rem(lax.axis_index("tp"), 2)


def prepare_kernel(
    lam, q_hbm, k_hbm, v_hbm, maps_hbm, lse_hbm, out_hbm, gain_hbm,
    yown, zown, plus, minus, far,
    q_in, k_in, v_in, maps_in, lse_in, out_in, gain_in, sems,
):
    z, _, _ = position()
    pairs = [
        (maps_hbm, maps_in), (out_hbm, out_in), (gain_hbm, gain_in), (lse_hbm, lse_in),
        (q_hbm, q_in), (k_hbm, k_in), (v_hbm, v_in),
    ]
    copies = [pltpu.make_async_copy(a, b, sems.at[n]) for n, (a, b) in enumerate(pairs)]
    for copy in copies:
        copy.start()
    row = iota((ROWS, ROWS), 0)
    col = iota((ROWS, ROWS), 1)
    spread = one_hot(col == 2 * (row % HALF) + row // HALF)
    deal = one_hot(col == 4 * (row % DH) + row // DH)
    for copy in copies[:4]:
        copy.wait()
    left = exact(deal, jnp.concatenate([maps_in[0:256], maps_in[256:512]], axis=1))
    right = exact(deal, jnp.concatenate([maps_in[512:768], maps_in[768:1024]], axis=1))

    def map_rows(which, head):
        rows = slice((which * 2 + head) * DH, (which * 2 + head + 1) * DH)
        return jnp.concatenate(
            [left[rows, 0:128], left[rows, 128:], right[rows, 0:128], right[rows, 128:]], axis=0
        )

    outs = []
    for half in range(2):
        outs.append(exact(spread, out_in[half * ROWS : (half + 1) * ROWS]))
    gain = gain_in[...]
    for head, ref in ((1, yown), (0, zown)):
        first = map_rows(0, head)
        second = map_rows(1, head)
        rows = slice(head * HALF, (head + 1) * HALF)
        cotangent = jnp.concatenate([outs[0][rows], outs[1][rows]], axis=0)
        combined = first - lam[head] * second
        inverse = lax.rsqrt(jnp.mean(combined * combined, axis=-1, keepdims=True) + EPSILON)
        weighted = gain * cotangent
        dot = jnp.mean(combined * weighted, axis=-1, keepdims=True)
        grad = (inverse * weighted - inverse * inverse * inverse * combined * dot).astype(BF)
        wide = grad.astype(F32)
        term1 = jnp.sum((wide * first).T, axis=0, keepdims=True)
        term2 = jnp.sum((wide * second).T, axis=0, keepdims=True)
        lse = lse_in[head]
        table = jnp.concatenate([lse[0:1], lse[1:2], term1, term2], axis=0)
        high = table.astype(BF).astype(F32)
        middle = (table - high).astype(BF).astype(F32)
        low = table - high - middle
        packed = jnp.concatenate([high, middle, low, jnp.zeros_like(table)], axis=0).astype(BF)
        ref[ROWS : 2 * ROWS] = grad
        ref[2 * ROWS : 2 * ROWS + 16] = packed[:, 0:128]
        ref[2 * ROWS + 16 : QG] = packed[:, 128:256]
    for copy in copies[4:7]:
        copy.wait()
    q0, q1, k0, k1 = two_heads(spread, q_in, k_in)
    v0, v1, _, _ = two_heads(spread, v_in, v_in)
    yown[0:ROWS] = q1.astype(BF)
    yown[QG : QG + ROWS] = k0.astype(BF)
    yown[QG + ROWS : SLOT] = v0.astype(BF)
    zown[0:ROWS] = q0.astype(BF)
    zown[QG : QG + ROWS] = k1.astype(BF)
    zown[QG + ROWS : SLOT] = v1.astype(BF)

    def send(ref, keys):
        @pl.when(keys)
        def _():
            ref[0 : 2 * ROWS] = zown[QG:SLOT]
            ref[2 * ROWS : QG] = jnp.zeros((STAT_ROWS, 128), BF)

        @pl.when(jnp.logical_not(keys))
        def _():
            ref[...] = zown[0:QG]

    send(plus, z < SIDE - 1)
    send(minus, z == 0)
    send(far, z < SIDE // 2)


def fetch_kernel(lat_hbm, lat_own, lat_near, lat_far, sems):
    z, _, core = position()

    def columns(block):
        return pl.ds(pl.multiple_of(lax.rem(block, SIDE) * WIDE, WIDE), WIDE)

    tokens = pl.ds(pl.multiple_of(core * HALF, HALF), HALF)
    near = jnp.where(core == 0, z + 1, z + SIDE - 1)
    copies = (
        pltpu.make_async_copy(lat_hbm.at[:, columns(near)], lat_near, sems.at[0]),
        pltpu.make_async_copy(lat_hbm.at[tokens, columns(z + 2)], lat_far, sems.at[1]),
        pltpu.make_async_copy(lat_hbm.at[:, columns(z)], lat_own, sems.at[2]),
    )
    for copy in copies:
        copy.start()
    for copy in copies:
        copy.wait()


def attend_kernel(
    lam, yown, yleft, yright, ytop, ybottom, zown, plus, minus, far,
    q_left, q_right, q_far, r_plus, r_minus, r_far,
    kv_left, kv_right, kv_far, own_q, own_k, own_v,
    buf, stat, kpad, kturn, qpad, dq, dk, dv, wide_w, tall_s,
):
    z, y, _ = position()
    buf[0] = yown[...]
    buf[1] = yleft[...]
    buf[2] = yright[...]
    buf[3, 0 : SLOT // 2] = ytop[...]
    buf[3, SLOT // 2 :] = ybottom[...]
    buf[SIDE] = zown[...]
    keys_plus = (z > 0).astype(jnp.int32)
    keys_minus = (z == SIDE - 1).astype(jnp.int32)
    keys_far = (z >= SIDE // 2).astype(jnp.int32)
    for slot, (ref, keys) in enumerate(((plus, keys_plus), (minus, keys_minus), (far, keys_far))):
        @pl.when(keys == 1)
        def _():
            buf[SIDE + 1 + slot, QG:SLOT] = ref[0 : 2 * ROWS]

        @pl.when(keys == 0)
        def _():
            buf[SIDE + 1 + slot, 0:QG] = ref[...]

    row = iota((128, 128), 0)
    col = iota((128, 128), 1)
    eye_first = one_hot(jnp.logical_and(row == col, row < DH))
    eye_second = one_hot(jnp.logical_and(row == col, row >= DH))

    def ready(slot, carry):
        lane = iota((ROWS, 128), 1)
        q = buf[slot, 0:ROWS]
        k = buf[slot, QG : QG + ROWS]
        zero = jnp.zeros_like(q)
        qpad[slot, 0:ROWS] = jnp.where(lane < DH, q, zero)
        qpad[slot, ROWS:] = jnp.where(lane < DH, zero, q)
        kpad[slot, 0:ROWS] = jnp.where(lane < DH, k, zero)
        kpad[slot, ROWS:] = jnp.where(lane < DH, zero, k)
        kturn[slot, :, 0:ROWS] = turned(eye_first, k).astype(BF)
        kturn[slot, :, ROWS:] = turned(eye_second, k).astype(BF)
        left = buf[slot, 2 * ROWS : 2 * ROWS + 16].astype(F32)
        right = buf[slot, 2 * ROWS + 16 : QG].astype(F32)
        pieces = jnp.concatenate([left, right], axis=1)
        rows = pieces[0:4] + pieces[4:8] + pieces[8:12]
        stat[slot, 0:2] = rows[0:2] * LOG2E
        stat[slot, 2:4] = rows[2:4]
        dq[slot] = jnp.zeros((128, ROWS), F32)
        dk[slot] = jnp.zeros((ROWS, 128), F32)
        dv[slot] = jnp.zeros((ROWS, 128), F32)
        return carry

    lax.fori_loop(0, 2 * SIDE, ready, 0)

    def slots_of(item):
        own = item < SIDE + 1
        rest = item - SIDE - 1
        zslot = jnp.where(own, SIDE, SIDE + 1 + rest // SIDE)
        yslot = jnp.where(own, jnp.maximum(item - 1, 0), lax.rem(jnp.maximum(rest, 0), SIDE))
        offset = jnp.where(yslot == 1, SIDE - 1, jnp.where(yslot == 2, 1, yslot - 1))
        behind = jnp.where(yslot == 0, item == 0, lax.rem(y + offset, SIDE) < y)
        kind = jnp.where(
            own,
            1 - behind.astype(jnp.int32),
            jnp.where(
                zslot == SIDE + 1, keys_plus, jnp.where(zslot == SIDE + 2, keys_minus, keys_far)
            ),
        )
        qs = jnp.where(kind == 0, zslot, yslot)
        ks = jnp.where(kind == 0, yslot, zslot)
        return qs, ks, kind

    def front(item):
        qs, ks, kind = slots_of(item)
        shift = jnp.where(item < 2, 0, 2 * ROWS)
        factor = lam[kind]
        q = buf[qs, 0:ROWS]
        g = buf[qs, ROWS : 2 * ROWS]
        v = buf[ks, QG + ROWS : SLOT]
        rows = stat[qs]
        scores = lax.dot_general(kpad[ks], q, NT, preferred_element_type=F32)
        mixed = lax.dot_general(v, g, NT, preferred_element_type=F32)
        scale = DH ** (-0.5) * LOG2E
        power1 = scores[0:ROWS] * scale - rows[0:1]
        power2 = scores[ROWS:] * scale - rows[1:2]
        seen = iota((ROWS, ROWS), 0) <= iota((ROWS, ROWS), 1) + shift
        gone = jnp.full((ROWS, ROWS), -1e30, F32)
        prob1 = jnp.exp2(jnp.where(seen, power1, gone))
        prob2 = factor * jnp.exp2(jnp.where(seen, power2, gone))
        weights = (prob1 - prob2).astype(BF)
        score1 = (prob1 * (mixed - rows[2:3])).astype(BF)
        score2 = (prob2 * (rows[3:4] - mixed)).astype(BF)
        return weights, score1, score2

    def keep(values):
        weights, score1, score2 = values
        wide_w[...] = weights
        tall_s[0:ROWS] = score1
        tall_s[ROWS:] = score2

    def back(item):
        qs, ks, _ = slots_of(item)
        weights = wide_w[...]
        score1 = tall_s[0:ROWS]
        score2 = tall_s[ROWS:]
        g = buf[qs, ROWS : 2 * ROWS]
        add_v = exact(weights, g)
        add_k = exact(jnp.concatenate([score1, score2], axis=1), qpad[qs])
        add_q = exact(kturn[ks], jnp.concatenate([score1, score2], axis=0))
        return qs, ks, add_q, add_k, add_v

    def add(sums):
        qs, ks, add_q, add_k, add_v = sums
        dv[ks] += add_v
        dk[ks] += add_k
        dq[qs] += add_q

    items = SIDE * SIDE + 1
    keep(front(0))

    def step(item, carry):
        sums = back(item)
        values = front(item + 1)
        add(sums)
        keep(values)
        return carry

    lax.fori_loop(0, items - 1, step, 0)
    add(back(items - 1))

    scale = DH ** (-0.5)

    def put_q(ref, slot):
        value = (dq[slot] * scale).astype(BF)
        ref[0:HALF] = value[:, 0:128]
        ref[HALF:ROWS] = value[:, 128:]

    for slot, (ref, kv) in enumerate(((q_left, kv_left), (q_right, kv_right), (q_far, kv_far))):
        put_q(ref, slot + 1)
        kv[0:ROWS] = (dk[slot + 1] * scale).astype(BF)
        kv[ROWS:] = dv[slot + 1].astype(BF)
    for slot, (ref, keys) in enumerate(
        ((r_plus, keys_plus), (r_minus, keys_minus), (r_far, keys_far))
    ):
        @pl.when(keys == 1)
        def _():
            ref[0:ROWS] = (dk[SIDE + 1 + slot] * scale).astype(BF)
            ref[ROWS:] = dv[SIDE + 1 + slot].astype(BF)

        @pl.when(keys == 0)
        def _():
            put_q(ref, SIDE + 1 + slot)
            ref[ROWS:] = jnp.zeros((ROWS, 128), BF)

    own_q[0] = dq[SIDE] * scale
    own_q[1] = dq[0] * scale
    own_k[0] = dk[0] * scale
    own_k[1] = dk[SIDE] * scale
    own_v[0] = dv[0]
    own_v[1] = dv[SIDE]


def queries_kernel(own_q, y1, y2, y3, z1, z2, z3, turned_out, acc):
    z, _, _ = position()

    def lanes(ref):
        return jnp.concatenate([ref[0:HALF].astype(F32), ref[HALF:ROWS].astype(F32)], axis=1)

    acc[...] = own_q[0]
    for ref, keys in ((z1, z < SIDE - 1), (z2, z == 0), (z3, z < SIDE // 2)):
        @pl.when(jnp.logical_not(keys))
        def _():
            acc[...] += lanes(ref)

    turned_out[0:128] = acc[...].astype(BF)
    turned_out[128:256] = (own_q[1] + lanes(y1) + lanes(y2) + lanes(y3)).astype(BF)


def keys_kernel(
    own_k, own_v, y1, y2, y3, z1, z2, z3, turned_in, q_out, k_out, v_out, acc_k, acc_v
):
    z, _, _ = position()
    acc_k[...] = own_k[1]
    acc_v[...] = own_v[1]
    for ref, keys in ((z1, z < SIDE - 1), (z2, z == 0), (z3, z < SIDE // 2)):
        @pl.when(keys)
        def _():
            acc_k[...] += ref[0:ROWS].astype(F32)
            acc_v[...] += ref[ROWS:].astype(F32)

    row = iota((ROWS, ROWS), 0)
    col = iota((ROWS, ROWS), 1)
    weave = one_hot(col == row % 2 * HALF + row // 2)
    k0 = own_k[0]
    v0 = own_v[0]
    for ref in (y1, y2, y3):
        k0 += ref[0:ROWS].astype(F32)
        v0 += ref[ROWS:].astype(F32)
    zero = jnp.concatenate([k0.astype(BF), v0.astype(BF)], axis=1)
    one = jnp.concatenate([acc_k[...].astype(BF), acc_v[...].astype(BF)], axis=1)
    for half in range(2):
        keep = slice(half * HALF, (half + 1) * HALF)
        rows = slice(half * ROWS, (half + 1) * ROWS)
        woven = exact(weave, jnp.concatenate([zero[keep], one[keep]], axis=0)).astype(BF)
        k_out[rows] = woven[:, 0:128]
        v_out[rows] = woven[:, 128:256]
        both = jnp.concatenate([turned_in[0:128, keep], turned_in[128:256, keep]], axis=1)
        q_out[rows] = turned(weave, both).astype(BF)


def project_kernel(
    g0, g1, g2, g3, lat0, near, near_swap, far, far_swap, own, to_plus, to_minus, to_far, lat
):
    _, y, core = position()
    lat[0:ROWS] = lat0[...]
    first = slice(ROWS, 2 * ROWS)
    second = slice(2 * ROWS, 3 * ROWS)
    third = slice(3 * ROWS, 3 * ROWS + HALF)
    fourth = slice(3 * ROWS + HALF, 4 * ROWS)

    @pl.when(core == 0)
    def _():
        lat[first] = near[...]
        lat[second] = near_swap[...]
        lat[third] = far[...]
        lat[fourth] = far_swap[...]

    @pl.when(core == 1)
    def _():
        lat[first] = near_swap[...]
        lat[second] = near[...]
        lat[third] = far_swap[...]
        lat[fourth] = far[...]

    grads = jnp.concatenate([g0[...], g1[...], g2[...], g3[...]], axis=1)
    for ref, step in ((to_plus, 1), (to_minus, SIDE - 1), (to_far, 2), (own, 0)):
        columns = pl.ds(pl.multiple_of(lax.rem(y + step, SIDE) * ROWS, ROWS), ROWS)
        ref[...] = exact(grads, lat[:, columns]).astype(ref.dtype)


def total_kernel(own, t1, t2, t3, out):
    whole = own[...] + t1[...].astype(F32) + t2[...].astype(F32) + t3[...].astype(F32)
    out[...] = whole.T


def moved(x, dz, dy):
    pairs = []
    for z in range(SIDE):
        for y in range(SIDE):
            pairs.append((z * SIDE + y, (z + dz) % SIDE * SIDE + (y + dy) % SIDE))
    return lax.ppermute(x, "sp", pairs)


def moved_apart(x):
    heads = lax.axis_size("tp")
    pairs = []
    for z in range(SIDE):
        for y in range(SIDE):
            for t in range(heads):
                there = (z + (1 if t % 2 == 0 else SIDE - 1)) % SIDE * SIDE + y
                pairs.append(((z * SIDE + y) * heads + t, there * heads + t))
    return lax.ppermute(x, ("sp", "tp"), pairs)


def partner(x):
    return lax.ppermute(x, "tp", [(t, t ^ 1) for t in range(lax.axis_size("tp"))])


def shape(*dims, dtype=BF):
    return jax.ShapeDtypeStruct(dims, dtype)


def call(kernel, outs, scalars, hbm, vmem, scratch, flops, mib=16):
    calling = pl.pallas_call(
        kernel,
        out_shape=outs,
        in_specs=[pl.BlockSpec(memory_space=pltpu.SMEM)] * scalars
        + [pl.BlockSpec(memory_space=pltpu.HBM)] * hbm
        + [pl.BlockSpec(memory_space=pltpu.VMEM)] * vmem,
        out_specs=jax.tree.map(lambda _: pl.BlockSpec(memory_space=pltpu.VMEM), outs),
        scratch_shapes=scratch,
        compiler_params=pltpu.CompilerParams(vmem_limit_bytes=mib * 2**20),
        cost_estimate=pl.CostEstimate(flops=flops, bytes_accessed=10**6, transcendentals=0),
    )

    def run(*arrays):
        held = [
            pltpu.with_memory_space_constraint(x, pltpu.HBM)
            for x in arrays[scalars : scalars + hbm]
        ]
        return calling(*arrays[:scalars], *held, *arrays[scalars + hbm :])

    return run


def body(
    latents,
    query_heads,
    key_heads,
    value_heads,
    map_outputs,
    log_sums,
    out_grad,
    mix_lambda,
    norm_gain,
):
    yown, zown, plus, minus, far = call(
        prepare_kernel,
        (shape(SLOT, 128),) * 2 + (shape(QG, 128),) * 3,
        1,
        7,
        0,
        [pltpu.VMEM((2 * ROWS, 128), BF)] * 3
        + [
            pltpu.VMEM((4 * ROWS, 128), BF),
            pltpu.VMEM((2, 2, ROWS), F32),
            pltpu.VMEM((2 * ROWS, 128), BF),
            pltpu.VMEM((1, 128), F32),
            pltpu.SemaphoreType.DMA((7,)),
        ],
        10**8,
    )(
        mix_lambda,
        query_heads.reshape(2 * ROWS, 128),
        key_heads.reshape(2 * ROWS, 128),
        value_heads.reshape(2 * ROWS, 128),
        map_outputs.reshape(4 * ROWS, 128),
        jnp.transpose(log_sums, (1, 2, 0)),
        out_grad.reshape(2 * ROWS, 128),
        norm_gain.reshape(1, 128),
    )
    yleft = moved(yown, 0, 1)
    yright = moved(yown, 0, -1)
    zplus = moved(plus, 1, 0)
    zminus = moved(minus, -1, 0)
    zfar = moved(far, 2, 0)
    ytop = moved(yleft[0 : SLOT // 2], 0, 1)
    ybottom = moved(yright[SLOT // 2 :], 0, -1)
    lat_own, lat_near, lat_far = call(
        fetch_kernel,
        (shape(ROWS, WIDE), shape(ROWS, WIDE), shape(HALF, WIDE)),
        0,
        1,
        0,
        [pltpu.SemaphoreType.DMA((3,))],
        10**7,
        1,
    )(latents)
    near = moved_apart(lat_near)
    apart = moved(lat_far, 2, 0)
    near_swap = partner(near)
    apart_swap = partner(apart)

    slots = 2 * SIDE
    small = shape(ROWS, 128)
    both = shape(2 * ROWS, 128)
    results = call(
        attend_kernel,
        (small,) * 3
        + (both,) * 6
        + (shape(2, 128, ROWS, dtype=F32),)
        + (shape(2, ROWS, 128, dtype=F32),) * 2,
        1,
        0,
        9,
        [
            pltpu.VMEM((slots, SLOT, 128), BF),
            pltpu.VMEM((slots, 8, ROWS), F32),
            pltpu.VMEM((slots, 2 * ROWS, 128), BF),
            pltpu.VMEM((slots, 128, 2 * ROWS), BF),
            pltpu.VMEM((slots, 2 * ROWS, 128), BF),
            pltpu.VMEM((slots, 128, ROWS), F32),
            pltpu.VMEM((slots, ROWS, 128), F32),
            pltpu.VMEM((slots, ROWS, 128), F32),
            pltpu.VMEM((ROWS, ROWS), BF),
            pltpu.VMEM((2 * ROWS, ROWS), BF),
        ],
        17 * 10 * ROWS * ROWS * 128,
        24,
    )(mix_lambda, yown, yleft, yright, ytop, ybottom, zown, zplus, zminus, zfar)
    q_left, q_right, q_far, r_plus, r_minus, r_far = results[0:6]
    kv_left, kv_right, kv_far, own_q, own_k, own_v = results[6:12]
    q_back = (moved(q_left, 0, -1), moved(q_right, 0, 1), moved(q_far, 0, 2))
    z_back = (moved(r_plus, -1, 0), moved(r_minus, 1, 0), moved(r_far, 2, 0))
    turned_grad = call(
        queries_kernel, shape(ROWS, ROWS), 0, 0, 7, [pltpu.VMEM((128, ROWS), F32)], 10**7
    )(own_q, *q_back, *z_back)
    grads = (
        turned_grad, moved(turned_grad, 1, 0), moved(turned_grad, -1, 0), moved(turned_grad, 2, 0)
    )
    kv_back = (moved(kv_left, 0, -1), moved(kv_right, 0, 1), moved(kv_far, 0, 2))
    square = shape(ROWS, ROWS)
    own, to_plus, to_minus, to_far = call(
        project_kernel,
        (shape(ROWS, ROWS, dtype=F32), square, square, square),
        0,
        0,
        9,
        [pltpu.VMEM((WIDE, WIDE), BF)],
        2 * WIDE * WIDE * ROWS,
    )(*grads, lat_own, near, near_swap, apart, apart_swap)
    query_rows, key_rows, value_rows = call(
        keys_kernel, (shape(2 * ROWS, 128),) * 3, 0, 0, 9, [pltpu.VMEM((ROWS, 128), F32)] * 2, 10**7
    )(own_k, own_v, *kv_back, *z_back, turned_grad)
    weight_grad = call(total_kernel, shape(ROWS, ROWS, dtype=F32), 0, 0, 4, [], 10**6)(
        own, moved(to_plus, 0, 1), moved(to_minus, 0, -1), moved(to_far, 0, 2)
    )
    whole = (ROWS, 2, 128)
    return (
        query_rows.reshape(whole),
        key_rows.reshape(whole),
        value_rows.reshape(whole),
        weight_grad,
    )


def solution(mesh):
    placed = (
        P("sp", None),
        P("sp", "tp", None),
        P("sp", "tp", None),
        P("sp", "tp", None),
        P("sp", None, "tp", None),
        P("sp", "tp", None),
        P("sp", "tp", None),
        P("tp"),
        P(),
    )
    return jax.shard_map(
        body,
        mesh=mesh,
        in_specs=placed,
        out_specs=(P("sp", "tp", None), P("sp", "tp", None), P("sp", "tp", None), P("sp", "tp")),
        check_vma=False,
    )
```

```python
import jax
import jax.numpy as jnp
from jax import lax
from jax.experimental import pallas as pl
from jax.experimental.pallas import tpu as pltpu
from jax.sharding import PartitionSpec as P


DH = 64
EPSILON = 1e-05
SIDE = 4
ROWS = 256
HALF = ROWS // 2
WIDE = 1024
STAT_ROWS = 32
QG = 2 * ROWS + STAT_ROWS
SLOT = QG + 2 * ROWS
LOG2E = 1.4426950408889634
NT = (((1,), (1,)), ((), ()))
BF = jnp.bfloat16
F32 = jnp.float32


def iota(shape, dim):
    return lax.broadcasted_iota(jnp.int32, shape, dim)


def one_hot(hit):
    return jnp.where(hit, 1.0, 0.0).astype(BF)


def exact(a, b):
    return jnp.dot(a, b, preferred_element_type=F32)


def turned(eye, x):
    return lax.dot_general(eye, x, NT, preferred_element_type=F32)


def two_heads(spread, first, second):
    parts = []
    for half in range(2):
        rows = pl.ds(half * ROWS, ROWS)
        parts.append(exact(spread, jnp.concatenate([first[rows], second[rows]], axis=1)))
    found = []
    for lanes in (slice(0, 128), slice(128, 256)):
        for head in range(2):
            keep = slice(head * HALF, (head + 1) * HALF)
            found.append(jnp.concatenate([part[keep, lanes] for part in parts], axis=0))
    return found


def position():
    index = lax.axis_index("sp")
    return index // SIDE, lax.rem(index, SIDE), lax.rem(lax.axis_index("tp"), 2)


def prepare_kernel(
    q_hbm, k_hbm, v_hbm, maps_hbm, lse_hbm, out_hbm, gain_hbm, lam_hbm,
    yown, zown, send1, send2, send3,
    q_in, k_in, v_in, maps_in, lse_in, out_in, gain_in, lam, sems,
):
    z, _, _ = position()
    pairs = [
        (maps_hbm, maps_in), (out_hbm, out_in), (gain_hbm, gain_in), (lse_hbm, lse_in),
        (lam_hbm, lam), (q_hbm, q_in), (k_hbm, k_in), (v_hbm, v_in),
    ]
    copies = [pltpu.make_async_copy(a, b, sems.at[n]) for n, (a, b) in enumerate(pairs)]
    for copy in copies:
        copy.start()
    row = iota((ROWS, ROWS), 0)
    col = iota((ROWS, ROWS), 1)
    spread = one_hot(col == 2 * (row % HALF) + row // HALF)
    deal = one_hot(col == 4 * (row % DH) + row // DH)
    for copy in copies[:5]:
        copy.wait()
    left = exact(deal, jnp.concatenate([maps_in[0:256], maps_in[256:512]], axis=1))
    right = exact(deal, jnp.concatenate([maps_in[512:768], maps_in[768:1024]], axis=1))

    def map_rows(which, head):
        rows = slice((which * 2 + head) * DH, (which * 2 + head + 1) * DH)
        return jnp.concatenate(
            [left[rows, 0:128], left[rows, 128:], right[rows, 0:128], right[rows, 128:]], axis=0
        )

    outs = []
    for half in range(2):
        outs.append(exact(spread, out_in[half * ROWS : (half + 1) * ROWS]))
    gain = gain_in[...]
    for head, ref in ((1, yown), (0, zown)):
        first = map_rows(0, head)
        second = map_rows(1, head)
        rows = slice(head * HALF, (head + 1) * HALF)
        cotangent = jnp.concatenate([outs[0][rows], outs[1][rows]], axis=0)
        combined = first - lam[head] * second
        inverse = lax.rsqrt(jnp.mean(combined * combined, axis=-1, keepdims=True) + EPSILON)
        weighted = gain * cotangent
        dot = jnp.mean(combined * weighted, axis=-1, keepdims=True)
        grad = (inverse * weighted - inverse * inverse * inverse * combined * dot).astype(BF)
        wide = grad.astype(F32)
        term1 = jnp.sum((wide * first).T, axis=0, keepdims=True)
        term2 = jnp.sum((wide * second).T, axis=0, keepdims=True)
        lse = lse_in[head]
        table = jnp.concatenate([lse[0:1], lse[1:2], term1, term2], axis=0)
        high = table.astype(BF).astype(F32)
        middle = (table - high).astype(BF).astype(F32)
        low = table - high - middle
        packed = jnp.concatenate([high, middle, low, jnp.zeros_like(table)], axis=0).astype(BF)
        ref[ROWS : 2 * ROWS] = grad
        ref[2 * ROWS : 2 * ROWS + 16] = packed[:, 0:128]
        ref[2 * ROWS + 16 : QG] = packed[:, 128:256]
    for copy in copies[5:]:
        copy.wait()
    q0, q1, k0, k1 = two_heads(spread, q_in, k_in)
    v0, v1, _, _ = two_heads(spread, v_in, v_in)
    yown[0:ROWS] = q1.astype(BF)
    yown[QG : QG + ROWS] = k0.astype(BF)
    yown[QG + ROWS : SLOT] = v0.astype(BF)
    zown[0:ROWS] = q0.astype(BF)
    zown[QG : QG + ROWS] = k1.astype(BF)
    zown[QG + ROWS : SLOT] = v1.astype(BF)

    def send(ref, keys):
        @pl.when(keys)
        def _():
            ref[0 : 2 * ROWS] = zown[QG:SLOT]
            ref[2 * ROWS : QG] = jnp.zeros((STAT_ROWS, 128), BF)

        @pl.when(jnp.logical_not(keys))
        def _():
            ref[...] = zown[0:QG]

    for n, ref in enumerate((send1, send2, send3)):
        send(ref, z < jnp.bitwise_xor(z, n + 1))


def fetch_kernel(lat_hbm, lat_own, lat_near, lat_far, sems):
    z, _, core = position()

    def columns(block):
        return pl.ds(pl.multiple_of(block * WIDE, WIDE), WIDE)

    tokens = pl.ds(pl.multiple_of(core * HALF, HALF), HALF)
    near = jnp.bitwise_xor(z, jnp.where(core == 0, 1, 3))
    copies = (
        pltpu.make_async_copy(lat_hbm.at[:, columns(near)], lat_near, sems.at[0]),
        pltpu.make_async_copy(lat_hbm.at[tokens, columns(jnp.bitwise_xor(z, 2))], lat_far, sems.at[1]),
        pltpu.make_async_copy(lat_hbm.at[:, columns(z)], lat_own, sems.at[2]),
    )
    for copy in copies:
        copy.start()
    for copy in copies:
        copy.wait()


def attend_kernel(
    lam, yown, y1, y2, y3, zown, z1, z2, z3,
    q1, q2, q3, r1, r2, r3, kv1, kv2, kv3, own_q, own_k, own_v,
    buf, stat, kpad, kturn, qpad, dq, dk, dv, wide_w, tall_s,
):
    z, y, _ = position()
    for slot, ref in enumerate((yown, y1, y2, y3, zown)):
        buf[slot] = ref[...]
    keys_of = [(jnp.bitwise_xor(z, n) < z).astype(jnp.int32) for n in range(1, SIDE)]
    for slot, (ref, keys) in enumerate(zip((z1, z2, z3), keys_of)):
        @pl.when(keys == 1)
        def _():
            buf[SIDE + 1 + slot, QG:SLOT] = ref[0 : 2 * ROWS]

        @pl.when(keys == 0)
        def _():
            buf[SIDE + 1 + slot, 0:QG] = ref[...]

    row = iota((128, 128), 0)
    col = iota((128, 128), 1)
    eye_first = one_hot(jnp.logical_and(row == col, row < DH))
    eye_second = one_hot(jnp.logical_and(row == col, row >= DH))

    def ready(slot, carry):
        lane = iota((ROWS, 128), 1)
        q = buf[slot, 0:ROWS]
        k = buf[slot, QG : QG + ROWS]
        zero = jnp.zeros_like(q)
        qpad[slot, 0:ROWS] = jnp.where(lane < DH, q, zero)
        qpad[slot, ROWS:] = jnp.where(lane < DH, zero, q)
        kpad[slot, 0:ROWS] = jnp.where(lane < DH, k, zero)
        kpad[slot, ROWS:] = jnp.where(lane < DH, zero, k)
        kturn[slot, :, 0:ROWS] = turned(eye_first, k).astype(BF)
        kturn[slot, :, ROWS:] = turned(eye_second, k).astype(BF)
        left = buf[slot, 2 * ROWS : 2 * ROWS + 16].astype(F32)
        right = buf[slot, 2 * ROWS + 16 : QG].astype(F32)
        pieces = jnp.concatenate([left, right], axis=1)
        rows = pieces[0:4] + pieces[4:8] + pieces[8:12]
        stat[slot, 0:2] = rows[0:2] * LOG2E
        stat[slot, 2:4] = rows[2:4]
        dq[slot] = jnp.zeros((128, ROWS), F32)
        dk[slot] = jnp.zeros((ROWS, 128), F32)
        dv[slot] = jnp.zeros((ROWS, 128), F32)
        return carry

    lax.fori_loop(0, 2 * SIDE, ready, 0)

    def slots_of(item):
        own = item < SIDE + 1
        rest = item - SIDE - 1
        zslot = jnp.where(own, SIDE, SIDE + 1 + rest // SIDE)
        yslot = jnp.where(own, jnp.maximum(item - 1, 0), lax.rem(jnp.maximum(rest, 0), SIDE))
        behind = jnp.where(yslot == 0, item == 0, jnp.bitwise_xor(y, yslot) < y)
        other = (jnp.bitwise_xor(z, zslot - SIDE) < z).astype(jnp.int32)
        kind = jnp.where(own, 1 - behind.astype(jnp.int32), other)
        qs = jnp.where(kind == 0, zslot, yslot)
        ks = jnp.where(kind == 0, yslot, zslot)
        return qs, ks, kind

    def front(item):
        qs, ks, kind = slots_of(item)
        shift = jnp.where(item < 2, 0, 2 * ROWS)
        factor = lam[kind]
        q = buf[qs, 0:ROWS]
        g = buf[qs, ROWS : 2 * ROWS]
        v = buf[ks, QG + ROWS : SLOT]
        rows = stat[qs]
        scores = lax.dot_general(kpad[ks], q, NT, preferred_element_type=F32)
        mixed = lax.dot_general(v, g, NT, preferred_element_type=F32)
        scale = DH ** (-0.5) * LOG2E
        power1 = scores[0:ROWS] * scale - rows[0:1]
        power2 = scores[ROWS:] * scale - rows[1:2]
        seen = iota((ROWS, ROWS), 0) <= iota((ROWS, ROWS), 1) + shift
        gone = jnp.full((ROWS, ROWS), -1e30, F32)
        prob1 = jnp.exp2(jnp.where(seen, power1, gone))
        prob2 = factor * jnp.exp2(jnp.where(seen, power2, gone))
        weights = (prob1 - prob2).astype(BF)
        score1 = (prob1 * (mixed - rows[2:3])).astype(BF)
        score2 = (prob2 * (rows[3:4] - mixed)).astype(BF)
        return weights, score1, score2

    def keep(values):
        weights, score1, score2 = values
        wide_w[...] = weights
        tall_s[0:ROWS] = score1
        tall_s[ROWS:] = score2

    def back(item):
        qs, ks, _ = slots_of(item)
        weights = wide_w[...]
        score1 = tall_s[0:ROWS]
        score2 = tall_s[ROWS:]
        g = buf[qs, ROWS : 2 * ROWS]
        add_v = exact(weights, g)
        add_k = exact(jnp.concatenate([score1, score2], axis=1), qpad[qs])
        add_q = exact(kturn[ks], jnp.concatenate([score1, score2], axis=0))
        return qs, ks, add_q, add_k, add_v

    def add(sums):
        qs, ks, add_q, add_k, add_v = sums
        dv[ks] += add_v
        dk[ks] += add_k
        dq[qs] += add_q

    items = SIDE * SIDE + 1
    keep(front(0))

    def step(item, carry):
        sums = back(item)
        values = front(item + 1)
        add(sums)
        keep(values)
        return carry

    lax.fori_loop(0, items - 1, step, 0)
    add(back(items - 1))

    scale = DH ** (-0.5)

    def put_q(ref, slot):
        value = (dq[slot] * scale).astype(BF)
        ref[0:HALF] = value[:, 0:128]
        ref[HALF:ROWS] = value[:, 128:]

    for slot, (ref, kv) in enumerate(((q1, kv1), (q2, kv2), (q3, kv3))):
        put_q(ref, slot + 1)
        kv[0:ROWS] = (dk[slot + 1] * scale).astype(BF)
        kv[ROWS:] = dv[slot + 1].astype(BF)
    for slot, (ref, keys) in enumerate(zip((r1, r2, r3), keys_of)):
        @pl.when(keys == 1)
        def _():
            ref[0:ROWS] = (dk[SIDE + 1 + slot] * scale).astype(BF)
            ref[ROWS:] = dv[SIDE + 1 + slot].astype(BF)

        @pl.when(keys == 0)
        def _():
            put_q(ref, SIDE + 1 + slot)
            ref[ROWS:] = jnp.zeros((ROWS, 128), BF)

    own_q[0] = dq[SIDE] * scale
    own_q[1] = dq[0] * scale
    own_k[0] = dk[0] * scale
    own_k[1] = dk[SIDE] * scale
    own_v[0] = dv[0]
    own_v[1] = dv[SIDE]


def queries_kernel(own_q, y1, y2, y3, z1, z2, z3, turned_out, acc):
    z, _, _ = position()

    def lanes(ref):
        return jnp.concatenate([ref[0:HALF].astype(F32), ref[HALF:ROWS].astype(F32)], axis=1)

    acc[...] = own_q[0]
    for n, ref in enumerate((z1, z2, z3)):
        keys = z < jnp.bitwise_xor(z, n + 1)

        @pl.when(jnp.logical_not(keys))
        def _():
            acc[...] += lanes(ref)

    turned_out[0:128] = acc[...].astype(BF)
    turned_out[128:256] = (own_q[1] + lanes(y1) + lanes(y2) + lanes(y3)).astype(BF)


def keys_kernel(
    own_k, own_v, y1, y2, y3, z1, z2, z3, turned_in, q_out, k_out, v_out, acc_k, acc_v
):
    z, _, _ = position()
    acc_k[...] = own_k[1]
    acc_v[...] = own_v[1]
    for n, ref in enumerate((z1, z2, z3)):
        keys = z < jnp.bitwise_xor(z, n + 1)

        @pl.when(keys)
        def _():
            acc_k[...] += ref[0:ROWS].astype(F32)
            acc_v[...] += ref[ROWS:].astype(F32)

    row = iota((ROWS, ROWS), 0)
    col = iota((ROWS, ROWS), 1)
    weave = one_hot(col == row % 2 * HALF + row // 2)
    k0 = own_k[0]
    v0 = own_v[0]
    for ref in (y1, y2, y3):
        k0 += ref[0:ROWS].astype(F32)
        v0 += ref[ROWS:].astype(F32)
    zero = jnp.concatenate([k0.astype(BF), v0.astype(BF)], axis=1)
    one = jnp.concatenate([acc_k[...].astype(BF), acc_v[...].astype(BF)], axis=1)
    for half in range(2):
        keep = slice(half * HALF, (half + 1) * HALF)
        rows = slice(half * ROWS, (half + 1) * ROWS)
        woven = exact(weave, jnp.concatenate([zero[keep], one[keep]], axis=0)).astype(BF)
        k_out[rows] = woven[:, 0:128]
        v_out[rows] = woven[:, 128:256]
        both = jnp.concatenate([turned_in[0:128, keep], turned_in[128:256, keep]], axis=1)
        q_out[rows] = turned(weave, both).astype(BF)


def project_kernel(
    g0, g1, g2, g3, lat0, near, near_swap, far, far_swap, own, to1, to2, to3, lat
):
    _, y, core = position()
    lat[0:ROWS] = lat0[...]
    first = slice(ROWS, 2 * ROWS)
    second = slice(2 * ROWS, 2 * ROWS + HALF)
    third = slice(2 * ROWS + HALF, 3 * ROWS)
    fourth = slice(3 * ROWS, 4 * ROWS)

    @pl.when(core == 0)
    def _():
        lat[first] = near[...]
        lat[second] = far[...]
        lat[third] = far_swap[...]
        lat[fourth] = near_swap[...]

    @pl.when(core == 1)
    def _():
        lat[first] = near_swap[...]
        lat[second] = far_swap[...]
        lat[third] = far[...]
        lat[fourth] = near[...]

    grads = jnp.concatenate([g0[...], g1[...], g2[...], g3[...]], axis=1)
    for n, ref in ((1, to1), (2, to2), (3, to3), (0, own)):
        columns = pl.ds(pl.multiple_of(jnp.bitwise_xor(y, n) * ROWS, ROWS), ROWS)
        ref[...] = exact(grads, lat[:, columns]).astype(ref.dtype)


def total_kernel(own, t1, t2, t3, out):
    whole = own[...] + t1[...].astype(F32) + t2[...].astype(F32) + t3[...].astype(F32)
    out[...] = whole.T


def traded(x, axis, n):
    step = n * (SIDE if axis == "z" else 1)
    return lax.ppermute(x, "sp", [(s, s ^ step) for s in range(SIDE * SIDE)])


def traded_apart(x):
    heads = lax.axis_size("tp")
    pairs = []
    for s in range(SIDE * SIDE):
        for t in range(heads):
            there = s ^ (SIDE * (1 if t % 2 == 0 else 3))
            pairs.append((s * heads + t, there * heads + t))
    return lax.ppermute(x, ("sp", "tp"), pairs)


def partner(x):
    return lax.ppermute(x, "tp", [(t, t ^ 1) for t in range(lax.axis_size("tp"))])


def shape(*dims, dtype=BF):
    return jax.ShapeDtypeStruct(dims, dtype)


def call(kernel, outs, scalars, hbm, vmem, scratch, flops, mib=16):
    calling = pl.pallas_call(
        kernel,
        out_shape=outs,
        in_specs=[pl.BlockSpec(memory_space=pltpu.SMEM)] * scalars
        + [pl.BlockSpec(memory_space=pltpu.HBM)] * hbm
        + [pl.BlockSpec(memory_space=pltpu.VMEM)] * vmem,
        out_specs=jax.tree.map(lambda _: pl.BlockSpec(memory_space=pltpu.VMEM), outs),
        scratch_shapes=scratch,
        compiler_params=pltpu.CompilerParams(vmem_limit_bytes=mib * 2**20),
        cost_estimate=pl.CostEstimate(flops=flops, bytes_accessed=10**6, transcendentals=0),
    )

    def run(*arrays):
        held = [
            pltpu.with_memory_space_constraint(x, pltpu.HBM)
            for x in arrays[scalars : scalars + hbm]
        ]
        return calling(*arrays[:scalars], *held, *arrays[scalars + hbm :])

    return run


def body(
    latents,
    query_heads,
    key_heads,
    value_heads,
    map_outputs,
    log_sums,
    out_grad,
    mix_lambda,
    norm_gain,
):
    yown, zown, *sends = call(
        prepare_kernel,
        (shape(SLOT, 128),) * 2 + (shape(QG, 128),) * 3,
        0,
        8,
        0,
        [pltpu.VMEM((2 * ROWS, 128), BF)] * 3
        + [
            pltpu.VMEM((4 * ROWS, 128), BF),
            pltpu.VMEM((2, 2, ROWS), F32),
            pltpu.VMEM((2 * ROWS, 128), BF),
            pltpu.VMEM((1, 128), F32),
            pltpu.SMEM((2,), F32),
            pltpu.SemaphoreType.DMA((8,)),
        ],
        10**8,
    )(
        query_heads.reshape(2 * ROWS, 128),
        key_heads.reshape(2 * ROWS, 128),
        value_heads.reshape(2 * ROWS, 128),
        map_outputs.reshape(4 * ROWS, 128),
        jnp.transpose(log_sums, (1, 2, 0)),
        out_grad.reshape(2 * ROWS, 128),
        norm_gain.reshape(1, 128),
        mix_lambda,
    )
    ys = [traded(yown, "y", n) for n in range(1, SIDE)]
    zs = [traded(x, "z", n) for n, x in enumerate(sends, 1)]
    lat_own, lat_near, lat_far = call(
        fetch_kernel,
        (shape(ROWS, WIDE), shape(ROWS, WIDE), shape(HALF, WIDE)),
        0,
        1,
        0,
        [pltpu.SemaphoreType.DMA((3,))],
        10**7,
        1,
    )(latents)
    near = traded_apart(lat_near)
    apart = traded(lat_far, "z", 2)
    near_swap = partner(near)
    apart_swap = partner(apart)

    slots = 2 * SIDE
    small = shape(ROWS, 128)
    both = shape(2 * ROWS, 128)
    results = call(
        attend_kernel,
        (small,) * 3
        + (both,) * 6
        + (shape(2, 128, ROWS, dtype=F32),)
        + (shape(2, ROWS, 128, dtype=F32),) * 2,
        1,
        0,
        8,
        [
            pltpu.VMEM((slots, SLOT, 128), BF),
            pltpu.VMEM((slots, 8, ROWS), F32),
            pltpu.VMEM((slots, 2 * ROWS, 128), BF),
            pltpu.VMEM((slots, 128, 2 * ROWS), BF),
            pltpu.VMEM((slots, 2 * ROWS, 128), BF),
            pltpu.VMEM((slots, 128, ROWS), F32),
            pltpu.VMEM((slots, ROWS, 128), F32),
            pltpu.VMEM((slots, ROWS, 128), F32),
            pltpu.VMEM((ROWS, ROWS), BF),
            pltpu.VMEM((2 * ROWS, ROWS), BF),
        ],
        17 * 10 * ROWS * ROWS * 128,
        24,
    )(mix_lambda, yown, *ys, zown, *zs)
    own_q, own_k, own_v = results[9:12]
    q_back = [traded(x, "y", n) for n, x in enumerate(results[0:3], 1)]
    z_back = [traded(x, "z", n) for n, x in enumerate(results[3:6], 1)]
    turned_grad = call(
        queries_kernel, shape(ROWS, ROWS), 0, 0, 7, [pltpu.VMEM((128, ROWS), F32)], 10**7
    )(own_q, *q_back, *z_back)
    grads = [traded(turned_grad, "z", n) for n in range(1, SIDE)]
    kv_back = [traded(x, "y", n) for n, x in enumerate(results[6:9], 1)]
    square = shape(ROWS, ROWS)
    own, *parts = call(
        project_kernel,
        (shape(ROWS, ROWS, dtype=F32), square, square, square),
        0,
        0,
        9,
        [pltpu.VMEM((WIDE, WIDE), BF)],
        2 * WIDE * WIDE * ROWS,
    )(turned_grad, *grads, lat_own, near, near_swap, apart, apart_swap)
    query_rows, key_rows, value_rows = call(
        keys_kernel, (shape(2 * ROWS, 128),) * 3, 0, 0, 9, [pltpu.VMEM((ROWS, 128), F32)] * 2, 10**7
    )(own_k, own_v, *kv_back, *z_back, turned_grad)
    weight_grad = call(
        total_kernel, shape(ROWS, ROWS, dtype=F32), 0, 0, 4, [], 10**6
    )(own, *[traded(x, "y", n) for n, x in enumerate(parts, 1)])
    whole = (ROWS, 2, 128)
    return (
        query_rows.reshape(whole),
        key_rows.reshape(whole),
        value_rows.reshape(whole),
        weight_grad,
    )


def solution(mesh):
    placed = (
        P("sp", None),
        P("sp", "tp", None),
        P("sp", "tp", None),
        P("sp", "tp", None),
        P("sp", None, "tp", None),
        P("sp", "tp", None),
        P("sp", "tp", None),
        P("tp"),
        P(),
    )
    return jax.shard_map(
        body,
        mesh=mesh,
        in_specs=placed,
        out_specs=(P("sp", "tp", None), P("sp", "tp", None), P("sp", "tp", None), P("sp", "tp")),
        check_vma=False,
    )
```

```python
import jax
import jax.numpy as jnp
from jax import lax
from jax.experimental import pallas as pl
from jax.experimental.pallas import tpu as pltpu
from jax.sharding import PartitionSpec as P


DH = 64
EPSILON = 1e-05
SIDE = 4
ROWS = 256
HALF = ROWS // 2
WIDE = 1024
STAT_ROWS = 32
QG = 2 * ROWS + STAT_ROWS
SLOT = QG + 2 * ROWS
LOG2E = 1.4426950408889634
NT = (((1,), (1,)), ((), ()))
BF = jnp.bfloat16
F32 = jnp.float32


def iota(shape, dim):
    return lax.broadcasted_iota(jnp.int32, shape, dim)


def one_hot(hit):
    return jnp.where(hit, 1.0, 0.0).astype(BF)


def exact(a, b):
    return jnp.dot(a, b, preferred_element_type=F32)


def turned(eye, x):
    return lax.dot_general(eye, x, NT, preferred_element_type=F32)


def two_heads(spread, first, second):
    parts = []
    for half in range(2):
        rows = pl.ds(half * ROWS, ROWS)
        parts.append(exact(spread, jnp.concatenate([first[rows], second[rows]], axis=1)))
    found = []
    for lanes in (slice(0, 128), slice(128, 256)):
        for head in range(2):
            keep = slice(head * HALF, (head + 1) * HALF)
            found.append(jnp.concatenate([part[keep, lanes] for part in parts], axis=0))
    return found


def position():
    index = lax.axis_index("sp")
    return index // SIDE, lax.rem(index, SIDE), lax.rem(lax.axis_index("tp"), 2)


def prepare_kernel(
    q_hbm, k_hbm, v_hbm, maps_hbm, lse_hbm, out_hbm, gain_hbm, lam_hbm,
    yown, zown, send1, send2, send3,
    q_in, k_in, v_in, maps_in, lse_in, out_in, gain_in, lam, sems,
):
    z, _, _ = position()
    pairs = [
        (maps_hbm, maps_in), (out_hbm, out_in), (gain_hbm, gain_in), (lse_hbm, lse_in),
        (lam_hbm, lam), (q_hbm, q_in), (k_hbm, k_in), (v_hbm, v_in),
    ]
    copies = [pltpu.make_async_copy(a, b, sems.at[n]) for n, (a, b) in enumerate(pairs)]
    for copy in copies:
        copy.start()
    row = iota((ROWS, ROWS), 0)
    col = iota((ROWS, ROWS), 1)
    spread = one_hot(col == 2 * (row % HALF) + row // HALF)
    deal = one_hot(col == 4 * (row % DH) + row // DH)
    for copy in copies[:5]:
        copy.wait()
    left = exact(deal, jnp.concatenate([maps_in[0:256], maps_in[256:512]], axis=1))
    right = exact(deal, jnp.concatenate([maps_in[512:768], maps_in[768:1024]], axis=1))

    def map_rows(which, head):
        rows = slice((which * 2 + head) * DH, (which * 2 + head + 1) * DH)
        return jnp.concatenate(
            [left[rows, 0:128], left[rows, 128:], right[rows, 0:128], right[rows, 128:]], axis=0
        )

    outs = []
    for half in range(2):
        outs.append(exact(spread, out_in[half * ROWS : (half + 1) * ROWS]))
    gain = gain_in[...]
    for head, ref in ((1, yown), (0, zown)):
        first = map_rows(0, head)
        second = map_rows(1, head)
        rows = slice(head * HALF, (head + 1) * HALF)
        cotangent = jnp.concatenate([outs[0][rows], outs[1][rows]], axis=0)
        combined = first - lam[head] * second
        inverse = lax.rsqrt(jnp.mean(combined * combined, axis=-1, keepdims=True) + EPSILON)
        weighted = gain * cotangent
        dot = jnp.mean(combined * weighted, axis=-1, keepdims=True)
        grad = (inverse * weighted - inverse * inverse * inverse * combined * dot).astype(BF)
        wide = grad.astype(F32)
        term1 = jnp.sum((wide * first).T, axis=0, keepdims=True)
        term2 = jnp.sum((wide * second).T, axis=0, keepdims=True)
        lse = lse_in[head]
        table = jnp.concatenate([lse[0:1], lse[1:2], term1, term2], axis=0)
        high = table.astype(BF).astype(F32)
        middle = (table - high).astype(BF).astype(F32)
        low = table - high - middle
        packed = jnp.concatenate([high, middle, low, jnp.zeros_like(table)], axis=0).astype(BF)
        ref[ROWS : 2 * ROWS] = grad
        ref[2 * ROWS : 2 * ROWS + 16] = packed[:, 0:128]
        ref[2 * ROWS + 16 : QG] = packed[:, 128:256]
    for copy in copies[5:]:
        copy.wait()
    q0, q1, k0, k1 = two_heads(spread, q_in, k_in)
    v0, v1, _, _ = two_heads(spread, v_in, v_in)
    yown[0:ROWS] = q1.astype(BF)
    yown[QG : QG + ROWS] = k0.astype(BF)
    yown[QG + ROWS : SLOT] = v0.astype(BF)
    zown[0:ROWS] = q0.astype(BF)
    zown[QG : QG + ROWS] = k1.astype(BF)
    zown[QG + ROWS : SLOT] = v1.astype(BF)

    def send(ref, keys):
        @pl.when(keys)
        def _():
            ref[0 : 2 * ROWS] = zown[QG:SLOT]
            ref[2 * ROWS : QG] = jnp.zeros((STAT_ROWS, 128), BF)

        @pl.when(jnp.logical_not(keys))
        def _():
            ref[...] = zown[0:QG]

    for n, ref in enumerate((send1, send2, send3)):
        send(ref, z < jnp.bitwise_xor(z, n + 1))


def fetch_kernel(lat_hbm, lat_own, lat_near, lat_far, sems):
    z, _, core = position()

    def columns(block):
        return pl.ds(pl.multiple_of(block * WIDE, WIDE), WIDE)

    tokens = pl.ds(pl.multiple_of(core * HALF, HALF), HALF)
    near = jnp.bitwise_xor(z, jnp.where(core == 0, 1, 3))
    copies = (
        pltpu.make_async_copy(lat_hbm.at[:, columns(near)], lat_near, sems.at[0]),
        pltpu.make_async_copy(lat_hbm.at[tokens, columns(jnp.bitwise_xor(z, 2))], lat_far, sems.at[1]),
        pltpu.make_async_copy(lat_hbm.at[:, columns(z)], lat_own, sems.at[2]),
    )
    for copy in copies:
        copy.start()
    for copy in copies:
        copy.wait()


def ready(slot, buf, stat, kpad, kturn, qpad, dq, dk, dv):
    row = iota((128, 128), 0)
    col = iota((128, 128), 1)
    lane = iota((ROWS, 128), 1)
    q = buf[slot, 0:ROWS]
    k = buf[slot, QG : QG + ROWS]
    zero = jnp.zeros_like(q)
    qpad[slot, 0:ROWS] = jnp.where(lane < DH, q, zero)
    qpad[slot, ROWS:] = jnp.where(lane < DH, zero, q)
    kpad[slot, 0:ROWS] = jnp.where(lane < DH, k, zero)
    kpad[slot, ROWS:] = jnp.where(lane < DH, zero, k)
    eye_first = one_hot(jnp.logical_and(row == col, row < DH))
    eye_second = one_hot(jnp.logical_and(row == col, row >= DH))
    kturn[slot, :, 0:ROWS] = turned(eye_first, k).astype(BF)
    kturn[slot, :, ROWS:] = turned(eye_second, k).astype(BF)
    left = buf[slot, 2 * ROWS : 2 * ROWS + 16].astype(F32)
    right = buf[slot, 2 * ROWS + 16 : QG].astype(F32)
    pieces = jnp.concatenate([left, right], axis=1)
    rows = pieces[0:4] + pieces[4:8] + pieces[8:12]
    stat[slot, 0:2] = rows[0:2] * LOG2E
    stat[slot, 2:4] = rows[2:4]
    dq[slot] = jnp.zeros((128, ROWS), F32)
    dk[slot] = jnp.zeros((ROWS, 128), F32)
    dv[slot] = jnp.zeros((ROWS, 128), F32)


def take(z, n, ref, buf):
    keys = jnp.bitwise_xor(z, n) < z

    @pl.when(keys)
    def _():
        buf[SIDE + n, QG:SLOT] = ref[0 : 2 * ROWS]

    @pl.when(jnp.logical_not(keys))
    def _():
        buf[SIDE + n, 0:QG] = ref[...]


def run_pairs(items, z, y, lam, state, wide_w, tall_s):
    buf, stat, kpad, kturn, qpad, dq, dk, dv = state

    def slots_of(item):
        zslot, yslot, kind = item
        if kind is None:
            if zslot == SIDE:
                kind = 1 - (jnp.bitwise_xor(y, yslot) < y).astype(jnp.int32)
            else:
                kind = (jnp.bitwise_xor(z, zslot - SIDE) < z).astype(jnp.int32)
            qs = jnp.where(kind == 0, zslot, yslot)
            return qs, zslot + yslot - qs, kind
        return (zslot, yslot, kind) if kind == 0 else (yslot, zslot, kind)

    slots = [slots_of(item) for item in items]

    def dots(n):
        qs, ks, _ = slots[n]
        q = buf[qs, 0:ROWS]
        g = buf[qs, ROWS : 2 * ROWS]
        v = buf[ks, QG + ROWS : SLOT]
        scores = lax.dot_general(kpad[ks], q, NT, preferred_element_type=F32)
        mixed = lax.dot_general(v, g, NT, preferred_element_type=F32)
        return scores, mixed

    def front(n, started):
        scores, mixed = started
        qs, _, kind = slots[n]
        factor = lam[kind]
        rows = stat[qs]
        scale = DH ** (-0.5) * LOG2E
        power1 = scores[0:ROWS] * scale - rows[0:1]
        power2 = scores[ROWS:] * scale - rows[1:2]
        if items[n][2] is not None:
            seen = iota((ROWS, ROWS), 0) <= iota((ROWS, ROWS), 1)
            gone = jnp.full((ROWS, ROWS), -1e30, F32)
            power1 = jnp.where(seen, power1, gone)
            power2 = jnp.where(seen, power2, gone)
        prob1 = jnp.exp2(power1)
        prob2 = factor * jnp.exp2(power2)
        hold = n % 2
        wide_w[hold] = (prob1 - prob2).astype(BF)
        tall_s[hold, 0:ROWS] = (prob1 * (mixed - rows[2:3])).astype(BF)
        tall_s[hold, ROWS:] = (prob2 * (rows[3:4] - mixed)).astype(BF)

    def back(n):
        qs, ks, _ = slots[n]
        hold = n % 2
        weights = wide_w[hold]
        score1 = tall_s[hold, 0:ROWS]
        score2 = tall_s[hold, ROWS:]
        g = buf[qs, ROWS : 2 * ROWS]
        add_v = exact(weights, g)
        add_k = exact(jnp.concatenate([score1, score2], axis=1), qpad[qs])
        add_q = exact(kturn[ks], tall_s[hold])
        return add_q, add_k, add_v

    front(0, dots(0))
    for n in range(len(items)):
        more = n + 1 < len(items)
        if more:
            started = dots(n + 1)
        add_q, add_k, add_v = back(n)
        if more:
            front(n + 1, started)
        qs, ks, _ = slots[n]
        dv[ks] += add_v
        dk[ks] += add_k
        dq[qs] += add_q


def attend_near_kernel(
    lam, yown, y1, y3, zown, z1, z3,
    buf, stat, kpad, kturn, qpad, dq, dk, dv, wide_w, tall_s,
):
    z, y, _ = position()
    state = (buf, stat, kpad, kturn, qpad, dq, dk, dv)
    for slot, ref in ((0, yown), (1, y1), (3, y3), (SIDE, zown)):
        buf[slot] = ref[...]
    take(z, 1, z1, buf)
    take(z, 3, z3, buf)
    for slot in (0, 1, 3, 4, 5, 7):
        ready(slot, *state)
    items = [(4, 0, 0), (4, 0, 1)]
    items += [(4, 1, None), (4, 3, None)]
    items += [(zslot, yslot, None) for zslot in (5, 7) for yslot in (0, 1, 3)]
    run_pairs(items, z, y, lam, state, wide_w, tall_s)


def attend_far_kernel(
    lam, y2, z2, buf_in, stat_in, kpad_in, kturn_in, qpad_in, dq_in, dk_in, dv_in,
    q1, q2, q3, r1, r2, r3, kv1, kv2, kv3, own_q, own_k, own_v,
    buf, stat, kpad, kturn, qpad, dq, dk, dv, wide_w, tall_s,
):
    z, y, _ = position()
    state = (buf, stat, kpad, kturn, qpad, dq, dk, dv)
    buf[2] = y2[...]
    take(z, 2, z2, buf)
    for slot in (2, 6):
        ready(slot, *state)
    items = [(zslot, 2, None) for zslot in (4, 5, 7)]
    items += [(6, yslot, None) for yslot in range(SIDE)]
    run_pairs(items, z, y, lam, state, wide_w, tall_s)
    scale = DH ** (-0.5)

    def put_q(ref, slot):
        value = (dq[slot] * scale).astype(BF)
        ref[0:HALF] = value[:, 0:128]
        ref[HALF:ROWS] = value[:, 128:]

    for slot, (ref, kv) in enumerate(((q1, kv1), (q2, kv2), (q3, kv3))):
        put_q(ref, slot + 1)
        kv[0:ROWS] = (dk[slot + 1] * scale).astype(BF)
        kv[ROWS:] = dv[slot + 1].astype(BF)
    for n, ref in enumerate((r1, r2, r3), 1):
        keys = jnp.bitwise_xor(z, n) < z

        @pl.when(keys)
        def _():
            ref[0:ROWS] = (dk[SIDE + n] * scale).astype(BF)
            ref[ROWS:] = dv[SIDE + n].astype(BF)

        @pl.when(jnp.logical_not(keys))
        def _():
            put_q(ref, SIDE + n)
            ref[ROWS:] = jnp.zeros((ROWS, 128), BF)

    own_q[0] = dq[SIDE] * scale
    own_q[1] = dq[0] * scale
    own_k[0] = dk[0] * scale
    own_k[1] = dk[SIDE] * scale
    own_v[0] = dv[0]
    own_v[1] = dv[SIDE]


def queries_kernel(own_q, y1, y2, y3, z1, z2, z3, turned_out, acc):
    z, _, _ = position()

    def lanes(ref):
        return jnp.concatenate([ref[0:HALF].astype(F32), ref[HALF:ROWS].astype(F32)], axis=1)

    acc[...] = own_q[0]
    for n, ref in enumerate((z1, z2, z3)):
        keys = z < jnp.bitwise_xor(z, n + 1)

        @pl.when(jnp.logical_not(keys))
        def _():
            acc[...] += lanes(ref)

    turned_out[0:128] = acc[...].astype(BF)
    turned_out[128:256] = (own_q[1] + lanes(y1) + lanes(y2) + lanes(y3)).astype(BF)


def keys_kernel(
    own_k, own_v, y1, y2, y3, z1, z2, z3, turned_in, q_out, k_out, v_out, acc_k, acc_v
):
    z, _, _ = position()
    acc_k[...] = own_k[1]
    acc_v[...] = own_v[1]
    for n, ref in enumerate((z1, z2, z3)):
        keys = z < jnp.bitwise_xor(z, n + 1)

        @pl.when(keys)
        def _():
            acc_k[...] += ref[0:ROWS].astype(F32)
            acc_v[...] += ref[ROWS:].astype(F32)

    row = iota((ROWS, ROWS), 0)
    col = iota((ROWS, ROWS), 1)
    weave = one_hot(col == row % 2 * HALF + row // 2)
    k0 = own_k[0]
    v0 = own_v[0]
    for ref in (y1, y2, y3):
        k0 += ref[0:ROWS].astype(F32)
        v0 += ref[ROWS:].astype(F32)
    zero = jnp.concatenate([k0.astype(BF), v0.astype(BF)], axis=1)
    one = jnp.concatenate([acc_k[...].astype(BF), acc_v[...].astype(BF)], axis=1)
    for half in range(2):
        keep = slice(half * HALF, (half + 1) * HALF)
        rows = slice(half * ROWS, (half + 1) * ROWS)
        woven = exact(weave, jnp.concatenate([zero[keep], one[keep]], axis=0)).astype(BF)
        k_out[rows] = woven[:, 0:128]
        v_out[rows] = woven[:, 128:256]
        both = jnp.concatenate([turned_in[0:128, keep], turned_in[128:256, keep]], axis=1)
        q_out[rows] = turned(weave, both).astype(BF)


def project_kernel(
    g0, g1, g2, g3, lat0, near, near_swap, far, far_swap, own, to1, to2, to3, lat
):
    _, y, core = position()
    lat[0:ROWS] = lat0[...]
    first = slice(ROWS, 2 * ROWS)
    second = slice(2 * ROWS, 2 * ROWS + HALF)
    third = slice(2 * ROWS + HALF, 3 * ROWS)
    fourth = slice(3 * ROWS, 4 * ROWS)

    @pl.when(core == 0)
    def _():
        lat[first] = near[...]
        lat[second] = far[...]
        lat[third] = far_swap[...]
        lat[fourth] = near_swap[...]

    @pl.when(core == 1)
    def _():
        lat[first] = near_swap[...]
        lat[second] = far_swap[...]
        lat[third] = far[...]
        lat[fourth] = near[...]

    grads = jnp.concatenate([g0[...], g1[...], g2[...], g3[...]], axis=1)
    for n, ref in ((1, to1), (2, to2), (3, to3), (0, own)):
        columns = pl.ds(pl.multiple_of(jnp.bitwise_xor(y, n) * ROWS, ROWS), ROWS)
        ref[...] = exact(grads, lat[:, columns]).astype(ref.dtype)


def total_kernel(own, t1, t2, t3, out):
    whole = own[...] + t1[...].astype(F32) + t2[...].astype(F32) + t3[...].astype(F32)
    out[...] = whole.T


def traded(x, axis, n):
    step = n * (SIDE if axis == "z" else 1)
    return lax.ppermute(x, "sp", [(s, s ^ step) for s in range(SIDE * SIDE)])


def traded_apart(x):
    heads = lax.axis_size("tp")
    pairs = []
    for s in range(SIDE * SIDE):
        for t in range(heads):
            there = s ^ (SIDE * (1 if t % 2 == 0 else 3))
            pairs.append((s * heads + t, there * heads + t))
    return lax.ppermute(x, ("sp", "tp"), pairs)


def partner(x):
    return lax.ppermute(x, "tp", [(t, t ^ 1) for t in range(lax.axis_size("tp"))])


def shape(*dims, dtype=BF):
    return jax.ShapeDtypeStruct(dims, dtype)


def call(kernel, outs, scalars, hbm, vmem, scratch, flops, mib=16, aliases=None):
    calling = pl.pallas_call(
        kernel,
        out_shape=outs,
        in_specs=[pl.BlockSpec(memory_space=pltpu.SMEM)] * scalars
        + [pl.BlockSpec(memory_space=pltpu.HBM)] * hbm
        + [pl.BlockSpec(memory_space=pltpu.VMEM)] * vmem,
        out_specs=jax.tree.map(lambda _: pl.BlockSpec(memory_space=pltpu.VMEM), outs),
        scratch_shapes=scratch,
        input_output_aliases=aliases or {},
        compiler_params=pltpu.CompilerParams(vmem_limit_bytes=mib * 2**20),
        cost_estimate=pl.CostEstimate(flops=flops, bytes_accessed=10**6, transcendentals=0),
    )

    def run(*arrays):
        held = [
            pltpu.with_memory_space_constraint(x, pltpu.HBM)
            for x in arrays[scalars : scalars + hbm]
        ]
        rest = arrays[scalars + hbm :]
        if aliases:
            rest = [pltpu.with_memory_space_constraint(x, pltpu.VMEM) for x in rest]
        return calling(*arrays[:scalars], *held, *rest)

    return run


def body(
    latents,
    query_heads,
    key_heads,
    value_heads,
    map_outputs,
    log_sums,
    out_grad,
    mix_lambda,
    norm_gain,
):
    yown, zown, *sends = call(
        prepare_kernel,
        (shape(SLOT, 128),) * 2 + (shape(QG, 128),) * 3,
        0,
        8,
        0,
        [pltpu.VMEM((2 * ROWS, 128), BF)] * 3
        + [
            pltpu.VMEM((4 * ROWS, 128), BF),
            pltpu.VMEM((2, 2, ROWS), F32),
            pltpu.VMEM((2 * ROWS, 128), BF),
            pltpu.VMEM((1, 128), F32),
            pltpu.SMEM((2,), F32),
            pltpu.SemaphoreType.DMA((8,)),
        ],
        10**8,
    )(
        query_heads.reshape(2 * ROWS, 128),
        key_heads.reshape(2 * ROWS, 128),
        value_heads.reshape(2 * ROWS, 128),
        map_outputs.reshape(4 * ROWS, 128),
        jnp.transpose(log_sums, (1, 2, 0)),
        out_grad.reshape(2 * ROWS, 128),
        norm_gain.reshape(1, 128),
        mix_lambda,
    )
    ys = [traded(yown, "y", n) for n in range(1, SIDE)]
    zs = [traded(x, "z", n) for n, x in enumerate(sends, 1)]
    lat_own, lat_near, lat_far = call(
        fetch_kernel,
        (shape(ROWS, WIDE), shape(ROWS, WIDE), shape(HALF, WIDE)),
        0,
        1,
        0,
        [pltpu.SemaphoreType.DMA((3,))],
        10**7,
        1,
    )(latents)
    near = traded_apart(lat_near)
    apart = traded(lat_far, "z", 2)
    near_swap = partner(near)
    apart_swap = partner(apart)

    slots = 2 * SIDE
    small = shape(ROWS, 128)
    both = shape(2 * ROWS, 128)
    state_shapes = (
        shape(slots, SLOT, 128),
        shape(slots, 8, ROWS, dtype=F32),
        shape(slots, 2 * ROWS, 128),
        shape(slots, 128, 2 * ROWS),
        shape(slots, 2 * ROWS, 128),
        shape(slots, 128, ROWS, dtype=F32),
        shape(slots, ROWS, 128, dtype=F32),
        shape(slots, ROWS, 128, dtype=F32),
    )
    holds = [pltpu.VMEM((2, ROWS, ROWS), BF), pltpu.VMEM((2, 2 * ROWS, ROWS), BF)]
    pair_flops = 10 * ROWS * ROWS * 128
    state = call(
        attend_near_kernel, state_shapes, 1, 0, 6, holds, 10 * pair_flops
    )(mix_lambda, yown, ys[0], ys[2], zown, zs[0], zs[2])
    result_shapes = (
        (small,) * 3
        + (both,) * 6
        + (shape(2, 128, ROWS, dtype=F32),)
        + (shape(2, ROWS, 128, dtype=F32),) * 2
    )
    results = call(
        attend_far_kernel,
        result_shapes + state_shapes,
        1,
        0,
        10,
        holds,
        7 * pair_flops,
        aliases={3 + n: len(result_shapes) + n for n in range(len(state_shapes))},
    )(mix_lambda, ys[1], zs[1], *state)
    own_q, own_k, own_v = results[9:12]
    q_back = [traded(x, "y", n) for n, x in enumerate(results[0:3], 1)]
    z_back = [traded(x, "z", n) for n, x in enumerate(results[3:6], 1)]
    turned_grad = call(
        queries_kernel,
        shape(ROWS, ROWS),
        0,
        0,
        7,
        [pltpu.VMEM((128, ROWS), F32)],
        10**7,
    )(own_q, *q_back, *z_back)
    grads = [traded(turned_grad, "z", n) for n in range(1, SIDE)]
    kv_back = [traded(x, "y", n) for n, x in enumerate(results[6:9], 1)]
    square = shape(ROWS, ROWS)
    own, *parts = call(
        project_kernel,
        (shape(ROWS, ROWS, dtype=F32), square, square, square),
        0,
        0,
        9,
        [pltpu.VMEM((WIDE, WIDE), BF)],
        2 * WIDE * WIDE * ROWS,
    )(turned_grad, *grads, lat_own, near, near_swap, apart, apart_swap)
    query_rows, key_rows, value_rows = call(
        keys_kernel,
        (shape(2 * ROWS, 128),) * 3,
        0,
        0,
        9,
        [pltpu.VMEM((ROWS, 128), F32)] * 2,
        10**7,
    )(own_k, own_v, *kv_back, *z_back, turned_grad)
    weight_grad = call(
        total_kernel, shape(ROWS, ROWS, dtype=F32), 0, 0, 4, [], 10**6
    )(own, *[traded(x, "y", n) for n, x in enumerate(parts, 1)])
    whole = (ROWS, 2, 128)
    return (
        query_rows.reshape(whole),
        key_rows.reshape(whole),
        value_rows.reshape(whole),
        weight_grad,
    )


def solution(mesh):
    placed = (
        P("sp", None),
        P("sp", "tp", None),
        P("sp", "tp", None),
        P("sp", "tp", None),
        P("sp", None, "tp", None),
        P("sp", "tp", None),
        P("sp", "tp", None),
        P("tp"),
        P(),
    )
    return jax.shard_map(
        body,
        mesh=mesh,
        in_specs=placed,
        out_specs=(P("sp", "tp", None), P("sp", "tp", None), P("sp", "tp", None), P("sp", "tp")),
        check_vma=False,
    )
```

```python
import jax
import jax.numpy as jnp
from jax import lax
from jax.experimental import pallas as pl
from jax.experimental.pallas import tpu as pltpu
from jax.sharding import PartitionSpec as P


DH = 64
EPSILON = 1e-05
SIDE = 4
ROWS = 256
HALF = ROWS // 2
WIDE = 1024
STAT_ROWS = 32
QG = 2 * ROWS + STAT_ROWS
SLOT = QG + 2 * ROWS
LOG2E = 1.4426950408889634
NT = (((1,), (1,)), ((), ()))
BF = jnp.bfloat16
F32 = jnp.float32


def iota(shape, dim):
    return lax.broadcasted_iota(jnp.int32, shape, dim)


def one_hot(hit):
    return jnp.where(hit, 1.0, 0.0).astype(BF)


def exact(a, b):
    return jnp.dot(a, b, preferred_element_type=F32)


def turned(eye, x):
    return lax.dot_general(eye, x, NT, preferred_element_type=F32)


def two_heads(spread, first, second):
    parts = []
    for half in range(2):
        rows = pl.ds(half * ROWS, ROWS)
        parts.append(exact(spread, jnp.concatenate([first[rows], second[rows]], axis=1)))
    found = []
    for lanes in (slice(0, 128), slice(128, 256)):
        for head in range(2):
            keep = slice(head * HALF, (head + 1) * HALF)
            found.append(jnp.concatenate([part[keep, lanes] for part in parts], axis=0))
    return found


def position():
    index = lax.axis_index("sp")
    return index // SIDE, lax.rem(index, SIDE), lax.rem(lax.axis_index("tp"), 2)


def prepare_kernel(
    q_hbm, k_hbm, v_hbm, maps_hbm, lse_hbm, out_hbm, gain_hbm, lam_hbm, lat_hbm,
    yown, zown, send1, send2, send3, lat_near, lat_far,
    q_in, k_in, v_in, maps_in, lse_in, out_in, gain_in, lam, sems,
):
    z, _, core = position()
    pairs = [
        (maps_hbm, maps_in), (out_hbm, out_in), (gain_hbm, gain_in), (lse_hbm, lse_in),
        (lam_hbm, lam), (q_hbm, q_in), (k_hbm, k_in), (v_hbm, v_in),
    ]
    near = jnp.bitwise_xor(z, jnp.where(core == 0, 1, 3))
    columns = pl.ds(pl.multiple_of(near * WIDE, WIDE), WIDE)
    pairs.append((lat_hbm.at[:, columns], lat_near))
    tokens = pl.ds(pl.multiple_of(core * HALF, HALF), HALF)
    columns = pl.ds(pl.multiple_of(jnp.bitwise_xor(z, 2) * WIDE, WIDE), WIDE)
    pairs.append((lat_hbm.at[tokens, columns], lat_far))
    copies = [pltpu.make_async_copy(a, b, sems.at[n]) for n, (a, b) in enumerate(pairs)]
    for copy in copies:
        copy.start()
    row = iota((ROWS, ROWS), 0)
    col = iota((ROWS, ROWS), 1)
    spread = one_hot(col == 2 * (row % HALF) + row // HALF)
    deal = one_hot(col == 4 * (row % DH) + row // DH)
    for copy in copies[:5]:
        copy.wait()
    left = exact(deal, jnp.concatenate([maps_in[0:256], maps_in[256:512]], axis=1))
    right = exact(deal, jnp.concatenate([maps_in[512:768], maps_in[768:1024]], axis=1))

    def map_rows(which, head):
        rows = slice((which * 2 + head) * DH, (which * 2 + head + 1) * DH)
        return jnp.concatenate(
            [left[rows, 0:128], left[rows, 128:], right[rows, 0:128], right[rows, 128:]], axis=0
        )

    outs = []
    for half in range(2):
        outs.append(exact(spread, out_in[half * ROWS : (half + 1) * ROWS]))
    gain = gain_in[...]
    for head, ref in ((1, yown), (0, zown)):
        first = map_rows(0, head)
        second = map_rows(1, head)
        rows = slice(head * HALF, (head + 1) * HALF)
        cotangent = jnp.concatenate([outs[0][rows], outs[1][rows]], axis=0)
        combined = first - lam[head] * second
        inverse = lax.rsqrt(jnp.mean(combined * combined, axis=-1, keepdims=True) + EPSILON)
        weighted = gain * cotangent
        dot = jnp.mean(combined * weighted, axis=-1, keepdims=True)
        grad = (inverse * weighted - inverse * inverse * inverse * combined * dot).astype(BF)
        wide = grad.astype(F32)
        term1 = jnp.sum((wide * first).T, axis=0, keepdims=True)
        term2 = jnp.sum((wide * second).T, axis=0, keepdims=True)
        lse = lse_in[head]
        table = jnp.concatenate([lse[0:1], lse[1:2], term1, term2], axis=0)
        high = table.astype(BF).astype(F32)
        middle = (table - high).astype(BF).astype(F32)
        low = table - high - middle
        packed = jnp.concatenate([high, middle, low, jnp.zeros_like(table)], axis=0).astype(BF)
        ref[ROWS : 2 * ROWS] = grad
        ref[2 * ROWS : 2 * ROWS + 16] = packed[:, 0:128]
        ref[2 * ROWS + 16 : QG] = packed[:, 128:256]
    for copy in copies[5:8]:
        copy.wait()
    q0, q1, k0, k1 = two_heads(spread, q_in, k_in)
    v0, v1, _, _ = two_heads(spread, v_in, v_in)
    yown[0:ROWS] = q1.astype(BF)
    yown[QG : QG + ROWS] = k0.astype(BF)
    yown[QG + ROWS : SLOT] = v0.astype(BF)
    zown[0:ROWS] = q0.astype(BF)
    zown[QG : QG + ROWS] = k1.astype(BF)
    zown[QG + ROWS : SLOT] = v1.astype(BF)

    def send(ref, keys):
        @pl.when(keys)
        def _():
            ref[0 : 2 * ROWS] = zown[QG:SLOT]
            ref[2 * ROWS : QG] = jnp.zeros((STAT_ROWS, 128), BF)

        @pl.when(jnp.logical_not(keys))
        def _():
            ref[...] = zown[0:QG]

    for n, ref in enumerate((send1, send2, send3)):
        send(ref, z < jnp.bitwise_xor(z, n + 1))
    for copy in copies[8:]:
        copy.wait()


def ready(slot, buf, stat, kpad, kturn, qpad, dq, dk, dv):
    row = iota((128, 128), 0)
    col = iota((128, 128), 1)
    lane = iota((ROWS, 128), 1)
    q = buf[slot, 0:ROWS]
    k = buf[slot, QG : QG + ROWS]
    zero = jnp.zeros_like(q)
    qpad[slot, 0:ROWS] = jnp.where(lane < DH, q, zero)
    qpad[slot, ROWS:] = jnp.where(lane < DH, zero, q)
    kpad[slot, 0:ROWS] = jnp.where(lane < DH, k, zero)
    kpad[slot, ROWS:] = jnp.where(lane < DH, zero, k)
    eye_first = one_hot(jnp.logical_and(row == col, row < DH))
    eye_second = one_hot(jnp.logical_and(row == col, row >= DH))
    kturn[slot, :, 0:ROWS] = turned(eye_first, k).astype(BF)
    kturn[slot, :, ROWS:] = turned(eye_second, k).astype(BF)
    left = buf[slot, 2 * ROWS : 2 * ROWS + 16].astype(F32)
    right = buf[slot, 2 * ROWS + 16 : QG].astype(F32)
    pieces = jnp.concatenate([left, right], axis=1)
    rows = pieces[0:4] + pieces[4:8] + pieces[8:12]
    stat[slot, 0:2] = rows[0:2] * LOG2E
    stat[slot, 2:4] = rows[2:4]
    dq[slot] = jnp.zeros((128, ROWS), F32)
    dk[slot] = jnp.zeros((ROWS, 128), F32)
    dv[slot] = jnp.zeros((ROWS, 128), F32)


def take(z, n, ref, buf):
    keys = jnp.bitwise_xor(z, n) < z

    @pl.when(keys)
    def _():
        buf[SIDE + n, QG:SLOT] = ref[0 : 2 * ROWS]

    @pl.when(jnp.logical_not(keys))
    def _():
        buf[SIDE + n, 0:QG] = ref[...]


def run_pairs(items, z, y, lam, state, wide_w, tall_s):
    buf, stat, kpad, kturn, qpad, dq, dk, dv = state

    def slots_of(item):
        zslot, yslot, kind = item
        if kind is None:
            if zslot == SIDE:
                kind = 1 - (jnp.bitwise_xor(y, yslot) < y).astype(jnp.int32)
            else:
                kind = (jnp.bitwise_xor(z, zslot - SIDE) < z).astype(jnp.int32)
            qs = jnp.where(kind == 0, zslot, yslot)
            return qs, zslot + yslot - qs, kind
        return (zslot, yslot, kind) if kind == 0 else (yslot, zslot, kind)

    slots = [slots_of(item) for item in items]

    def dots(n):
        qs, ks, _ = slots[n]
        q = buf[qs, 0:ROWS]
        g = buf[qs, ROWS : 2 * ROWS]
        v = buf[ks, QG + ROWS : SLOT]
        scores = lax.dot_general(kpad[ks], q, NT, preferred_element_type=F32)
        mixed = lax.dot_general(v, g, NT, preferred_element_type=F32)
        return scores, mixed

    def front(n, started):
        scores, mixed = started
        qs, _, kind = slots[n]
        factor = lam[kind]
        rows = stat[qs]
        scale = DH ** (-0.5) * LOG2E
        power1 = scores[0:ROWS] * scale - rows[0:1]
        power2 = scores[ROWS:] * scale - rows[1:2]
        if items[n][2] is not None:
            seen = iota((ROWS, ROWS), 0) <= iota((ROWS, ROWS), 1)
            gone = jnp.full((ROWS, ROWS), -1e30, F32)
            power1 = jnp.where(seen, power1, gone)
            power2 = jnp.where(seen, power2, gone)
        prob1 = jnp.exp2(power1)
        prob2 = factor * jnp.exp2(power2)
        hold = n % 2
        wide_w[hold] = (prob1 - prob2).astype(BF)
        tall_s[hold, 0:ROWS] = (prob1 * (mixed - rows[2:3])).astype(BF)
        tall_s[hold, ROWS:] = (prob2 * (rows[3:4] - mixed)).astype(BF)

    def back(n):
        qs, ks, _ = slots[n]
        hold = n % 2
        weights = wide_w[hold]
        score1 = tall_s[hold, 0:ROWS]
        score2 = tall_s[hold, ROWS:]
        g = buf[qs, ROWS : 2 * ROWS]
        add_v = exact(weights, g)
        add_k = exact(jnp.concatenate([score1, score2], axis=1), qpad[qs])
        add_q = exact(kturn[ks], tall_s[hold])
        return add_q, add_k, add_v

    front(0, dots(0))
    for n in range(len(items)):
        more = n + 1 < len(items)
        if more:
            started = dots(n + 1)
        add_q, add_k, add_v = back(n)
        if more:
            front(n + 1, started)
        qs, ks, _ = slots[n]
        dv[ks] += add_v
        dk[ks] += add_k
        dq[qs] += add_q


def attend_near_kernel(
    lam, lat_hbm, yown, y1, y3, zown, z1, z3,
    buf, stat, kpad, kturn, qpad, dq, dk, dv, lat_own, wide_w, tall_s, sem,
):
    z, y, _ = position()
    columns = pl.ds(pl.multiple_of(z * WIDE, WIDE), WIDE)
    fetch = pltpu.make_async_copy(lat_hbm.at[:, columns], lat_own, sem)
    fetch.start()
    state = (buf, stat, kpad, kturn, qpad, dq, dk, dv)
    for slot, ref in ((0, yown), (1, y1), (3, y3), (SIDE, zown)):
        buf[slot] = ref[...]
    take(z, 1, z1, buf)
    take(z, 3, z3, buf)
    for slot in (0, 1, 3, 4, 5, 7):
        ready(slot, *state)
    items = [(4, 0, 0), (4, 0, 1)]
    items += [(4, 1, None), (4, 3, None)]
    items += [(zslot, yslot, None) for zslot in (5, 7) for yslot in (0, 1, 3)]
    run_pairs(items, z, y, lam, state, wide_w, tall_s)
    fetch.wait()


def attend_far_kernel(
    lam, y2, z2, buf_in, stat_in, kpad_in, kturn_in, qpad_in, dq_in, dk_in, dv_in,
    g1, g2, g3, r1, r2, r3, own_q, own_k, own_v,
    buf, stat, kpad, kturn, qpad, dq, dk, dv, wide_w, tall_s,
):
    z, y, _ = position()
    state = (buf, stat, kpad, kturn, qpad, dq, dk, dv)
    buf[2] = y2[...]
    take(z, 2, z2, buf)
    for slot in (2, 6):
        ready(slot, *state)
    items = [(zslot, 2, None) for zslot in (4, 5, 7)]
    items += [(6, yslot, None) for yslot in range(SIDE)]
    run_pairs(items, z, y, lam, state, wide_w, tall_s)
    scale = DH ** (-0.5)

    def put_q(ref, slot):
        value = (dq[slot] * scale).astype(BF)
        ref[0:HALF] = value[:, 0:128]
        ref[HALF:ROWS] = value[:, 128:]

    for slot, ref in enumerate((g1, g2, g3), 1):
        put_q(ref, slot)
        ref[ROWS : 2 * ROWS] = (dk[slot] * scale).astype(BF)
        ref[2 * ROWS :] = dv[slot].astype(BF)
    for n, ref in enumerate((r1, r2, r3), 1):
        keys = jnp.bitwise_xor(z, n) < z

        @pl.when(keys)
        def _():
            ref[0:ROWS] = (dk[SIDE + n] * scale).astype(BF)
            ref[ROWS:] = dv[SIDE + n].astype(BF)

        @pl.when(jnp.logical_not(keys))
        def _():
            put_q(ref, SIDE + n)
            ref[ROWS:] = jnp.zeros((ROWS, 128), BF)

    own_q[0] = dq[SIDE] * scale
    own_q[1] = dq[0] * scale
    own_k[0] = dk[0] * scale
    own_k[1] = dk[SIDE] * scale
    own_v[0] = dv[0]
    own_v[1] = dv[SIDE]


def queries_kernel(own_q, y1, y2, y3, z1, z2, z3, turned_out, acc):
    z, _, _ = position()

    def lanes(ref):
        return jnp.concatenate([ref[0:HALF].astype(F32), ref[HALF:ROWS].astype(F32)], axis=1)

    acc[...] = own_q[0]
    for n, ref in enumerate((z1, z2, z3)):
        keys = z < jnp.bitwise_xor(z, n + 1)

        @pl.when(jnp.logical_not(keys))
        def _():
            acc[...] += lanes(ref)

    turned_out[0:128] = acc[...].astype(BF)
    turned_out[128:256] = (own_q[1] + lanes(y1) + lanes(y2) + lanes(y3)).astype(BF)


def keys_kernel(
    own_k, own_v, y1, y2, y3, z1, z2, z3, turned_in, q_out, k_out, v_out, acc_k, acc_v
):
    z, _, _ = position()
    acc_k[...] = own_k[1]
    acc_v[...] = own_v[1]
    for n, ref in enumerate((z1, z2, z3)):
        keys = z < jnp.bitwise_xor(z, n + 1)

        @pl.when(keys)
        def _():
            acc_k[...] += ref[0:ROWS].astype(F32)
            acc_v[...] += ref[ROWS:].astype(F32)

    row = iota((ROWS, ROWS), 0)
    col = iota((ROWS, ROWS), 1)
    weave = one_hot(col == row % 2 * HALF + row // 2)
    k0 = own_k[0]
    v0 = own_v[0]
    for ref in (y1, y2, y3):
        k0 += ref[ROWS : 2 * ROWS].astype(F32)
        v0 += ref[2 * ROWS :].astype(F32)
    zero = jnp.concatenate([k0.astype(BF), v0.astype(BF)], axis=1)
    one = jnp.concatenate([acc_k[...].astype(BF), acc_v[...].astype(BF)], axis=1)
    for half in range(2):
        keep = slice(half * HALF, (half + 1) * HALF)
        rows = slice(half * ROWS, (half + 1) * ROWS)
        woven = exact(weave, jnp.concatenate([zero[keep], one[keep]], axis=0)).astype(BF)
        k_out[rows] = woven[:, 0:128]
        v_out[rows] = woven[:, 128:256]
        both = jnp.concatenate([turned_in[0:128, keep], turned_in[128:256, keep]], axis=1)
        q_out[rows] = turned(weave, both).astype(BF)


def project_kernel(
    g0, g1, g2, g3, lat0, near, near_swap, far, far_swap, own, to1, to2, to3, lat
):
    _, y, core = position()
    lat[0:ROWS] = lat0[...]
    first = slice(ROWS, 2 * ROWS)
    second = slice(2 * ROWS, 2 * ROWS + HALF)
    third = slice(2 * ROWS + HALF, 3 * ROWS)
    fourth = slice(3 * ROWS, 4 * ROWS)

    @pl.when(core == 0)
    def _():
        lat[first] = near[...]
        lat[second] = far[...]
        lat[third] = far_swap[...]
        lat[fourth] = near_swap[...]

    @pl.when(core == 1)
    def _():
        lat[first] = near_swap[...]
        lat[second] = far_swap[...]
        lat[third] = far[...]
        lat[fourth] = near[...]

    grads = jnp.concatenate([g0[...], g1[...], g2[...], g3[...]], axis=1)
    for n, ref in ((1, to1), (2, to2), (3, to3), (0, own)):
        columns = pl.ds(pl.multiple_of(jnp.bitwise_xor(y, n) * ROWS, ROWS), ROWS)
        ref[...] = exact(grads, lat[:, columns]).astype(ref.dtype)


def total_kernel(own, t1, t2, t3, out):
    whole = own[...] + t1[...].astype(F32) + t2[...].astype(F32) + t3[...].astype(F32)
    out[...] = whole.T


def traded(x, axis, n):
    step = n * (SIDE if axis == "z" else 1)
    return lax.ppermute(x, "sp", [(s, s ^ step) for s in range(SIDE * SIDE)])


def traded_apart(x):
    heads = lax.axis_size("tp")
    pairs = []
    for s in range(SIDE * SIDE):
        for t in range(heads):
            there = s ^ (SIDE * (1 if t % 2 == 0 else 3))
            pairs.append((s * heads + t, there * heads + t))
    return lax.ppermute(x, ("sp", "tp"), pairs)


def partner(x):
    return lax.ppermute(x, "tp", [(t, t ^ 1) for t in range(lax.axis_size("tp"))])


def shape(*dims, dtype=BF):
    return jax.ShapeDtypeStruct(dims, dtype)


def call(kernel, outs, scalars, hbm, vmem, scratch, flops, mib=16, aliases=None):
    calling = pl.pallas_call(
        kernel,
        out_shape=outs,
        in_specs=[pl.BlockSpec(memory_space=pltpu.SMEM)] * scalars
        + [pl.BlockSpec(memory_space=pltpu.HBM)] * hbm
        + [pl.BlockSpec(memory_space=pltpu.VMEM)] * vmem,
        out_specs=jax.tree.map(lambda _: pl.BlockSpec(memory_space=pltpu.VMEM), outs),
        scratch_shapes=scratch,
        input_output_aliases=aliases or {},
        compiler_params=pltpu.CompilerParams(vmem_limit_bytes=mib * 2**20),
        cost_estimate=pl.CostEstimate(flops=flops, bytes_accessed=10**6, transcendentals=0),
    )

    def run(*arrays):
        held = [
            pltpu.with_memory_space_constraint(x, pltpu.HBM)
            for x in arrays[scalars : scalars + hbm]
        ]
        rest = arrays[scalars + hbm :]
        if aliases:
            rest = [pltpu.with_memory_space_constraint(x, pltpu.VMEM) for x in rest]
        return calling(*arrays[:scalars], *held, *rest)

    return run


def body(
    latents,
    query_heads,
    key_heads,
    value_heads,
    map_outputs,
    log_sums,
    out_grad,
    mix_lambda,
    norm_gain,
):
    yown, zown, *sends, lat_near, lat_far = call(
        prepare_kernel,
        (shape(SLOT, 128),) * 2
        + (shape(QG, 128),) * 3
        + (shape(ROWS, WIDE), shape(HALF, WIDE)),
        0,
        9,
        0,
        [pltpu.VMEM((2 * ROWS, 128), BF)] * 3
        + [
            pltpu.VMEM((4 * ROWS, 128), BF),
            pltpu.VMEM((2, 2, ROWS), F32),
            pltpu.VMEM((2 * ROWS, 128), BF),
            pltpu.VMEM((1, 128), F32),
            pltpu.SMEM((2,), F32),
            pltpu.SemaphoreType.DMA((10,)),
        ],
        10**8,
    )(
        query_heads.reshape(2 * ROWS, 128),
        key_heads.reshape(2 * ROWS, 128),
        value_heads.reshape(2 * ROWS, 128),
        map_outputs.reshape(4 * ROWS, 128),
        jnp.transpose(log_sums, (1, 2, 0)),
        out_grad.reshape(2 * ROWS, 128),
        norm_gain.reshape(1, 128),
        mix_lambda,
        latents,
    )
    ys = [traded(yown, "y", n) for n in range(1, SIDE)]
    zs = [traded(x, "z", n) for n, x in enumerate(sends, 1)]
    near = traded_apart(lat_near)
    apart = traded(lat_far, "z", 2)
    near_swap = partner(near)
    apart_swap = partner(apart)

    slots = 2 * SIDE
    state_shapes = (
        shape(slots, SLOT, 128),
        shape(slots, 8, ROWS, dtype=F32),
        shape(slots, 2 * ROWS, 128),
        shape(slots, 128, 2 * ROWS),
        shape(slots, 2 * ROWS, 128),
        shape(slots, 128, ROWS, dtype=F32),
        shape(slots, ROWS, 128, dtype=F32),
        shape(slots, ROWS, 128, dtype=F32),
    )
    holds = [pltpu.VMEM((2, ROWS, ROWS), BF), pltpu.VMEM((2, 2 * ROWS, ROWS), BF)]
    pair_flops = 10 * ROWS * ROWS * 128
    *state, lat_own = call(
        attend_near_kernel,
        state_shapes + (shape(ROWS, WIDE),),
        1,
        1,
        6,
        holds + [pltpu.SemaphoreType.DMA],
        10 * pair_flops,
    )(mix_lambda, latents, yown, ys[0], ys[2], zown, zs[0], zs[2])
    result_shapes = (
        (shape(3 * ROWS, 128),) * 3
        + (shape(2 * ROWS, 128),) * 3
        + (shape(2, 128, ROWS, dtype=F32),)
        + (shape(2, ROWS, 128, dtype=F32),) * 2
    )
    results = call(
        attend_far_kernel,
        result_shapes + state_shapes,
        1,
        0,
        10,
        holds,
        7 * pair_flops,
        aliases={3 + n: len(result_shapes) + n for n in range(len(state_shapes))},
    )(mix_lambda, ys[1], zs[1], *state)
    own_q, own_k, own_v = results[6:9]
    y_back = [traded(x, "y", n) for n, x in enumerate(results[0:3], 1)]
    z_back = [traded(x, "z", n) for n, x in enumerate(results[3:6], 1)]
    turned_grad = call(
        queries_kernel,
        shape(ROWS, ROWS),
        0,
        0,
        7,
        [pltpu.VMEM((128, ROWS), F32)],
        10**7,
    )(own_q, *y_back, *z_back)
    grads = [traded(turned_grad, "z", n) for n in range(1, SIDE)]
    square = shape(ROWS, ROWS)
    own, *parts = call(
        project_kernel,
        (shape(ROWS, ROWS, dtype=F32), square, square, square),
        0,
        0,
        9,
        [pltpu.VMEM((WIDE, WIDE), BF)],
        2 * WIDE * WIDE * ROWS,
    )(turned_grad, *grads, lat_own, near, near_swap, apart, apart_swap)
    query_rows, key_rows, value_rows = call(
        keys_kernel,
        (shape(2 * ROWS, 128),) * 3,
        0,
        0,
        9,
        [pltpu.VMEM((ROWS, 128), F32)] * 2,
        10**7,
    )(own_k, own_v, *y_back, *z_back, turned_grad)
    weight_grad = call(
        total_kernel, shape(ROWS, ROWS, dtype=F32), 0, 0, 4, [], 10**6
    )(own, *[traded(x, "y", n) for n, x in enumerate(parts, 1)])
    whole = (ROWS, 2, 128)
    return (
        query_rows.reshape(whole),
        key_rows.reshape(whole),
        value_rows.reshape(whole),
        weight_grad,
    )


def solution(mesh):
    placed = (
        P("sp", None),
        P("sp", "tp", None),
        P("sp", "tp", None),
        P("sp", "tp", None),
        P("sp", None, "tp", None),
        P("sp", "tp", None),
        P("sp", "tp", None),
        P("tp"),
        P(),
    )
    return jax.shard_map(
        body,
        mesh=mesh,
        in_specs=placed,
        out_specs=(P("sp", "tp", None), P("sp", "tp", None), P("sp", "tp", None), P("sp", "tp")),
        check_vma=False,
    )
```

```python
import jax
import jax.numpy as jnp
from jax import lax
from jax.experimental import pallas as pl
from jax.experimental.pallas import tpu as pltpu
from jax.sharding import PartitionSpec as P


DH = 64
EPSILON = 1e-05
SIDE = 4
ROWS = 256
HALF = ROWS // 2
WIDE = 1024
STAT_ROWS = 32
QG = 2 * ROWS + STAT_ROWS
SLOT = QG + 2 * ROWS
LOG2E = 1.4426950408889634
NT = (((1,), (1,)), ((), ()))
BF = jnp.bfloat16
F32 = jnp.float32


def iota(shape, dim):
    return lax.broadcasted_iota(jnp.int32, shape, dim)


def one_hot(hit):
    return jnp.where(hit, 1.0, 0.0).astype(BF)


def exact(a, b):
    return jnp.dot(a, b, preferred_element_type=F32)


def turned(eye, x):
    return lax.dot_general(eye, x, NT, preferred_element_type=F32)


def two_heads(spread, first, second):
    parts = []
    for half in range(2):
        rows = pl.ds(half * ROWS, ROWS)
        parts.append(exact(spread, jnp.concatenate([first[rows], second[rows]], axis=1)))
    found = []
    for lanes in (slice(0, 128), slice(128, 256)):
        for head in range(2):
            keep = slice(head * HALF, (head + 1) * HALF)
            found.append(jnp.concatenate([part[keep, lanes] for part in parts], axis=0))
    return found


def position():
    index = lax.axis_index("sp")
    return index // SIDE, lax.rem(index, SIDE), lax.rem(lax.axis_index("tp"), 2)


def side():
    return lax.rem(lax.axis_index("tp") // 2, 2)


def prepare_kernel(
    q_hbm, k_hbm, v_hbm, maps_hbm, lse_hbm, out_hbm, gain_hbm, lam_hbm, lat_hbm,
    yown, zown, send1, send2, send3, lat_near, lat_far,
    q_in, k_in, v_in, maps_in, lse_in, out_in, gain_in, lam, sems,
):
    z, _, core = position()
    pairs = [
        (maps_hbm, maps_in), (out_hbm, out_in), (gain_hbm, gain_in), (lse_hbm, lse_in),
        (lam_hbm, lam), (q_hbm, q_in), (k_hbm, k_in), (v_hbm, v_in),
    ]
    near = jnp.bitwise_xor(z, jnp.where(core == 0, 1, 3))
    columns = pl.ds(pl.multiple_of(near * WIDE, WIDE), WIDE)
    tokens = pl.ds(pl.multiple_of(side() * HALF, HALF), HALF)
    pairs.append((lat_hbm.at[tokens, columns], lat_near))
    columns = pl.ds(pl.multiple_of(jnp.bitwise_xor(z, 2) * WIDE, WIDE), WIDE)
    tokens = pl.ds(pl.multiple_of(core * HALF + side() * DH, DH), DH)
    pairs.append((lat_hbm.at[tokens, columns], lat_far))
    copies = [pltpu.make_async_copy(a, b, sems.at[n]) for n, (a, b) in enumerate(pairs)]
    for copy in copies:
        copy.start()
    row = iota((ROWS, ROWS), 0)
    col = iota((ROWS, ROWS), 1)
    spread = one_hot(col == 2 * (row % HALF) + row // HALF)
    deal = one_hot(col == 4 * (row % DH) + row // DH)
    for copy in copies[:5]:
        copy.wait()
    left = exact(deal, jnp.concatenate([maps_in[0:256], maps_in[256:512]], axis=1))
    right = exact(deal, jnp.concatenate([maps_in[512:768], maps_in[768:1024]], axis=1))

    def map_rows(which, head):
        rows = slice((which * 2 + head) * DH, (which * 2 + head + 1) * DH)
        return jnp.concatenate(
            [left[rows, 0:128], left[rows, 128:], right[rows, 0:128], right[rows, 128:]], axis=0
        )

    outs = []
    for half in range(2):
        outs.append(exact(spread, out_in[half * ROWS : (half + 1) * ROWS]))
    gain = gain_in[...]
    for head, ref in ((1, yown), (0, zown)):
        first = map_rows(0, head)
        second = map_rows(1, head)
        rows = slice(head * HALF, (head + 1) * HALF)
        cotangent = jnp.concatenate([outs[0][rows], outs[1][rows]], axis=0)
        combined = first - lam[head] * second
        inverse = lax.rsqrt(jnp.mean(combined * combined, axis=-1, keepdims=True) + EPSILON)
        weighted = gain * cotangent
        dot = jnp.mean(combined * weighted, axis=-1, keepdims=True)
        grad = (inverse * weighted - inverse * inverse * inverse * combined * dot).astype(BF)
        wide = grad.astype(F32)
        term1 = jnp.sum((wide * first).T, axis=0, keepdims=True)
        term2 = jnp.sum((wide * second).T, axis=0, keepdims=True)
        lse = lse_in[head]
        table = jnp.concatenate([lse[0:1], lse[1:2], term1, term2], axis=0)
        high = table.astype(BF).astype(F32)
        middle = (table - high).astype(BF).astype(F32)
        low = table - high - middle
        packed = jnp.concatenate([high, middle, low, jnp.zeros_like(table)], axis=0).astype(BF)
        ref[ROWS : 2 * ROWS] = grad
        ref[2 * ROWS : 2 * ROWS + 16] = packed[:, 0:128]
        ref[2 * ROWS + 16 : QG] = packed[:, 128:256]
    for copy in copies[5:8]:
        copy.wait()
    q0, q1, k0, k1 = two_heads(spread, q_in, k_in)
    v0, v1, _, _ = two_heads(spread, v_in, v_in)
    yown[0:ROWS] = q1.astype(BF)
    yown[QG : QG + ROWS] = k0.astype(BF)
    yown[QG + ROWS : SLOT] = v0.astype(BF)
    zown[0:ROWS] = q0.astype(BF)
    zown[QG : QG + ROWS] = k1.astype(BF)
    zown[QG + ROWS : SLOT] = v1.astype(BF)

    def send(ref, keys):
        @pl.when(keys)
        def _():
            ref[0 : 2 * ROWS] = zown[QG:SLOT]
            ref[2 * ROWS : QG] = jnp.zeros((STAT_ROWS, 128), BF)

        @pl.when(jnp.logical_not(keys))
        def _():
            ref[...] = zown[0:QG]

    for n, ref in enumerate((send1, send2, send3)):
        send(ref, z < jnp.bitwise_xor(z, n + 1))
    for copy in copies[8:]:
        copy.wait()


def ready(slot, buf, stat, kpad, kturn, qpad, dq, dk, dv):
    row = iota((128, 128), 0)
    col = iota((128, 128), 1)
    lane = iota((ROWS, 128), 1)
    q = buf[slot, 0:ROWS]
    k = buf[slot, QG : QG + ROWS]
    zero = jnp.zeros_like(q)
    qpad[slot, 0:ROWS] = jnp.where(lane < DH, q, zero)
    qpad[slot, ROWS:] = jnp.where(lane < DH, zero, q)
    kpad[slot, 0:ROWS] = jnp.where(lane < DH, k, zero)
    kpad[slot, ROWS:] = jnp.where(lane < DH, zero, k)
    eye_first = one_hot(jnp.logical_and(row == col, row < DH))
    eye_second = one_hot(jnp.logical_and(row == col, row >= DH))
    kturn[slot, :, 0:ROWS] = turned(eye_first, k).astype(BF)
    kturn[slot, :, ROWS:] = turned(eye_second, k).astype(BF)
    left = buf[slot, 2 * ROWS : 2 * ROWS + 16].astype(F32)
    right = buf[slot, 2 * ROWS + 16 : QG].astype(F32)
    pieces = jnp.concatenate([left, right], axis=1)
    rows = pieces[0:4] + pieces[4:8] + pieces[8:12]
    stat[slot, 0:2] = rows[0:2] * LOG2E
    stat[slot, 2:4] = rows[2:4]
    dq[slot] = jnp.zeros((128, ROWS), F32)
    dk[slot] = jnp.zeros((ROWS, 128), F32)
    dv[slot] = jnp.zeros((ROWS, 128), F32)


def take(z, n, ref, buf):
    keys = jnp.bitwise_xor(z, n) < z

    @pl.when(keys)
    def _():
        buf[SIDE + n, QG:SLOT] = ref[0 : 2 * ROWS]

    @pl.when(jnp.logical_not(keys))
    def _():
        buf[SIDE + n, 0:QG] = ref[...]


def run_pairs(items, z, y, lam, state, wide_w, tall_s):
    buf, stat, kpad, kturn, qpad, dq, dk, dv = state

    def slots_of(item):
        zslot, yslot, kind = item
        if kind is None:
            if zslot == SIDE:
                kind = 1 - (jnp.bitwise_xor(y, yslot) < y).astype(jnp.int32)
            else:
                kind = (jnp.bitwise_xor(z, zslot - SIDE) < z).astype(jnp.int32)
            qs = jnp.where(kind == 0, zslot, yslot)
            return qs, zslot + yslot - qs, kind
        return (zslot, yslot, kind) if kind == 0 else (yslot, zslot, kind)

    slots = [slots_of(item) for item in items]

    def dots(n):
        qs, ks, _ = slots[n]
        q = buf[qs, 0:ROWS]
        g = buf[qs, ROWS : 2 * ROWS]
        v = buf[ks, QG + ROWS : SLOT]
        scores = lax.dot_general(kpad[ks], q, NT, preferred_element_type=F32)
        mixed = lax.dot_general(v, g, NT, preferred_element_type=F32)
        return scores, mixed

    def front(n, started):
        scores, mixed = started
        qs, _, kind = slots[n]
        factor = lam[kind]
        rows = stat[qs]
        scale = DH ** (-0.5) * LOG2E
        power1 = scores[0:ROWS] * scale - rows[0:1]
        power2 = scores[ROWS:] * scale - rows[1:2]
        if items[n][2] is not None:
            seen = iota((ROWS, ROWS), 0) <= iota((ROWS, ROWS), 1)
            gone = jnp.full((ROWS, ROWS), -1e30, F32)
            power1 = jnp.where(seen, power1, gone)
            power2 = jnp.where(seen, power2, gone)
        prob1 = jnp.exp2(power1)
        prob2 = factor * jnp.exp2(power2)
        hold = n % 2
        wide_w[hold] = (prob1 - prob2).astype(BF)
        tall_s[hold, 0:ROWS] = (prob1 * (mixed - rows[2:3])).astype(BF)
        tall_s[hold, ROWS:] = (prob2 * (rows[3:4] - mixed)).astype(BF)

    def back(n):
        qs, ks, _ = slots[n]
        hold = n % 2
        weights = wide_w[hold]
        score1 = tall_s[hold, 0:ROWS]
        score2 = tall_s[hold, ROWS:]
        g = buf[qs, ROWS : 2 * ROWS]
        add_v = exact(weights, g)
        add_k = exact(jnp.concatenate([score1, score2], axis=1), qpad[qs])
        add_q = exact(kturn[ks], tall_s[hold])
        return add_q, add_k, add_v

    front(0, dots(0))
    for n in range(len(items)):
        more = n + 1 < len(items)
        if more:
            started = dots(n + 1)
        add_q, add_k, add_v = back(n)
        if more:
            front(n + 1, started)
        qs, ks, _ = slots[n]
        dv[ks] += add_v
        dk[ks] += add_k
        dq[qs] += add_q


def attend_near_kernel(
    lam, lat_hbm, yown, y1, y3, zown, z1, z3,
    buf, stat, kpad, kturn, qpad, dq, dk, dv, lat_own, wide_w, tall_s, sem,
):
    z, y, _ = position()
    columns = pl.ds(pl.multiple_of(z * WIDE, WIDE), WIDE)
    fetch = pltpu.make_async_copy(lat_hbm.at[:, columns], lat_own, sem)
    fetch.start()
    state = (buf, stat, kpad, kturn, qpad, dq, dk, dv)
    for slot, ref in ((0, yown), (1, y1), (3, y3), (SIDE, zown)):
        buf[slot] = ref[...]
    take(z, 1, z1, buf)
    take(z, 3, z3, buf)
    for slot in (0, 1, 3, 4, 5, 7):
        ready(slot, *state)
    items = [(4, 0, 0), (4, 0, 1)]
    items += [(4, 1, None), (4, 3, None)]
    items += [(zslot, yslot, None) for zslot in (5, 7) for yslot in (0, 1, 3)]
    run_pairs(items, z, y, lam, state, wide_w, tall_s)
    fetch.wait()


def attend_far_kernel(
    lam, y2, z2, buf_in, stat_in, kpad_in, kturn_in, qpad_in, dq_in, dk_in, dv_in,
    g1, g2, g3, r1, r2, r3, own_q, own_k, own_v,
    buf, stat, kpad, kturn, qpad, dq, dk, dv, wide_w, tall_s,
):
    z, y, _ = position()
    state = (buf, stat, kpad, kturn, qpad, dq, dk, dv)
    buf[2] = y2[...]
    take(z, 2, z2, buf)
    for slot in (2, 6):
        ready(slot, *state)
    items = [(zslot, 2, None) for zslot in (4, 5, 7)]
    items += [(6, yslot, None) for yslot in range(SIDE)]
    run_pairs(items, z, y, lam, state, wide_w, tall_s)
    scale = DH ** (-0.5)

    def put_q(ref, slot):
        value = (dq[slot] * scale).astype(BF)
        ref[0:HALF] = value[:, 0:128]
        ref[HALF:ROWS] = value[:, 128:]

    for slot, ref in enumerate((g1, g2, g3), 1):
        put_q(ref, slot)
        ref[ROWS : 2 * ROWS] = (dk[slot] * scale).astype(BF)
        ref[2 * ROWS :] = dv[slot].astype(BF)
    for n, ref in enumerate((r1, r2, r3), 1):
        keys = jnp.bitwise_xor(z, n) < z

        @pl.when(keys)
        def _():
            ref[0:ROWS] = (dk[SIDE + n] * scale).astype(BF)
            ref[ROWS:] = dv[SIDE + n].astype(BF)

        @pl.when(jnp.logical_not(keys))
        def _():
            put_q(ref, SIDE + n)
            ref[ROWS:] = jnp.zeros((ROWS, 128), BF)

    own_q[0] = dq[SIDE] * scale
    own_q[1] = dq[0] * scale
    own_k[0] = dk[0] * scale
    own_k[1] = dk[SIDE] * scale
    own_v[0] = dv[0]
    own_v[1] = dv[SIDE]


def queries_kernel(own_q, y1, y2, y3, z1, z2, z3, turned_out, acc):
    z, _, _ = position()

    def lanes(ref):
        return jnp.concatenate([ref[0:HALF].astype(F32), ref[HALF:ROWS].astype(F32)], axis=1)

    acc[...] = own_q[0]
    for n, ref in enumerate((z1, z2, z3)):
        keys = z < jnp.bitwise_xor(z, n + 1)

        @pl.when(jnp.logical_not(keys))
        def _():
            acc[...] += lanes(ref)

    turned_out[0:128] = acc[...].astype(BF)
    turned_out[128:256] = (own_q[1] + lanes(y1) + lanes(y2) + lanes(y3)).astype(BF)


def keys_kernel(
    own_k, own_v, y1, y2, y3, z1, z2, z3, turned_in, q_out, k_out, v_out, acc_k, acc_v
):
    z, _, _ = position()
    acc_k[...] = own_k[1]
    acc_v[...] = own_v[1]
    for n, ref in enumerate((z1, z2, z3)):
        keys = z < jnp.bitwise_xor(z, n + 1)

        @pl.when(keys)
        def _():
            acc_k[...] += ref[0:ROWS].astype(F32)
            acc_v[...] += ref[ROWS:].astype(F32)

    row = iota((ROWS, ROWS), 0)
    col = iota((ROWS, ROWS), 1)
    weave = one_hot(col == row % 2 * HALF + row // 2)
    k0 = own_k[0]
    v0 = own_v[0]
    for ref in (y1, y2, y3):
        k0 += ref[ROWS : 2 * ROWS].astype(F32)
        v0 += ref[2 * ROWS :].astype(F32)
    zero = jnp.concatenate([k0.astype(BF), v0.astype(BF)], axis=1)
    one = jnp.concatenate([acc_k[...].astype(BF), acc_v[...].astype(BF)], axis=1)
    for half in range(2):
        keep = slice(half * HALF, (half + 1) * HALF)
        rows = slice(half * ROWS, (half + 1) * ROWS)
        woven = exact(weave, jnp.concatenate([zero[keep], one[keep]], axis=0)).astype(BF)
        k_out[rows] = woven[:, 0:128]
        v_out[rows] = woven[:, 128:256]
        both = jnp.concatenate([turned_in[0:128, keep], turned_in[128:256, keep]], axis=1)
        q_out[rows] = turned(weave, both).astype(BF)


def project_kernel(
    g0, g1, g2, g3, lat0, n0, n1, m0, m1, f0, f1, e0, e1, own, to1, to2, to3, lat
):
    _, y, core = position()
    lat[0:ROWS] = lat0[...]
    other = side()
    for c in range(2):
        for x in range(2):
            @pl.when(jnp.logical_and(core == c, other == x))
            def _():
                for half in range(2):
                    mine = (n0, n1, f0, f1) if half == c else (m0, m1, e0, e1)
                    block = ROWS * (1 if half == 0 else 3)
                    far = 2 * ROWS + half * HALF
                    for step in range(2):
                        which = step ^ x
                        rows = block + step * HALF
                        lat[rows : rows + HALF] = mine[which][...]
                        rows = far + step * DH
                        lat[rows : rows + DH] = mine[2 + which][...]

    grads = jnp.concatenate([g0[...], g1[...], g2[...], g3[...]], axis=1)
    for n, ref in ((1, to1), (2, to2), (3, to3), (0, own)):
        columns = pl.ds(pl.multiple_of(jnp.bitwise_xor(y, n) * ROWS, ROWS), ROWS)
        ref[...] = exact(grads, lat[:, columns]).astype(ref.dtype)


def total_kernel(own, t1, t2, t3, out):
    whole = own[...] + t1[...].astype(F32) + t2[...].astype(F32) + t3[...].astype(F32)
    out[...] = whole.T


def traded(x, axis, n):
    step = n * (SIDE if axis == "z" else 1)
    return lax.ppermute(x, "sp", [(s, s ^ step) for s in range(SIDE * SIDE)])


def traded_apart(x):
    heads = lax.axis_size("tp")
    pairs = []
    for s in range(SIDE * SIDE):
        for t in range(heads):
            there = s ^ (SIDE * (1 if t % 2 == 0 else 3))
            pairs.append((s * heads + t, there * heads + t))
    return lax.ppermute(x, ("sp", "tp"), pairs)


def across(x):
    return lax.ppermute(x, "tp", [(t, t ^ 2) for t in range(lax.axis_size("tp"))])


def partner(x):
    return lax.ppermute(x, "tp", [(t, t ^ 1) for t in range(lax.axis_size("tp"))])


def shape(*dims, dtype=BF):
    return jax.ShapeDtypeStruct(dims, dtype)


def call(kernel, outs, scalars, hbm, vmem, scratch, flops, mib=16, aliases=None):
    calling = pl.pallas_call(
        kernel,
        out_shape=outs,
        in_specs=[pl.BlockSpec(memory_space=pltpu.SMEM)] * scalars
        + [pl.BlockSpec(memory_space=pltpu.HBM)] * hbm
        + [pl.BlockSpec(memory_space=pltpu.VMEM)] * vmem,
        out_specs=jax.tree.map(lambda _: pl.BlockSpec(memory_space=pltpu.VMEM), outs),
        scratch_shapes=scratch,
        input_output_aliases=aliases or {},
        compiler_params=pltpu.CompilerParams(vmem_limit_bytes=mib * 2**20),
        cost_estimate=pl.CostEstimate(flops=flops, bytes_accessed=10**6, transcendentals=0),
    )

    def run(*arrays):
        held = [
            pltpu.with_memory_space_constraint(x, pltpu.HBM)
            for x in arrays[scalars : scalars + hbm]
        ]
        rest = arrays[scalars + hbm :]
        if aliases:
            rest = [pltpu.with_memory_space_constraint(x, pltpu.VMEM) for x in rest]
        return calling(*arrays[:scalars], *held, *rest)

    return run


def body(
    latents,
    query_heads,
    key_heads,
    value_heads,
    map_outputs,
    log_sums,
    out_grad,
    mix_lambda,
    norm_gain,
):
    yown, zown, *sends, lat_near, lat_far = call(
        prepare_kernel,
        (shape(SLOT, 128),) * 2
        + (shape(QG, 128),) * 3
        + (shape(HALF, WIDE), shape(DH, WIDE)),
        0,
        9,
        0,
        [pltpu.VMEM((2 * ROWS, 128), BF)] * 3
        + [
            pltpu.VMEM((4 * ROWS, 128), BF),
            pltpu.VMEM((2, 2, ROWS), F32),
            pltpu.VMEM((2 * ROWS, 128), BF),
            pltpu.VMEM((1, 128), F32),
            pltpu.SMEM((2,), F32),
            pltpu.SemaphoreType.DMA((10,)),
        ],
        10**8,
    )(
        query_heads.reshape(2 * ROWS, 128),
        key_heads.reshape(2 * ROWS, 128),
        value_heads.reshape(2 * ROWS, 128),
        map_outputs.reshape(4 * ROWS, 128),
        jnp.transpose(log_sums, (1, 2, 0)),
        out_grad.reshape(2 * ROWS, 128),
        norm_gain.reshape(1, 128),
        mix_lambda,
        latents,
    )
    ys = [traded(yown, "y", n) for n in range(1, SIDE)]
    zs = [traded(x, "z", n) for n, x in enumerate(sends, 1)]
    near = traded_apart(lat_near)
    apart = traded(lat_far, "z", 2)
    near_side = across(near)
    apart_side = across(apart)
    lats = (
        near,
        near_side,
        partner(near),
        partner(near_side),
        apart,
        apart_side,
        partner(apart),
        partner(apart_side),
    )

    slots = 2 * SIDE
    state_shapes = (
        shape(slots, SLOT, 128),
        shape(slots, 8, ROWS, dtype=F32),
        shape(slots, 2 * ROWS, 128),
        shape(slots, 128, 2 * ROWS),
        shape(slots, 2 * ROWS, 128),
        shape(slots, 128, ROWS, dtype=F32),
        shape(slots, ROWS, 128, dtype=F32),
        shape(slots, ROWS, 128, dtype=F32),
    )
    holds = [pltpu.VMEM((2, ROWS, ROWS), BF), pltpu.VMEM((2, 2 * ROWS, ROWS), BF)]
    pair_flops = 10 * ROWS * ROWS * 128
    *state, lat_own = call(
        attend_near_kernel,
        state_shapes + (shape(ROWS, WIDE),),
        1,
        1,
        6,
        holds + [pltpu.SemaphoreType.DMA],
        10 * pair_flops,
    )(mix_lambda, latents, yown, ys[0], ys[2], zown, zs[0], zs[2])
    result_shapes = (
        (shape(3 * ROWS, 128),) * 3
        + (shape(2 * ROWS, 128),) * 3
        + (shape(2, 128, ROWS, dtype=F32),)
        + (shape(2, ROWS, 128, dtype=F32),) * 2
    )
    results = call(
        attend_far_kernel,
        result_shapes + state_shapes,
        1,
        0,
        10,
        holds,
        7 * pair_flops,
        aliases={3 + n: len(result_shapes) + n for n in range(len(state_shapes))},
    )(mix_lambda, ys[1], zs[1], *state)
    own_q, own_k, own_v = results[6:9]
    y_back = [traded(x, "y", n) for n, x in enumerate(results[0:3], 1)]
    z_back = [traded(x, "z", n) for n, x in enumerate(results[3:6], 1)]
    turned_grad = call(
        queries_kernel,
        shape(ROWS, ROWS),
        0,
        0,
        7,
        [pltpu.VMEM((128, ROWS), F32)],
        10**7,
    )(own_q, *y_back, *z_back)
    grads = [traded(turned_grad, "z", n) for n in range(1, SIDE)]
    square = shape(ROWS, ROWS)
    own, *parts = call(
        project_kernel,
        (shape(ROWS, ROWS, dtype=F32), square, square, square),
        0,
        0,
        13,
        [pltpu.VMEM((WIDE, WIDE), BF)],
        2 * WIDE * WIDE * ROWS,
    )(turned_grad, *grads, lat_own, *lats)
    query_rows, key_rows, value_rows = call(
        keys_kernel,
        (shape(2 * ROWS, 128),) * 3,
        0,
        0,
        9,
        [pltpu.VMEM((ROWS, 128), F32)] * 2,
        10**7,
    )(own_k, own_v, *y_back, *z_back, turned_grad)
    weight_grad = call(
        total_kernel, shape(ROWS, ROWS, dtype=F32), 0, 0, 4, [], 10**6
    )(own, *[traded(x, "y", n) for n, x in enumerate(parts, 1)])
    whole = (ROWS, 2, 128)
    return (
        query_rows.reshape(whole),
        key_rows.reshape(whole),
        value_rows.reshape(whole),
        weight_grad,
    )


def solution(mesh):
    placed = (
        P("sp", None),
        P("sp", "tp", None),
        P("sp", "tp", None),
        P("sp", "tp", None),
        P("sp", None, "tp", None),
        P("sp", "tp", None),
        P("sp", "tp", None),
        P("tp"),
        P(),
    )
    return jax.shard_map(
        body,
        mesh=mesh,
        in_specs=placed,
        out_specs=(P("sp", "tp", None), P("sp", "tp", None), P("sp", "tp", None), P("sp", "tp")),
        check_vma=False,
    )
```

```python
import jax
import jax.numpy as jnp
from jax import lax
from jax.experimental import pallas as pl
from jax.experimental.pallas import tpu as pltpu
from jax.sharding import PartitionSpec as P


DH = 64
EPSILON = 1e-05
SIDE = 4
ROWS = 256
HALF = ROWS // 2
WIDE = 1024
STAT_ROWS = 32
QG = 2 * ROWS + STAT_ROWS
SLOT = QG + 2 * ROWS
LOG2E = 1.4426950408889634
NT = (((1,), (1,)), ((), ()))
BF = jnp.bfloat16
F32 = jnp.float32


def iota(shape, dim):
    return lax.broadcasted_iota(jnp.int32, shape, dim)


def one_hot(hit):
    return jnp.where(hit, 1.0, 0.0).astype(BF)


def exact(a, b):
    return jnp.dot(a, b, preferred_element_type=F32)


def turned(eye, x):
    return lax.dot_general(eye, x, NT, preferred_element_type=F32)


def two_heads(spread, first, second):
    parts = []
    for half in range(2):
        rows = pl.ds(half * ROWS, ROWS)
        parts.append(exact(spread, jnp.concatenate([first[rows], second[rows]], axis=1)))
    found = []
    for lanes in (slice(0, 128), slice(128, 256)):
        for head in range(2):
            keep = slice(head * HALF, (head + 1) * HALF)
            found.append(jnp.concatenate([part[keep, lanes] for part in parts], axis=0))
    return found


def position():
    index = lax.axis_index("sp")
    return index // SIDE, lax.rem(index, SIDE), lax.rem(lax.axis_index("tp"), 2)


def side():
    return lax.rem(lax.axis_index("tp") // 2, 2)


def prepare_kernel(
    q_hbm, k_hbm, v_hbm, maps_hbm, lse_hbm, out_hbm, gain_hbm, lam_hbm, lat_hbm,
    yown, zown, send1, send2, send3,
    q_in, k_in, v_in, maps_in, lse_in, out_in, gain_in, lam, sems,
):
    z, _, core = position()
    pairs = [
        (maps_hbm, maps_in), (out_hbm, out_in), (gain_hbm, gain_in), (lse_hbm, lse_in),
        (lam_hbm, lam), (q_hbm, q_in), (k_hbm, k_in), (v_hbm, v_in),
    ]
    tokens = pl.ds(pl.multiple_of(core * HALF + side() * DH, DH), DH)
    for n, ref in enumerate((send1, send2, send3), 1):
        for tile in range(WIDE // 128):
            first = jnp.bitwise_xor(z, n) * WIDE + tile * 128
            columns = pl.ds(pl.multiple_of(first, 128), 128)
            rows = pl.ds(QG + tile * DH, DH)
            pairs.append((lat_hbm.at[tokens, columns], ref.at[rows]))
    copies = [pltpu.make_async_copy(a, b, sems.at[n]) for n, (a, b) in enumerate(pairs)]
    for copy in copies:
        copy.start()
    row = iota((ROWS, ROWS), 0)
    col = iota((ROWS, ROWS), 1)
    spread = one_hot(col == 2 * (row % HALF) + row // HALF)
    deal = one_hot(col == 4 * (row % DH) + row // DH)
    for copy in copies[:5]:
        copy.wait()
    left = exact(deal, jnp.concatenate([maps_in[0:256], maps_in[256:512]], axis=1))
    right = exact(deal, jnp.concatenate([maps_in[512:768], maps_in[768:1024]], axis=1))

    def map_rows(which, head):
        rows = slice((which * 2 + head) * DH, (which * 2 + head + 1) * DH)
        return jnp.concatenate(
            [left[rows, 0:128], left[rows, 128:], right[rows, 0:128], right[rows, 128:]], axis=0
        )

    outs = []
    for half in range(2):
        outs.append(exact(spread, out_in[half * ROWS : (half + 1) * ROWS]))
    gain = gain_in[...]
    for head, ref in ((1, yown), (0, zown)):
        first = map_rows(0, head)
        second = map_rows(1, head)
        rows = slice(head * HALF, (head + 1) * HALF)
        cotangent = jnp.concatenate([outs[0][rows], outs[1][rows]], axis=0)
        combined = first - lam[head] * second
        inverse = lax.rsqrt(jnp.mean(combined * combined, axis=-1, keepdims=True) + EPSILON)
        weighted = gain * cotangent
        dot = jnp.mean(combined * weighted, axis=-1, keepdims=True)
        grad = (inverse * weighted - inverse * inverse * inverse * combined * dot).astype(BF)
        wide = grad.astype(F32)
        term1 = jnp.sum((wide * first).T, axis=0, keepdims=True)
        term2 = jnp.sum((wide * second).T, axis=0, keepdims=True)
        lse = lse_in[head]
        table = jnp.concatenate([lse[0:1], lse[1:2], term1, term2], axis=0)
        high = table.astype(BF).astype(F32)
        middle = (table - high).astype(BF).astype(F32)
        low = table - high - middle
        packed = jnp.concatenate([high, middle, low, jnp.zeros_like(table)], axis=0).astype(BF)
        ref[ROWS : 2 * ROWS] = grad
        ref[2 * ROWS : 2 * ROWS + 16] = packed[:, 0:128]
        ref[2 * ROWS + 16 : QG] = packed[:, 128:256]
    for copy in copies[5:8]:
        copy.wait()
    q0, q1, k0, k1 = two_heads(spread, q_in, k_in)
    v0, v1, _, _ = two_heads(spread, v_in, v_in)
    yown[0:ROWS] = q1.astype(BF)
    yown[QG : QG + ROWS] = k0.astype(BF)
    yown[QG + ROWS : SLOT] = v0.astype(BF)
    zown[0:ROWS] = q0.astype(BF)
    zown[QG : QG + ROWS] = k1.astype(BF)
    zown[QG + ROWS : SLOT] = v1.astype(BF)

    def send(ref, keys):
        @pl.when(keys)
        def _():
            ref[0 : 2 * ROWS] = zown[QG:SLOT]
            ref[2 * ROWS : QG] = jnp.zeros((STAT_ROWS, 128), BF)

        @pl.when(jnp.logical_not(keys))
        def _():
            ref[0:QG] = zown[0:QG]

    for n, ref in enumerate((send1, send2, send3)):
        send(ref, z < jnp.bitwise_xor(z, n + 1))
    for copy in copies[8:]:
        copy.wait()


def ready(slot, buf, stat, kpad, kturn, qpad, dq, dk, dv):
    row = iota((128, 128), 0)
    col = iota((128, 128), 1)
    lane = iota((ROWS, 128), 1)
    q = buf[slot, 0:ROWS]
    k = buf[slot, QG : QG + ROWS]
    zero = jnp.zeros_like(q)
    qpad[slot, 0:ROWS] = jnp.where(lane < DH, q, zero)
    qpad[slot, ROWS:] = jnp.where(lane < DH, zero, q)
    kpad[slot, 0:ROWS] = jnp.where(lane < DH, k, zero)
    kpad[slot, ROWS:] = jnp.where(lane < DH, zero, k)
    eye_first = one_hot(jnp.logical_and(row == col, row < DH))
    eye_second = one_hot(jnp.logical_and(row == col, row >= DH))
    kturn[slot, :, 0:ROWS] = turned(eye_first, k).astype(BF)
    kturn[slot, :, ROWS:] = turned(eye_second, k).astype(BF)
    left = buf[slot, 2 * ROWS : 2 * ROWS + 16].astype(F32)
    right = buf[slot, 2 * ROWS + 16 : QG].astype(F32)
    pieces = jnp.concatenate([left, right], axis=1)
    rows = pieces[0:4] + pieces[4:8] + pieces[8:12]
    stat[slot, 0:2] = rows[0:2] * LOG2E
    stat[slot, 2:4] = rows[2:4]
    dq[slot] = jnp.zeros((128, ROWS), F32)
    dk[slot] = jnp.zeros((ROWS, 128), F32)
    dv[slot] = jnp.zeros((ROWS, 128), F32)


def take(z, n, ref, buf):
    keys = jnp.bitwise_xor(z, n) < z

    @pl.when(keys)
    def _():
        buf[SIDE + n, QG:SLOT] = ref[0 : 2 * ROWS]

    @pl.when(jnp.logical_not(keys))
    def _():
        buf[SIDE + n, 0:QG] = ref[0:QG]


def run_pairs(items, z, y, lam, state, wide_w, tall_s):
    buf, stat, kpad, kturn, qpad, dq, dk, dv = state

    def slots_of(item):
        zslot, yslot, kind = item
        if kind is None:
            if zslot == SIDE:
                kind = 1 - (jnp.bitwise_xor(y, yslot) < y).astype(jnp.int32)
            else:
                kind = (jnp.bitwise_xor(z, zslot - SIDE) < z).astype(jnp.int32)
            qs = jnp.where(kind == 0, zslot, yslot)
            return qs, zslot + yslot - qs, kind
        return (zslot, yslot, kind) if kind == 0 else (yslot, zslot, kind)

    slots = [slots_of(item) for item in items]

    def dots(n):
        qs, ks, _ = slots[n]
        q = buf[qs, 0:ROWS]
        g = buf[qs, ROWS : 2 * ROWS]
        v = buf[ks, QG + ROWS : SLOT]
        scores = lax.dot_general(kpad[ks], q, NT, preferred_element_type=F32)
        mixed = lax.dot_general(v, g, NT, preferred_element_type=F32)
        return scores, mixed

    def front(n, started):
        scores, mixed = started
        qs, _, kind = slots[n]
        factor = lam[kind]
        rows = stat[qs]
        scale = DH ** (-0.5) * LOG2E
        power1 = scores[0:ROWS] * scale - rows[0:1]
        power2 = scores[ROWS:] * scale - rows[1:2]
        if items[n][2] is not None:
            seen = iota((ROWS, ROWS), 0) <= iota((ROWS, ROWS), 1)
            gone = jnp.full((ROWS, ROWS), -1e30, F32)
            power1 = jnp.where(seen, power1, gone)
            power2 = jnp.where(seen, power2, gone)
        prob1 = jnp.exp2(power1)
        prob2 = factor * jnp.exp2(power2)
        hold = n % 2
        wide_w[hold] = (prob1 - prob2).astype(BF)
        tall_s[hold, 0:ROWS] = (prob1 * (mixed - rows[2:3])).astype(BF)
        tall_s[hold, ROWS:] = (prob2 * (rows[3:4] - mixed)).astype(BF)

    def back(n):
        qs, ks, _ = slots[n]
        hold = n % 2
        weights = wide_w[hold]
        score1 = tall_s[hold, 0:ROWS]
        score2 = tall_s[hold, ROWS:]
        g = buf[qs, ROWS : 2 * ROWS]
        add_v = exact(weights, g)
        add_k = exact(jnp.concatenate([score1, score2], axis=1), qpad[qs])
        add_q = exact(kturn[ks], tall_s[hold])
        return add_q, add_k, add_v

    front(0, dots(0))
    for n in range(len(items)):
        more = n + 1 < len(items)
        if more:
            started = dots(n + 1)
        add_q, add_k, add_v = back(n)
        if more:
            front(n + 1, started)
        qs, ks, _ = slots[n]
        dv[ks] += add_v
        dk[ks] += add_k
        dq[qs] += add_q


def attend_near_kernel(
    lam, lat_hbm, yown, y1, y3, zown, z1, z3,
    buf, stat, kpad, kturn, qpad, dq, dk, dv, lat_own, wide_w, tall_s, sem,
):
    z, y, _ = position()
    columns = pl.ds(pl.multiple_of(z * WIDE, WIDE), WIDE)
    fetch = pltpu.make_async_copy(lat_hbm.at[:, columns], lat_own, sem)
    fetch.start()
    state = (buf, stat, kpad, kturn, qpad, dq, dk, dv)
    for slot, ref in ((0, yown), (1, y1), (3, y3), (SIDE, zown)):
        buf[slot] = ref[...]
    take(z, 1, z1, buf)
    take(z, 3, z3, buf)
    for slot in (0, 1, 3, 4, 5, 7):
        ready(slot, *state)
    items = [(4, 0, 0), (4, 0, 1)]
    items += [(4, 1, None), (4, 3, None)]
    items += [(zslot, yslot, None) for zslot in (5, 7) for yslot in (0, 1, 3)]
    run_pairs(items, z, y, lam, state, wide_w, tall_s)
    fetch.wait()


def attend_far_kernel(
    lam, y2, z2, z1, z3, buf_in, stat_in, kpad_in, kturn_in, qpad_in, dq_in, dk_in, dv_in,
    g1, g2, g3, r1, r2, r3, own_q, own_k, own_v, lat_mine,
    buf, stat, kpad, kturn, qpad, dq, dk, dv, wide_w, tall_s,
):
    z, y, _ = position()
    state = (buf, stat, kpad, kturn, qpad, dq, dk, dv)
    for n, ref in enumerate((z1, z2, z3)):
        lat_mine[n * 2 * ROWS : (n + 1) * 2 * ROWS] = ref[QG:SLOT]
    buf[2] = y2[...]
    take(z, 2, z2, buf)
    for slot in (2, 6):
        ready(slot, *state)
    items = [(zslot, 2, None) for zslot in (4, 5, 7)]
    items += [(6, yslot, None) for yslot in range(SIDE)]
    run_pairs(items, z, y, lam, state, wide_w, tall_s)
    scale = DH ** (-0.5)

    def put_q(ref, slot):
        value = (dq[slot] * scale).astype(BF)
        ref[0:HALF] = value[:, 0:128]
        ref[HALF:ROWS] = value[:, 128:]

    for slot, ref in enumerate((g1, g2, g3), 1):
        put_q(ref, slot)
        ref[ROWS : 2 * ROWS] = (dk[slot] * scale).astype(BF)
        ref[2 * ROWS :] = dv[slot].astype(BF)
    for n, ref in enumerate((r1, r2, r3), 1):
        keys = jnp.bitwise_xor(z, n) < z

        @pl.when(keys)
        def _():
            ref[0:ROWS] = (dk[SIDE + n] * scale).astype(BF)
            ref[ROWS:] = dv[SIDE + n].astype(BF)

        @pl.when(jnp.logical_not(keys))
        def _():
            put_q(ref, SIDE + n)
            ref[ROWS:] = jnp.zeros((ROWS, 128), BF)

    own_q[0] = dq[SIDE] * scale
    own_q[1] = dq[0] * scale
    own_k[0] = dk[0] * scale
    own_k[1] = dk[SIDE] * scale
    own_v[0] = dv[0]
    own_v[1] = dv[SIDE]


def queries_kernel(own_q, y1, y2, y3, z1, z2, z3, turned_out, acc):
    z, _, _ = position()

    def lanes(ref):
        return jnp.concatenate([ref[0:HALF].astype(F32), ref[HALF:ROWS].astype(F32)], axis=1)

    acc[...] = own_q[0]
    for n, ref in enumerate((z1, z2, z3)):
        keys = z < jnp.bitwise_xor(z, n + 1)

        @pl.when(jnp.logical_not(keys))
        def _():
            acc[...] += lanes(ref)

    turned_out[0:128] = acc[...].astype(BF)
    turned_out[128:256] = (own_q[1] + lanes(y1) + lanes(y2) + lanes(y3)).astype(BF)


def keys_kernel(
    own_k, own_v, y1, y2, y3, z1, z2, z3, turned_in, q_out, k_out, v_out, acc_k, acc_v
):
    z, _, _ = position()
    acc_k[...] = own_k[1]
    acc_v[...] = own_v[1]
    for n, ref in enumerate((z1, z2, z3)):
        keys = z < jnp.bitwise_xor(z, n + 1)

        @pl.when(keys)
        def _():
            acc_k[...] += ref[0:ROWS].astype(F32)
            acc_v[...] += ref[ROWS:].astype(F32)

    row = iota((ROWS, ROWS), 0)
    col = iota((ROWS, ROWS), 1)
    weave = one_hot(col == row % 2 * HALF + row // 2)
    k0 = own_k[0]
    v0 = own_v[0]
    for ref in (y1, y2, y3):
        k0 += ref[ROWS : 2 * ROWS].astype(F32)
        v0 += ref[2 * ROWS :].astype(F32)
    zero = jnp.concatenate([k0.astype(BF), v0.astype(BF)], axis=1)
    one = jnp.concatenate([acc_k[...].astype(BF), acc_v[...].astype(BF)], axis=1)
    for half in range(2):
        keep = slice(half * HALF, (half + 1) * HALF)
        rows = slice(half * ROWS, (half + 1) * ROWS)
        woven = exact(weave, jnp.concatenate([zero[keep], one[keep]], axis=0)).astype(BF)
        k_out[rows] = woven[:, 0:128]
        v_out[rows] = woven[:, 128:256]
        both = jnp.concatenate([turned_in[0:128, keep], turned_in[128:256, keep]], axis=1)
        q_out[rows] = turned(weave, both).astype(BF)


def project_kernel(g0, g1, g2, g3, lat0, a0, a1, b0, b1, own, to1, to2, to3, lat):
    _, y, core = position()
    lat[0:ROWS] = lat0[...]
    other = side()
    for c in range(2):
        for x in range(2):
            @pl.when(jnp.logical_and(core == c, other == x))
            def _():
                for half in range(2):
                    for part in range(2):
                        ref = ((a0, a1) if half == c else (b0, b1))[part ^ x]
                        for n in range(SIDE - 1):
                            first = (n + 1) * ROWS + half * HALF + part * DH
                            for tile in range(WIDE // 128):
                                rows = n * 2 * ROWS + tile * DH
                                lat[first : first + DH, tile * 128 : (tile + 1) * 128] = ref[
                                    rows : rows + DH
                                ]

    grads = jnp.concatenate([g0[...], g1[...], g2[...], g3[...]], axis=1)
    for n, ref in ((1, to1), (2, to2), (3, to3), (0, own)):
        columns = pl.ds(pl.multiple_of(jnp.bitwise_xor(y, n) * ROWS, ROWS), ROWS)
        ref[...] = exact(grads, lat[:, columns]).astype(ref.dtype)


def total_kernel(own, t1, t2, t3, out):
    whole = own[...] + t1[...].astype(F32) + t2[...].astype(F32) + t3[...].astype(F32)
    out[...] = whole.T


def traded(x, axis, n):
    step = n * (SIDE if axis == "z" else 1)
    return lax.ppermute(x, "sp", [(s, s ^ step) for s in range(SIDE * SIDE)])


def across(x):
    return lax.ppermute(x, "tp", [(t, t ^ 2) for t in range(lax.axis_size("tp"))])


def partner(x):
    return lax.ppermute(x, "tp", [(t, t ^ 1) for t in range(lax.axis_size("tp"))])


def shape(*dims, dtype=BF):
    return jax.ShapeDtypeStruct(dims, dtype)


def call(kernel, outs, scalars, hbm, vmem, scratch, flops, mib=16, aliases=None):
    calling = pl.pallas_call(
        kernel,
        out_shape=outs,
        in_specs=[pl.BlockSpec(memory_space=pltpu.SMEM)] * scalars
        + [pl.BlockSpec(memory_space=pltpu.HBM)] * hbm
        + [pl.BlockSpec(memory_space=pltpu.VMEM)] * vmem,
        out_specs=jax.tree.map(lambda _: pl.BlockSpec(memory_space=pltpu.VMEM), outs),
        scratch_shapes=scratch,
        input_output_aliases=aliases or {},
        compiler_params=pltpu.CompilerParams(vmem_limit_bytes=mib * 2**20),
        cost_estimate=pl.CostEstimate(flops=flops, bytes_accessed=10**6, transcendentals=0),
    )

    def run(*arrays):
        held = [
            pltpu.with_memory_space_constraint(x, pltpu.HBM)
            for x in arrays[scalars : scalars + hbm]
        ]
        rest = arrays[scalars + hbm :]
        if aliases:
            rest = [pltpu.with_memory_space_constraint(x, pltpu.VMEM) for x in rest]
        return calling(*arrays[:scalars], *held, *rest)

    return run


def body(
    latents,
    query_heads,
    key_heads,
    value_heads,
    map_outputs,
    log_sums,
    out_grad,
    mix_lambda,
    norm_gain,
):
    yown, zown, *sends = call(
        prepare_kernel,
        (shape(SLOT, 128),) * 5,
        0,
        9,
        0,
        [pltpu.VMEM((2 * ROWS, 128), BF)] * 3
        + [
            pltpu.VMEM((4 * ROWS, 128), BF),
            pltpu.VMEM((2, 2, ROWS), F32),
            pltpu.VMEM((2 * ROWS, 128), BF),
            pltpu.VMEM((1, 128), F32),
            pltpu.SMEM((2,), F32),
            pltpu.SemaphoreType.DMA((32,)),
        ],
        10**8,
    )(
        query_heads.reshape(2 * ROWS, 128),
        key_heads.reshape(2 * ROWS, 128),
        value_heads.reshape(2 * ROWS, 128),
        map_outputs.reshape(4 * ROWS, 128),
        jnp.transpose(log_sums, (1, 2, 0)),
        out_grad.reshape(2 * ROWS, 128),
        norm_gain.reshape(1, 128),
        mix_lambda,
        latents,
    )
    ys = [traded(yown, "y", n) for n in range(1, SIDE)]
    zs = [traded(x, "z", n) for n, x in enumerate(sends, 1)]
    slots = 2 * SIDE
    state_shapes = (
        shape(slots, SLOT, 128),
        shape(slots, 8, ROWS, dtype=F32),
        shape(slots, 2 * ROWS, 128),
        shape(slots, 128, 2 * ROWS),
        shape(slots, 2 * ROWS, 128),
        shape(slots, 128, ROWS, dtype=F32),
        shape(slots, ROWS, 128, dtype=F32),
        shape(slots, ROWS, 128, dtype=F32),
    )
    holds = [pltpu.VMEM((2, ROWS, ROWS), BF), pltpu.VMEM((2, 2 * ROWS, ROWS), BF)]
    pair_flops = 10 * ROWS * ROWS * 128
    *state, lat_own = call(
        attend_near_kernel,
        state_shapes + (shape(ROWS, WIDE),),
        1,
        1,
        6,
        holds + [pltpu.SemaphoreType.DMA],
        10 * pair_flops,
    )(mix_lambda, latents, yown, ys[0], ys[2], zown, zs[0], zs[2])
    result_shapes = (
        (shape(3 * ROWS, 128),) * 3
        + (shape(2 * ROWS, 128),) * 3
        + (shape(2, 128, ROWS, dtype=F32),)
        + (shape(2, ROWS, 128, dtype=F32),) * 2
        + (shape(6 * ROWS, 128),)
    )
    results = call(
        attend_far_kernel,
        result_shapes + state_shapes,
        1,
        0,
        12,
        holds,
        7 * pair_flops,
        aliases={5 + n: len(result_shapes) + n for n in range(len(state_shapes))},
    )(mix_lambda, ys[1], zs[1], zs[0], zs[2], *state)
    own_q, own_k, own_v, lat_mine = results[6:10]
    lat_side = across(lat_mine)
    lats = (lat_mine, lat_side, partner(lat_mine), partner(lat_side))
    y_back = [traded(x, "y", n) for n, x in enumerate(results[0:3], 1)]
    z_back = [traded(x, "z", n) for n, x in enumerate(results[3:6], 1)]
    turned_grad = call(
        queries_kernel, shape(ROWS, ROWS), 0, 0, 7, [pltpu.VMEM((128, ROWS), F32)], 10**7
    )(own_q, *y_back, *z_back)
    grads = [traded(turned_grad, "z", n) for n in range(1, SIDE)]
    square = shape(ROWS, ROWS)
    own, *parts = call(
        project_kernel,
        (shape(ROWS, ROWS, dtype=F32), square, square, square),
        0,
        0,
        9,
        [pltpu.VMEM((WIDE, WIDE), BF)],
        2 * WIDE * WIDE * ROWS,
    )(turned_grad, *grads, lat_own, *lats)
    query_rows, key_rows, value_rows = call(
        keys_kernel, (shape(2 * ROWS, 128),) * 3, 0, 0, 9, [pltpu.VMEM((ROWS, 128), F32)] * 2, 10**7
    )(own_k, own_v, *y_back, *z_back, turned_grad)
    weight_grad = call(
        total_kernel, shape(ROWS, ROWS, dtype=F32), 0, 0, 4, [], 10**6
    )(own, *[traded(x, "y", n) for n, x in enumerate(parts, 1)])
    whole = (ROWS, 2, 128)
    return (
        query_rows.reshape(whole),
        key_rows.reshape(whole),
        value_rows.reshape(whole),
        weight_grad,
    )


def solution(mesh):
    placed = (
        P("sp", None),
        P("sp", "tp", None),
        P("sp", "tp", None),
        P("sp", "tp", None),
        P("sp", None, "tp", None),
        P("sp", "tp", None),
        P("sp", "tp", None),
        P("tp"),
        P(),
    )
    return jax.shard_map(
        body,
        mesh=mesh,
        in_specs=placed,
        out_specs=(P("sp", "tp", None), P("sp", "tp", None), P("sp", "tp", None), P("sp", "tp")),
        check_vma=False,
    )
```

```python
import jax
import jax.numpy as jnp
from jax import lax
from jax.experimental import pallas as pl
from jax.experimental.pallas import tpu as pltpu
from jax.sharding import PartitionSpec as P


DH = 64
EPSILON = 1e-05
SIDE = 4
ROWS = 256
HALF = ROWS // 2
WIDE = 1024
STAT_ROWS = 32
QG = 2 * ROWS + STAT_ROWS
SLOT = QG + 2 * ROWS
LOG2E = 1.4426950408889634
NT = (((1,), (1,)), ((), ()))
BF = jnp.bfloat16
F32 = jnp.float32


def iota(shape, dim):
    return lax.broadcasted_iota(jnp.int32, shape, dim)


def one_hot(hit):
    return jnp.where(hit, 1.0, 0.0).astype(BF)


def exact(a, b):
    return jnp.dot(a, b, preferred_element_type=F32)


def turned(eye, x):
    return lax.dot_general(eye, x, NT, preferred_element_type=F32)


def two_heads(spread, first, second):
    parts = []
    for half in range(2):
        rows = pl.ds(half * ROWS, ROWS)
        parts.append(exact(spread, jnp.concatenate([first[rows], second[rows]], axis=1)))
    found = []
    for lanes in (slice(0, 128), slice(128, 256)):
        for head in range(2):
            keep = slice(head * HALF, (head + 1) * HALF)
            found.append(jnp.concatenate([part[keep, lanes] for part in parts], axis=0))
    return found


def position():
    index = lax.axis_index("sp")
    return index // SIDE, lax.rem(index, SIDE), lax.rem(lax.axis_index("tp"), 2)


def prepare_kernel(
    q_hbm, k_hbm, v_hbm, maps_hbm, lse_hbm, out_hbm, gain_hbm, lam_hbm, lat_hbm,
    yown, zown, send1, send2, send3, lat_near, lat_far,
    q_in, k_in, v_in, maps_in, lse_in, out_in, gain_in, lam, sems,
):
    z, _, core = position()
    pairs = [
        (maps_hbm, maps_in), (out_hbm, out_in), (gain_hbm, gain_in), (lse_hbm, lse_in),
        (lam_hbm, lam), (q_hbm, q_in), (k_hbm, k_in), (v_hbm, v_in),
    ]
    near = jnp.bitwise_xor(z, jnp.where(core == 0, 1, 3))
    columns = pl.ds(pl.multiple_of(near * WIDE, WIDE), WIDE)
    pairs.append((lat_hbm.at[:, columns], lat_near))
    tokens = pl.ds(pl.multiple_of(core * HALF, HALF), HALF)
    columns = pl.ds(pl.multiple_of(jnp.bitwise_xor(z, 2) * WIDE, WIDE), WIDE)
    pairs.append((lat_hbm.at[tokens, columns], lat_far))
    copies = [pltpu.make_async_copy(a, b, sems.at[n]) for n, (a, b) in enumerate(pairs)]
    for copy in copies:
        copy.start()
    row = iota((ROWS, ROWS), 0)
    col = iota((ROWS, ROWS), 1)
    spread = one_hot(col == 2 * (row % HALF) + row // HALF)
    deal = one_hot(col == 4 * (row % DH) + row // DH)
    for copy in copies[:5]:
        copy.wait()
    left = exact(deal, jnp.concatenate([maps_in[0:256], maps_in[256:512]], axis=1))
    right = exact(deal, jnp.concatenate([maps_in[512:768], maps_in[768:1024]], axis=1))

    def map_rows(which, head):
        rows = slice((which * 2 + head) * DH, (which * 2 + head + 1) * DH)
        return jnp.concatenate(
            [left[rows, 0:128], left[rows, 128:], right[rows, 0:128], right[rows, 128:]], axis=0
        )

    outs = []
    for half in range(2):
        outs.append(exact(spread, out_in[half * ROWS : (half + 1) * ROWS]))
    gain = gain_in[...]
    for head, ref in ((1, yown), (0, zown)):
        first = map_rows(0, head)
        second = map_rows(1, head)
        rows = slice(head * HALF, (head + 1) * HALF)
        cotangent = jnp.concatenate([outs[0][rows], outs[1][rows]], axis=0)
        combined = first - lam[head] * second
        inverse = lax.rsqrt(jnp.mean(combined * combined, axis=-1, keepdims=True) + EPSILON)
        weighted = gain * cotangent
        dot = jnp.mean(combined * weighted, axis=-1, keepdims=True)
        grad = (inverse * weighted - inverse * inverse * inverse * combined * dot).astype(BF)
        wide = grad.astype(F32)
        term1 = jnp.sum((wide * first).T, axis=0, keepdims=True)
        term2 = jnp.sum((wide * second).T, axis=0, keepdims=True)
        lse = lse_in[head]
        table = jnp.concatenate([lse[0:1], lse[1:2], term1, term2], axis=0)
        high = table.astype(BF).astype(F32)
        middle = (table - high).astype(BF).astype(F32)
        low = table - high - middle
        packed = jnp.concatenate([high, middle, low, jnp.zeros_like(table)], axis=0).astype(BF)
        ref[ROWS : 2 * ROWS] = grad
        ref[2 * ROWS : 2 * ROWS + 16] = packed[:, 0:128]
        ref[2 * ROWS + 16 : QG] = packed[:, 128:256]
    for copy in copies[5:8]:
        copy.wait()
    q0, q1, k0, k1 = two_heads(spread, q_in, k_in)
    v0, v1, _, _ = two_heads(spread, v_in, v_in)
    yown[0:ROWS] = q1.astype(BF)
    yown[QG : QG + ROWS] = k0.astype(BF)
    yown[QG + ROWS : SLOT] = v0.astype(BF)
    zown[0:ROWS] = q0.astype(BF)
    zown[QG : QG + ROWS] = k1.astype(BF)
    zown[QG + ROWS : SLOT] = v1.astype(BF)

    def send(ref, keys):
        @pl.when(keys)
        def _():
            ref[0 : 2 * ROWS] = zown[QG:SLOT]
            ref[2 * ROWS : QG] = jnp.zeros((STAT_ROWS, 128), BF)

        @pl.when(jnp.logical_not(keys))
        def _():
            ref[...] = zown[0:QG]

    for n, ref in enumerate((send1, send2, send3)):
        send(ref, z < jnp.bitwise_xor(z, n + 1))
    for copy in copies[8:]:
        copy.wait()


def ready(slot, buf, stat, kpad, kturn, qpad, dq, dk, dv):
    row = iota((128, 128), 0)
    col = iota((128, 128), 1)
    lane = iota((ROWS, 128), 1)
    q = buf[slot, 0:ROWS]
    k = buf[slot, QG : QG + ROWS]
    zero = jnp.zeros_like(q)
    qpad[slot, 0:ROWS] = jnp.where(lane < DH, q, zero)
    qpad[slot, ROWS:] = jnp.where(lane < DH, zero, q)
    kpad[slot, 0:ROWS] = jnp.where(lane < DH, k, zero)
    kpad[slot, ROWS:] = jnp.where(lane < DH, zero, k)
    eye_first = one_hot(jnp.logical_and(row == col, row < DH))
    eye_second = one_hot(jnp.logical_and(row == col, row >= DH))
    kturn[slot, :, 0:ROWS] = turned(eye_first, k).astype(BF)
    kturn[slot, :, ROWS:] = turned(eye_second, k).astype(BF)
    left = buf[slot, 2 * ROWS : 2 * ROWS + 16].astype(F32)
    right = buf[slot, 2 * ROWS + 16 : QG].astype(F32)
    pieces = jnp.concatenate([left, right], axis=1)
    rows = pieces[0:4] + pieces[4:8] + pieces[8:12]
    stat[slot, 0:2] = rows[0:2] * LOG2E
    stat[slot, 2:4] = rows[2:4]
    dq[slot] = jnp.zeros((128, ROWS), F32)
    dk[slot] = jnp.zeros((ROWS, 128), F32)
    dv[slot] = jnp.zeros((ROWS, 128), F32)


def take(z, n, ref, buf):
    keys = jnp.bitwise_xor(z, n) < z

    @pl.when(keys)
    def _():
        buf[SIDE + n, QG:SLOT] = ref[0 : 2 * ROWS]

    @pl.when(jnp.logical_not(keys))
    def _():
        buf[SIDE + n, 0:QG] = ref[...]


def run_pairs(items, z, y, lam, state, wide_w, tall_s):
    buf, stat, kpad, kturn, qpad, dq, dk, dv = state

    def slots_of(item):
        zslot, yslot, kind = item
        if kind is None:
            if zslot == SIDE:
                kind = 1 - (jnp.bitwise_xor(y, yslot) < y).astype(jnp.int32)
            else:
                kind = (jnp.bitwise_xor(z, zslot - SIDE) < z).astype(jnp.int32)
            qs = jnp.where(kind == 0, zslot, yslot)
            return qs, zslot + yslot - qs, kind
        return (zslot, yslot, kind) if kind == 0 else (yslot, zslot, kind)

    slots = [slots_of(item) for item in items]

    def dots(n):
        qs, ks, _ = slots[n]
        q = buf[qs, 0:ROWS]
        g = buf[qs, ROWS : 2 * ROWS]
        v = buf[ks, QG + ROWS : SLOT]
        scores = lax.dot_general(kpad[ks], q, NT, preferred_element_type=F32)
        mixed = lax.dot_general(v, g, NT, preferred_element_type=F32)
        return scores, mixed

    def front(n, started):
        scores, mixed = started
        qs, _, kind = slots[n]
        factor = lam[kind]
        rows = stat[qs]
        scale = DH ** (-0.5) * LOG2E
        power1 = scores[0:ROWS] * scale - rows[0:1]
        power2 = scores[ROWS:] * scale - rows[1:2]
        if items[n][2] is not None:
            seen = iota((ROWS, ROWS), 0) <= iota((ROWS, ROWS), 1)
            gone = jnp.full((ROWS, ROWS), -1e30, F32)
            power1 = jnp.where(seen, power1, gone)
            power2 = jnp.where(seen, power2, gone)
        prob1 = jnp.exp2(power1)
        prob2 = factor * jnp.exp2(power2)
        hold = n % 2
        wide_w[hold] = (prob1 - prob2).astype(BF)
        tall_s[hold, 0:ROWS] = (prob1 * (mixed - rows[2:3])).astype(BF)
        tall_s[hold, ROWS:] = (prob2 * (rows[3:4] - mixed)).astype(BF)

    def back(n):
        qs, ks, _ = slots[n]
        hold = n % 2
        weights = wide_w[hold]
        score1 = tall_s[hold, 0:ROWS]
        score2 = tall_s[hold, ROWS:]
        g = buf[qs, ROWS : 2 * ROWS]
        add_v = exact(weights, g)
        add_k = exact(jnp.concatenate([score1, score2], axis=1), qpad[qs])
        add_q = exact(kturn[ks], tall_s[hold])
        return add_q, add_k, add_v

    front(0, dots(0))
    for n in range(len(items)):
        more = n + 1 < len(items)
        if more:
            started = dots(n + 1)
        add_q, add_k, add_v = back(n)
        if more:
            front(n + 1, started)
        qs, ks, _ = slots[n]
        dv[ks] += add_v
        dk[ks] += add_k
        dq[qs] += add_q


def attend_near_kernel(
    lam, lat_hbm, yown, y1, y3, zown, z1, z3,
    buf, stat, kpad, kturn, qpad, dq, dk, dv, lat_own, wide_w, tall_s, sem,
):
    z, y, _ = position()
    columns = pl.ds(pl.multiple_of(z * WIDE, WIDE), WIDE)
    fetch = pltpu.make_async_copy(lat_hbm.at[:, columns], lat_own, sem)
    fetch.start()
    state = (buf, stat, kpad, kturn, qpad, dq, dk, dv)
    for slot, ref in ((0, yown), (1, y1), (3, y3), (SIDE, zown)):
        buf[slot] = ref[...]
    take(z, 1, z1, buf)
    take(z, 3, z3, buf)
    for slot in (0, 1, 3, 4, 5, 7):
        ready(slot, *state)
    items = [(4, 0, 0), (4, 0, 1)]
    items += [(4, 1, None), (4, 3, None)]
    items += [(zslot, yslot, None) for zslot in (5, 7) for yslot in (0, 1, 3)]
    run_pairs(items, z, y, lam, state, wide_w, tall_s)
    fetch.wait()


def attend_far_kernel(
    lam, y2, z2, buf_in, stat_in, kpad_in, kturn_in, qpad_in, dq_in, dk_in, dv_in,
    g1, g2, g3, r1, r2, r3, v1, v2, v3, own_q, own_k, own_v,
    buf, stat, kpad, kturn, qpad, dq, dk, dv, wide_w, tall_s,
):
    z, y, _ = position()
    state = (buf, stat, kpad, kturn, qpad, dq, dk, dv)
    buf[2] = y2[...]
    take(z, 2, z2, buf)
    for slot in (2, 6):
        ready(slot, *state)
    items = [(zslot, 2, None) for zslot in (4, 5, 7)]
    items += [(6, yslot, None) for yslot in range(SIDE)]
    run_pairs(items, z, y, lam, state, wide_w, tall_s)
    scale = DH ** (-0.5)

    def put_q(ref, slot):
        value = (dq[slot] * scale).astype(BF)
        ref[0:HALF] = value[:, 0:128]
        ref[HALF:ROWS] = value[:, 128:]

    for slot, ref in enumerate((g1, g2, g3), 1):
        put_q(ref, slot)
        ref[ROWS : 2 * ROWS] = (dk[slot] * scale).astype(BF)
        ref[2 * ROWS :] = dv[slot].astype(BF)
    for n, (ref, ref_v) in enumerate(((r1, v1), (r2, v2), (r3, v3)), 1):
        keys = jnp.bitwise_xor(z, n) < z
        ref_v[...] = dv[SIDE + n].astype(BF)

        @pl.when(keys)
        def _():
            ref[...] = (dk[SIDE + n] * scale).astype(BF)

        @pl.when(jnp.logical_not(keys))
        def _():
            put_q(ref, SIDE + n)

    own_q[0] = dq[SIDE] * scale
    own_q[1] = dq[0] * scale
    own_k[0] = dk[0] * scale
    own_k[1] = dk[SIDE] * scale
    own_v[0] = dv[0]
    own_v[1] = dv[SIDE]


def queries_kernel(own_q, y1, y2, y3, z1, z2, z3, turned_out, acc):
    z, _, _ = position()

    def lanes(ref):
        return jnp.concatenate([ref[0:HALF].astype(F32), ref[HALF:ROWS].astype(F32)], axis=1)

    acc[...] = own_q[0]
    for n, ref in enumerate((z1, z2, z3)):
        keys = z < jnp.bitwise_xor(z, n + 1)

        @pl.when(jnp.logical_not(keys))
        def _():
            acc[...] += lanes(ref)

    turned_out[0:128] = acc[...].astype(BF)
    turned_out[128:256] = (own_q[1] + lanes(y1) + lanes(y2) + lanes(y3)).astype(BF)


def keys_kernel(
    own_k, own_v, y1, y2, y3, z1, z2, z3, v1, v2, v3, turned_in,
    q_out, k_out, v_out, acc_k, acc_v,
):
    z, _, _ = position()
    acc_k[...] = own_k[1]
    acc_v[...] = own_v[1]
    for n, (ref, ref_v) in enumerate(((z1, v1), (z2, v2), (z3, v3)), 1):
        keys = z < jnp.bitwise_xor(z, n)

        @pl.when(keys)
        def _():
            acc_k[...] += ref[...].astype(F32)
            acc_v[...] += ref_v[...].astype(F32)

    row = iota((ROWS, ROWS), 0)
    col = iota((ROWS, ROWS), 1)
    weave = one_hot(col == row % 2 * HALF + row // 2)
    k0 = own_k[0]
    v0 = own_v[0]
    for ref in (y1, y2, y3):
        k0 += ref[ROWS : 2 * ROWS].astype(F32)
        v0 += ref[2 * ROWS :].astype(F32)
    zero = jnp.concatenate([k0.astype(BF), v0.astype(BF)], axis=1)
    one = jnp.concatenate([acc_k[...].astype(BF), acc_v[...].astype(BF)], axis=1)
    for half in range(2):
        keep = slice(half * HALF, (half + 1) * HALF)
        rows = slice(half * ROWS, (half + 1) * ROWS)
        woven = exact(weave, jnp.concatenate([zero[keep], one[keep]], axis=0)).astype(BF)
        k_out[rows] = woven[:, 0:128]
        v_out[rows] = woven[:, 128:256]
        both = jnp.concatenate([turned_in[0:128, keep], turned_in[128:256, keep]], axis=1)
        q_out[rows] = turned(weave, both).astype(BF)


def project_kernel(
    g0, g1, g2, g3, lat0, near, near_swap, far, far_swap, own, to1, to2, to3, lat
):
    _, y, core = position()
    lat[0:ROWS] = lat0[...]
    first = slice(ROWS, 2 * ROWS)
    second = slice(2 * ROWS, 2 * ROWS + HALF)
    third = slice(2 * ROWS + HALF, 3 * ROWS)
    fourth = slice(3 * ROWS, 4 * ROWS)

    @pl.when(core == 0)
    def _():
        lat[first] = near[...]
        lat[second] = far[...]
        lat[third] = far_swap[...]
        lat[fourth] = near_swap[...]

    @pl.when(core == 1)
    def _():
        lat[first] = near_swap[...]
        lat[second] = far_swap[...]
        lat[third] = far[...]
        lat[fourth] = near[...]

    grads = jnp.concatenate([g0[...], g1[...], g2[...], g3[...]], axis=1)
    for n, ref in ((1, to1), (2, to2), (3, to3), (0, own)):
        columns = pl.ds(pl.multiple_of(jnp.bitwise_xor(y, n) * ROWS, ROWS), ROWS)
        ref[...] = exact(grads, lat[:, columns]).astype(ref.dtype)


def total_kernel(own, t1, t2, t3, out):
    whole = own[...] + t1[...].astype(F32) + t2[...].astype(F32) + t3[...].astype(F32)
    out[...] = whole.T


def traded(x, axis, n):
    step = n * (SIDE if axis == "z" else 1)
    return lax.ppermute(x, "sp", [(s, s ^ step) for s in range(SIDE * SIDE)])


def traded_apart(x):
    heads = lax.axis_size("tp")
    pairs = []
    for s in range(SIDE * SIDE):
        for t in range(heads):
            there = s ^ (SIDE * (1 if t % 2 == 0 else 3))
            pairs.append((s * heads + t, there * heads + t))
    return lax.ppermute(x, ("sp", "tp"), pairs)


def partner(x):
    return lax.ppermute(x, "tp", [(t, t ^ 1) for t in range(lax.axis_size("tp"))])


def shape(*dims, dtype=BF):
    return jax.ShapeDtypeStruct(dims, dtype)


def call(kernel, outs, scalars, hbm, vmem, scratch, flops, mib=16, aliases=None):
    calling = pl.pallas_call(
        kernel,
        out_shape=outs,
        in_specs=[pl.BlockSpec(memory_space=pltpu.SMEM)] * scalars
        + [pl.BlockSpec(memory_space=pltpu.HBM)] * hbm
        + [pl.BlockSpec(memory_space=pltpu.VMEM)] * vmem,
        out_specs=jax.tree.map(lambda _: pl.BlockSpec(memory_space=pltpu.VMEM), outs),
        scratch_shapes=scratch,
        input_output_aliases=aliases or {},
        compiler_params=pltpu.CompilerParams(vmem_limit_bytes=mib * 2**20),
        cost_estimate=pl.CostEstimate(flops=flops, bytes_accessed=10**6, transcendentals=0),
    )

    def run(*arrays):
        held = [
            pltpu.with_memory_space_constraint(x, pltpu.HBM)
            for x in arrays[scalars : scalars + hbm]
        ]
        rest = arrays[scalars + hbm :]
        if aliases:
            rest = [pltpu.with_memory_space_constraint(x, pltpu.VMEM) for x in rest]
        return calling(*arrays[:scalars], *held, *rest)

    return run


def body(
    latents,
    query_heads,
    key_heads,
    value_heads,
    map_outputs,
    log_sums,
    out_grad,
    mix_lambda,
    norm_gain,
):
    yown, zown, *sends, lat_near, lat_far = call(
        prepare_kernel,
        (shape(SLOT, 128),) * 2
        + (shape(QG, 128),) * 3
        + (shape(ROWS, WIDE), shape(HALF, WIDE)),
        0,
        9,
        0,
        [pltpu.VMEM((2 * ROWS, 128), BF)] * 3
        + [
            pltpu.VMEM((4 * ROWS, 128), BF),
            pltpu.VMEM((2, 2, ROWS), F32),
            pltpu.VMEM((2 * ROWS, 128), BF),
            pltpu.VMEM((1, 128), F32),
            pltpu.SMEM((2,), F32),
            pltpu.SemaphoreType.DMA((10,)),
        ],
        10**8,
    )(
        query_heads.reshape(2 * ROWS, 128),
        key_heads.reshape(2 * ROWS, 128),
        value_heads.reshape(2 * ROWS, 128),
        map_outputs.reshape(4 * ROWS, 128),
        jnp.transpose(log_sums, (1, 2, 0)),
        out_grad.reshape(2 * ROWS, 128),
        norm_gain.reshape(1, 128),
        mix_lambda,
        latents,
    )
    ys = [traded(yown, "y", n) for n in range(1, SIDE)]
    zs = [traded(x, "z", n) for n, x in enumerate(sends, 1)]
    near = traded_apart(lat_near)
    apart = traded(lat_far, "z", 2)
    near_swap = partner(near)
    apart_swap = partner(apart)

    slots = 2 * SIDE
    state_shapes = (
        shape(slots, SLOT, 128),
        shape(slots, 8, ROWS, dtype=F32),
        shape(slots, 2 * ROWS, 128),
        shape(slots, 128, 2 * ROWS),
        shape(slots, 2 * ROWS, 128),
        shape(slots, 128, ROWS, dtype=F32),
        shape(slots, ROWS, 128, dtype=F32),
        shape(slots, ROWS, 128, dtype=F32),
    )
    holds = [pltpu.VMEM((2, ROWS, ROWS), BF), pltpu.VMEM((2, 2 * ROWS, ROWS), BF)]
    pair_flops = 10 * ROWS * ROWS * 128
    *state, lat_own = call(
        attend_near_kernel,
        state_shapes + (shape(ROWS, WIDE),),
        1,
        1,
        6,
        holds + [pltpu.SemaphoreType.DMA],
        10 * pair_flops,
    )(mix_lambda, latents, yown, ys[0], ys[2], zown, zs[0], zs[2])
    result_shapes = (
        (shape(3 * ROWS, 128),) * 3
        + (shape(ROWS, 128),) * 6
        + (shape(2, 128, ROWS, dtype=F32),)
        + (shape(2, ROWS, 128, dtype=F32),) * 2
    )
    results = call(
        attend_far_kernel,
        result_shapes + state_shapes,
        1,
        0,
        10,
        holds,
        7 * pair_flops,
        aliases={3 + n: len(result_shapes) + n for n in range(len(state_shapes))},
    )(mix_lambda, ys[1], zs[1], *state)
    own_q, own_k, own_v = results[9:12]
    y_back = [traded(x, "y", n) for n, x in enumerate(results[0:3], 1)]
    z_back = [traded(x, "z", n) for n, x in enumerate(results[3:6], 1)]
    v_back = [traded(x, "z", n) for n, x in enumerate(results[6:9], 1)]
    turned_grad = call(
        queries_kernel,
        shape(ROWS, ROWS),
        0,
        0,
        7,
        [pltpu.VMEM((128, ROWS), F32)],
        10**7,
    )(own_q, *y_back, *z_back)
    grads = [traded(turned_grad, "z", n) for n in range(1, SIDE)]
    square = shape(ROWS, ROWS)
    own, *parts = call(
        project_kernel,
        (shape(ROWS, ROWS, dtype=F32), square, square, square),
        0,
        0,
        9,
        [pltpu.VMEM((WIDE, WIDE), BF)],
        2 * WIDE * WIDE * ROWS,
    )(turned_grad, *grads, lat_own, near, near_swap, apart, apart_swap)
    query_rows, key_rows, value_rows = call(
        keys_kernel,
        (shape(2 * ROWS, 128),) * 3,
        0,
        0,
        12,
        [pltpu.VMEM((ROWS, 128), F32)] * 2,
        10**7,
    )(own_k, own_v, *y_back, *z_back, *v_back, turned_grad)
    weight_grad = call(
        total_kernel, shape(ROWS, ROWS, dtype=F32), 0, 0, 4, [], 10**6
    )(own, *[traded(x, "y", n) for n, x in enumerate(parts, 1)])
    whole = (ROWS, 2, 128)
    return (
        query_rows.reshape(whole),
        key_rows.reshape(whole),
        value_rows.reshape(whole),
        weight_grad,
    )


def solution(mesh):
    placed = (
        P("sp", None),
        P("sp", "tp", None),
        P("sp", "tp", None),
        P("sp", "tp", None),
        P("sp", None, "tp", None),
        P("sp", "tp", None),
        P("sp", "tp", None),
        P("tp"),
        P(),
    )
    return jax.shard_map(
        body,
        mesh=mesh,
        in_specs=placed,
        out_specs=(P("sp", "tp", None), P("sp", "tp", None), P("sp", "tp", None), P("sp", "tp")),
        check_vma=False,
    )
```

```python
import jax
import jax.numpy as jnp
from jax import lax
from jax.experimental import pallas as pl
from jax.experimental.pallas import tpu as pltpu
from jax.sharding import PartitionSpec as P


DH = 64
EPSILON = 1e-05
SIDE = 4
ROWS = 256
HALF = ROWS // 2
WIDE = 1024
STAT_ROWS = 32
QG = 2 * ROWS + STAT_ROWS
SLOT = QG + 2 * ROWS
LOG2E = 1.4426950408889634
NT = (((1,), (1,)), ((), ()))
BF = jnp.bfloat16
F32 = jnp.float32


def iota(shape, dim):
    return lax.broadcasted_iota(jnp.int32, shape, dim)


def one_hot(hit):
    return jnp.where(hit, 1.0, 0.0).astype(BF)


def exact(a, b):
    return jnp.dot(a, b, preferred_element_type=F32)


def turned(eye, x):
    return lax.dot_general(eye, x, NT, preferred_element_type=F32)


def two_heads(spread, first, second):
    parts = []
    for half in range(2):
        rows = pl.ds(half * ROWS, ROWS)
        parts.append(exact(spread, jnp.concatenate([first[rows], second[rows]], axis=1)))
    found = []
    for lanes in (slice(0, 128), slice(128, 256)):
        for head in range(2):
            keep = slice(head * HALF, (head + 1) * HALF)
            found.append(jnp.concatenate([part[keep, lanes] for part in parts], axis=0))
    return found


def position():
    index = lax.axis_index("sp")
    return index // SIDE, lax.rem(index, SIDE), lax.rem(lax.axis_index("tp"), 2)


def side():
    return lax.rem(lax.axis_index("tp") // 2, 2)


def prepare_kernel(
    q_hbm, k_hbm, v_hbm, maps_hbm, lse_hbm, out_hbm, gain_hbm, lam_hbm, lat_hbm,
    yown, zown, send1, send2, send3, lat_near, lat_far,
    q_in, k_in, v_in, maps_in, lse_in, out_in, gain_in, lam, sems,
):
    z, _, core = position()
    pairs = [
        (maps_hbm, maps_in), (out_hbm, out_in), (gain_hbm, gain_in), (lse_hbm, lse_in),
        (lam_hbm, lam), (q_hbm, q_in), (k_hbm, k_in), (v_hbm, v_in),
    ]
    near = jnp.bitwise_xor(z, jnp.where(core == 0, 1, 3))
    columns = pl.ds(pl.multiple_of(near * WIDE, WIDE), WIDE)
    tokens = pl.ds(pl.multiple_of(side() * HALF, HALF), HALF)
    pairs.append((lat_hbm.at[tokens, columns], lat_near))
    columns = pl.ds(pl.multiple_of(jnp.bitwise_xor(z, 2) * WIDE, WIDE), WIDE)
    tokens = pl.ds(pl.multiple_of(core * HALF + side() * DH, DH), DH)
    pairs.append((lat_hbm.at[tokens, columns], lat_far))
    copies = [pltpu.make_async_copy(a, b, sems.at[n]) for n, (a, b) in enumerate(pairs)]
    for copy in copies:
        copy.start()
    row = iota((ROWS, ROWS), 0)
    col = iota((ROWS, ROWS), 1)
    spread = one_hot(col == 2 * (row % HALF) + row // HALF)
    deal = one_hot(col == 4 * (row % DH) + row // DH)
    for copy in copies[:5]:
        copy.wait()
    left = exact(deal, jnp.concatenate([maps_in[0:256], maps_in[256:512]], axis=1))
    right = exact(deal, jnp.concatenate([maps_in[512:768], maps_in[768:1024]], axis=1))

    def map_rows(which, head):
        rows = slice((which * 2 + head) * DH, (which * 2 + head + 1) * DH)
        return jnp.concatenate(
            [left[rows, 0:128], left[rows, 128:], right[rows, 0:128], right[rows, 128:]], axis=0
        )

    outs = []
    for half in range(2):
        outs.append(exact(spread, out_in[half * ROWS : (half + 1) * ROWS]))
    gain = gain_in[...]
    for head, ref in ((1, yown), (0, zown)):
        first = map_rows(0, head)
        second = map_rows(1, head)
        rows = slice(head * HALF, (head + 1) * HALF)
        cotangent = jnp.concatenate([outs[0][rows], outs[1][rows]], axis=0)
        combined = first - lam[head] * second
        inverse = lax.rsqrt(jnp.mean(combined * combined, axis=-1, keepdims=True) + EPSILON)
        weighted = gain * cotangent
        dot = jnp.mean(combined * weighted, axis=-1, keepdims=True)
        grad = (inverse * weighted - inverse * inverse * inverse * combined * dot).astype(BF)
        wide = grad.astype(F32)
        term1 = jnp.sum((wide * first).T, axis=0, keepdims=True)
        term2 = jnp.sum((wide * second).T, axis=0, keepdims=True)
        lse = lse_in[head]
        table = jnp.concatenate([lse[0:1], lse[1:2], term1, term2], axis=0)
        high = table.astype(BF).astype(F32)
        middle = (table - high).astype(BF).astype(F32)
        low = table - high - middle
        packed = jnp.concatenate([high, middle, low, jnp.zeros_like(table)], axis=0).astype(BF)
        ref[ROWS : 2 * ROWS] = grad
        ref[2 * ROWS : 2 * ROWS + 16] = packed[:, 0:128]
        ref[2 * ROWS + 16 : QG] = packed[:, 128:256]
    for copy in copies[5:8]:
        copy.wait()
    q0, q1, k0, k1 = two_heads(spread, q_in, k_in)
    v0, v1, _, _ = two_heads(spread, v_in, v_in)
    yown[0:ROWS] = q1.astype(BF)
    yown[QG : QG + ROWS] = k0.astype(BF)
    yown[QG + ROWS : SLOT] = v0.astype(BF)
    zown[0:ROWS] = q0.astype(BF)
    zown[QG : QG + ROWS] = k1.astype(BF)
    zown[QG + ROWS : SLOT] = v1.astype(BF)

    def send(ref, keys):
        @pl.when(keys)
        def _():
            ref[0 : 2 * ROWS] = zown[QG:SLOT]
            ref[2 * ROWS : QG] = jnp.zeros((STAT_ROWS, 128), BF)

        @pl.when(jnp.logical_not(keys))
        def _():
            ref[...] = zown[0:QG]

    for n, ref in enumerate((send1, send2, send3)):
        send(ref, z < jnp.bitwise_xor(z, n + 1))
    for copy in copies[8:]:
        copy.wait()


def ready(slot, buf, stat, kpad, kturn, qpad, dq, dk, dv):
    row = iota((128, 128), 0)
    col = iota((128, 128), 1)
    lane = iota((ROWS, 128), 1)
    q = buf[slot, 0:ROWS]
    k = buf[slot, QG : QG + ROWS]
    zero = jnp.zeros_like(q)
    qpad[slot, 0:ROWS] = jnp.where(lane < DH, q, zero)
    qpad[slot, ROWS:] = jnp.where(lane < DH, zero, q)
    kpad[slot, 0:ROWS] = jnp.where(lane < DH, k, zero)
    kpad[slot, ROWS:] = jnp.where(lane < DH, zero, k)
    eye_first = one_hot(jnp.logical_and(row == col, row < DH))
    eye_second = one_hot(jnp.logical_and(row == col, row >= DH))
    kturn[slot, :, 0:ROWS] = turned(eye_first, k).astype(BF)
    kturn[slot, :, ROWS:] = turned(eye_second, k).astype(BF)
    left = buf[slot, 2 * ROWS : 2 * ROWS + 16].astype(F32)
    right = buf[slot, 2 * ROWS + 16 : QG].astype(F32)
    pieces = jnp.concatenate([left, right], axis=1)
    rows = pieces[0:4] + pieces[4:8] + pieces[8:12]
    stat[slot, 0:2] = rows[0:2] * LOG2E
    stat[slot, 2:4] = rows[2:4]
    dq[slot] = jnp.zeros((128, ROWS), F32)
    dk[slot] = jnp.zeros((ROWS, 128), F32)
    dv[slot] = jnp.zeros((ROWS, 128), F32)


def take(z, n, ref, buf):
    keys = jnp.bitwise_xor(z, n) < z

    @pl.when(keys)
    def _():
        buf[SIDE + n, QG:SLOT] = ref[0 : 2 * ROWS]

    @pl.when(jnp.logical_not(keys))
    def _():
        buf[SIDE + n, 0:QG] = ref[...]


def run_pairs(items, z, y, lam, state, wide_w, tall_s):
    buf, stat, kpad, kturn, qpad, dq, dk, dv = state

    def slots_of(item):
        zslot, yslot, kind = item
        if kind is None:
            if zslot == SIDE:
                kind = 1 - (jnp.bitwise_xor(y, yslot) < y).astype(jnp.int32)
            else:
                kind = (jnp.bitwise_xor(z, zslot - SIDE) < z).astype(jnp.int32)
            qs = jnp.where(kind == 0, zslot, yslot)
            return qs, zslot + yslot - qs, kind
        return (zslot, yslot, kind) if kind == 0 else (yslot, zslot, kind)

    slots = [slots_of(item) for item in items]

    def dots(n):
        qs, ks, _ = slots[n]
        q = buf[qs, 0:ROWS]
        g = buf[qs, ROWS : 2 * ROWS]
        v = buf[ks, QG + ROWS : SLOT]
        scores = lax.dot_general(kpad[ks], q, NT, preferred_element_type=F32)
        mixed = lax.dot_general(v, g, NT, preferred_element_type=F32)
        return scores, mixed

    def front(n, started):
        scores, mixed = started
        qs, _, kind = slots[n]
        factor = lam[kind]
        rows = stat[qs]
        scale = DH ** (-0.5) * LOG2E
        power1 = scores[0:ROWS] * scale - rows[0:1]
        power2 = scores[ROWS:] * scale - rows[1:2]
        if items[n][2] is not None:
            seen = iota((ROWS, ROWS), 0) <= iota((ROWS, ROWS), 1)
            gone = jnp.full((ROWS, ROWS), -1e30, F32)
            power1 = jnp.where(seen, power1, gone)
            power2 = jnp.where(seen, power2, gone)
        prob1 = jnp.exp2(power1)
        prob2 = factor * jnp.exp2(power2)
        hold = n % 2
        wide_w[hold] = (prob1 - prob2).astype(BF)
        tall_s[hold, 0:ROWS] = (prob1 * (mixed - rows[2:3])).astype(BF)
        tall_s[hold, ROWS:] = (prob2 * (rows[3:4] - mixed)).astype(BF)

    def back(n):
        qs, ks, _ = slots[n]
        hold = n % 2
        weights = wide_w[hold]
        score1 = tall_s[hold, 0:ROWS]
        score2 = tall_s[hold, ROWS:]
        g = buf[qs, ROWS : 2 * ROWS]
        add_v = exact(weights, g)
        add_k = exact(jnp.concatenate([score1, score2], axis=1), qpad[qs])
        add_q = exact(kturn[ks], tall_s[hold])
        return add_q, add_k, add_v

    front(0, dots(0))
    for n in range(len(items)):
        more = n + 1 < len(items)
        if more:
            started = dots(n + 1)
        add_q, add_k, add_v = back(n)
        if more:
            front(n + 1, started)
        qs, ks, _ = slots[n]
        dv[ks] += add_v
        dk[ks] += add_k
        dq[qs] += add_q


def attend_near_kernel(
    lam, lat_hbm, yown, y1, y3, zown, z1, z3,
    buf, stat, kpad, kturn, qpad, dq, dk, dv, lat_own, wide_w, tall_s, sem,
):
    z, y, _ = position()
    columns = pl.ds(pl.multiple_of(z * WIDE, WIDE), WIDE)
    fetch = pltpu.make_async_copy(lat_hbm.at[:, columns], lat_own, sem)
    fetch.start()
    state = (buf, stat, kpad, kturn, qpad, dq, dk, dv)
    for slot, ref in ((0, yown), (1, y1), (3, y3), (SIDE, zown)):
        buf[slot] = ref[...]
    take(z, 1, z1, buf)
    take(z, 3, z3, buf)
    for slot in (0, 1, 3, 4, 5, 7):
        ready(slot, *state)
    items = [(4, 0, 0), (4, 0, 1)]
    items += [(4, 1, None), (4, 3, None)]
    items += [(zslot, yslot, None) for zslot in (5, 7) for yslot in (0, 1, 3)]
    run_pairs(items, z, y, lam, state, wide_w, tall_s)
    fetch.wait()


def attend_far_kernel(
    lam, y2, z2, buf_in, stat_in, kpad_in, kturn_in, qpad_in, dq_in, dk_in, dv_in,
    g1, g2, g3, r1, r2, r3, v1, v2, v3, own_q, own_k, own_v,
    buf, stat, kpad, kturn, qpad, dq, dk, dv, wide_w, tall_s,
):
    z, y, _ = position()
    state = (buf, stat, kpad, kturn, qpad, dq, dk, dv)
    buf[2] = y2[...]
    take(z, 2, z2, buf)
    for slot in (2, 6):
        ready(slot, *state)
    items = [(zslot, 2, None) for zslot in (4, 5, 7)]
    items += [(6, yslot, None) for yslot in range(SIDE)]
    run_pairs(items, z, y, lam, state, wide_w, tall_s)
    scale = DH ** (-0.5)

    def put_q(ref, slot):
        value = (dq[slot] * scale).astype(BF)
        ref[0:HALF] = value[:, 0:128]
        ref[HALF:ROWS] = value[:, 128:]

    for slot, ref in enumerate((g1, g2, g3), 1):
        put_q(ref, slot)
        ref[ROWS : 2 * ROWS] = (dk[slot] * scale).astype(BF)
        ref[2 * ROWS :] = dv[slot].astype(BF)
    for n, (ref, ref_v) in enumerate(((r1, v1), (r2, v2), (r3, v3)), 1):
        keys = jnp.bitwise_xor(z, n) < z
        ref_v[...] = dv[SIDE + n].astype(BF)

        @pl.when(keys)
        def _():
            ref[...] = (dk[SIDE + n] * scale).astype(BF)

        @pl.when(jnp.logical_not(keys))
        def _():
            put_q(ref, SIDE + n)

    own_q[0] = dq[SIDE] * scale
    own_q[1] = dq[0] * scale
    own_k[0] = dk[0] * scale
    own_k[1] = dk[SIDE] * scale
    own_v[0] = dv[0]
    own_v[1] = dv[SIDE]


def queries_kernel(own_q, y1, y2, y3, z1, z2, z3, turned_out, acc):
    z, _, _ = position()

    def lanes(ref):
        return jnp.concatenate([ref[0:HALF].astype(F32), ref[HALF:ROWS].astype(F32)], axis=1)

    acc[...] = own_q[0]
    for n, ref in enumerate((z1, z2, z3)):
        keys = z < jnp.bitwise_xor(z, n + 1)

        @pl.when(jnp.logical_not(keys))
        def _():
            acc[...] += lanes(ref)

    turned_out[0:128] = acc[...].astype(BF)
    turned_out[128:256] = (own_q[1] + lanes(y1) + lanes(y2) + lanes(y3)).astype(BF)


def keys_kernel(
    own_k, own_v, y1, y2, y3, z1, z2, z3, v1, v2, v3, turned_in,
    q_out, k_out, v_out, acc_k, acc_v,
):
    z, _, _ = position()
    acc_k[...] = own_k[1]
    acc_v[...] = own_v[1]
    for n, (ref, ref_v) in enumerate(((z1, v1), (z2, v2), (z3, v3)), 1):
        keys = z < jnp.bitwise_xor(z, n)

        @pl.when(keys)
        def _():
            acc_k[...] += ref[...].astype(F32)
            acc_v[...] += ref_v[...].astype(F32)

    row = iota((ROWS, ROWS), 0)
    col = iota((ROWS, ROWS), 1)
    weave = one_hot(col == row % 2 * HALF + row // 2)
    k0 = own_k[0]
    v0 = own_v[0]
    for ref in (y1, y2, y3):
        k0 += ref[ROWS : 2 * ROWS].astype(F32)
        v0 += ref[2 * ROWS :].astype(F32)
    zero = jnp.concatenate([k0.astype(BF), v0.astype(BF)], axis=1)
    one = jnp.concatenate([acc_k[...].astype(BF), acc_v[...].astype(BF)], axis=1)
    for half in range(2):
        keep = slice(half * HALF, (half + 1) * HALF)
        rows = slice(half * ROWS, (half + 1) * ROWS)
        woven = exact(weave, jnp.concatenate([zero[keep], one[keep]], axis=0)).astype(BF)
        k_out[rows] = woven[:, 0:128]
        v_out[rows] = woven[:, 128:256]
        both = jnp.concatenate([turned_in[0:128, keep], turned_in[128:256, keep]], axis=1)
        q_out[rows] = turned(weave, both).astype(BF)


def project_kernel(
    g0, g1, g2, g3, lat0, n0, n1, m0, m1, f0, f1, e0, e1, own, to1, to2, to3, lat
):
    _, y, core = position()
    lat[0:ROWS] = lat0[...]
    other = side()
    for c in range(2):
        for x in range(2):
            @pl.when(jnp.logical_and(core == c, other == x))
            def _():
                for half in range(2):
                    mine = (n0, n1, f0, f1) if half == c else (m0, m1, e0, e1)
                    block = ROWS * (1 if half == 0 else 3)
                    far = 2 * ROWS + half * HALF
                    for step in range(2):
                        which = step ^ x
                        rows = block + step * HALF
                        lat[rows : rows + HALF] = mine[which][...]
                        rows = far + step * DH
                        lat[rows : rows + DH] = mine[2 + which][...]

    grads = jnp.concatenate([g0[...], g1[...], g2[...], g3[...]], axis=1)
    for n, ref in ((1, to1), (2, to2), (3, to3), (0, own)):
        columns = pl.ds(pl.multiple_of(jnp.bitwise_xor(y, n) * ROWS, ROWS), ROWS)
        ref[...] = exact(grads, lat[:, columns]).astype(ref.dtype)


def total_kernel(own, t1, t2, t3, out):
    whole = own[...] + t1[...].astype(F32) + t2[...].astype(F32) + t3[...].astype(F32)
    out[...] = whole.T


def traded(x, axis, n):
    step = n * (SIDE if axis == "z" else 1)
    return lax.ppermute(x, "sp", [(s, s ^ step) for s in range(SIDE * SIDE)])


def traded_apart(x):
    heads = lax.axis_size("tp")
    pairs = []
    for s in range(SIDE * SIDE):
        for t in range(heads):
            there = s ^ (SIDE * (1 if t % 2 == 0 else 3))
            pairs.append((s * heads + t, there * heads + t))
    return lax.ppermute(x, ("sp", "tp"), pairs)


def across(x):
    return lax.ppermute(x, "tp", [(t, t ^ 2) for t in range(lax.axis_size("tp"))])


def partner(x):
    return lax.ppermute(x, "tp", [(t, t ^ 1) for t in range(lax.axis_size("tp"))])


def shape(*dims, dtype=BF):
    return jax.ShapeDtypeStruct(dims, dtype)


def call(kernel, outs, scalars, hbm, vmem, scratch, flops, mib=16, aliases=None):
    calling = pl.pallas_call(
        kernel,
        out_shape=outs,
        in_specs=[pl.BlockSpec(memory_space=pltpu.SMEM)] * scalars
        + [pl.BlockSpec(memory_space=pltpu.HBM)] * hbm
        + [pl.BlockSpec(memory_space=pltpu.VMEM)] * vmem,
        out_specs=jax.tree.map(lambda _: pl.BlockSpec(memory_space=pltpu.VMEM), outs),
        scratch_shapes=scratch,
        input_output_aliases=aliases or {},
        compiler_params=pltpu.CompilerParams(vmem_limit_bytes=mib * 2**20),
        cost_estimate=pl.CostEstimate(flops=flops, bytes_accessed=10**6, transcendentals=0),
    )

    def run(*arrays):
        held = [
            pltpu.with_memory_space_constraint(x, pltpu.HBM)
            for x in arrays[scalars : scalars + hbm]
        ]
        rest = arrays[scalars + hbm :]
        if aliases:
            rest = [pltpu.with_memory_space_constraint(x, pltpu.VMEM) for x in rest]
        return calling(*arrays[:scalars], *held, *rest)

    return run


def body(
    latents,
    query_heads,
    key_heads,
    value_heads,
    map_outputs,
    log_sums,
    out_grad,
    mix_lambda,
    norm_gain,
):
    yown, zown, *sends, lat_near, lat_far = call(
        prepare_kernel,
        (shape(SLOT, 128),) * 2
        + (shape(QG, 128),) * 3
        + (shape(HALF, WIDE), shape(DH, WIDE)),
        0,
        9,
        0,
        [pltpu.VMEM((2 * ROWS, 128), BF)] * 3
        + [
            pltpu.VMEM((4 * ROWS, 128), BF),
            pltpu.VMEM((2, 2, ROWS), F32),
            pltpu.VMEM((2 * ROWS, 128), BF),
            pltpu.VMEM((1, 128), F32),
            pltpu.SMEM((2,), F32),
            pltpu.SemaphoreType.DMA((10,)),
        ],
        10**8,
    )(
        query_heads.reshape(2 * ROWS, 128),
        key_heads.reshape(2 * ROWS, 128),
        value_heads.reshape(2 * ROWS, 128),
        map_outputs.reshape(4 * ROWS, 128),
        jnp.transpose(log_sums, (1, 2, 0)),
        out_grad.reshape(2 * ROWS, 128),
        norm_gain.reshape(1, 128),
        mix_lambda,
        latents,
    )
    ys = [traded(yown, "y", n) for n in range(1, SIDE)]
    zs = [traded(x, "z", n) for n, x in enumerate(sends, 1)]
    near = traded_apart(lat_near)
    apart = traded(lat_far, "z", 2)
    near_side = across(near)
    apart_side = across(apart)
    lats = (
        near,
        near_side,
        partner(near),
        partner(near_side),
        apart,
        apart_side,
        partner(apart),
        partner(apart_side),
    )

    slots = 2 * SIDE
    state_shapes = (
        shape(slots, SLOT, 128),
        shape(slots, 8, ROWS, dtype=F32),
        shape(slots, 2 * ROWS, 128),
        shape(slots, 128, 2 * ROWS),
        shape(slots, 2 * ROWS, 128),
        shape(slots, 128, ROWS, dtype=F32),
        shape(slots, ROWS, 128, dtype=F32),
        shape(slots, ROWS, 128, dtype=F32),
    )
    holds = [pltpu.VMEM((2, ROWS, ROWS), BF), pltpu.VMEM((2, 2 * ROWS, ROWS), BF)]
    pair_flops = 10 * ROWS * ROWS * 128
    *state, lat_own = call(
        attend_near_kernel,
        state_shapes + (shape(ROWS, WIDE),),
        1,
        1,
        6,
        holds + [pltpu.SemaphoreType.DMA],
        10 * pair_flops,
    )(mix_lambda, latents, yown, ys[0], ys[2], zown, zs[0], zs[2])
    result_shapes = (
        (shape(3 * ROWS, 128),) * 3
        + (shape(ROWS, 128),) * 6
        + (shape(2, 128, ROWS, dtype=F32),)
        + (shape(2, ROWS, 128, dtype=F32),) * 2
    )
    results = call(
        attend_far_kernel,
        result_shapes + state_shapes,
        1,
        0,
        10,
        holds,
        7 * pair_flops,
        aliases={3 + n: len(result_shapes) + n for n in range(len(state_shapes))},
    )(mix_lambda, ys[1], zs[1], *state)
    own_q, own_k, own_v = results[9:12]
    y_back = [traded(x, "y", n) for n, x in enumerate(results[0:3], 1)]
    z_back = [traded(x, "z", n) for n, x in enumerate(results[3:6], 1)]
    v_back = [traded(x, "z", n) for n, x in enumerate(results[6:9], 1)]
    turned_grad = call(
        queries_kernel,
        shape(ROWS, ROWS),
        0,
        0,
        7,
        [pltpu.VMEM((128, ROWS), F32)],
        10**7,
    )(own_q, *y_back, *z_back)
    grads = [traded(turned_grad, "z", n) for n in range(1, SIDE)]
    square = shape(ROWS, ROWS)
    own, *parts = call(
        project_kernel,
        (shape(ROWS, ROWS, dtype=F32), square, square, square),
        0,
        0,
        13,
        [pltpu.VMEM((WIDE, WIDE), BF)],
        2 * WIDE * WIDE * ROWS,
    )(turned_grad, *grads, lat_own, *lats)
    query_rows, key_rows, value_rows = call(
        keys_kernel,
        (shape(2 * ROWS, 128),) * 3,
        0,
        0,
        12,
        [pltpu.VMEM((ROWS, 128), F32)] * 2,
        10**7,
    )(own_k, own_v, *y_back, *z_back, *v_back, turned_grad)
    weight_grad = call(
        total_kernel, shape(ROWS, ROWS, dtype=F32), 0, 0, 4, [], 10**6
    )(own, *[traded(x, "y", n) for n, x in enumerate(parts, 1)])
    whole = (ROWS, 2, 128)
    return (
        query_rows.reshape(whole),
        key_rows.reshape(whole),
        value_rows.reshape(whole),
        weight_grad,
    )


def solution(mesh):
    placed = (
        P("sp", None),
        P("sp", "tp", None),
        P("sp", "tp", None),
        P("sp", "tp", None),
        P("sp", None, "tp", None),
        P("sp", "tp", None),
        P("sp", "tp", None),
        P("tp"),
        P(),
    )
    return jax.shard_map(
        body,
        mesh=mesh,
        in_specs=placed,
        out_specs=(P("sp", "tp", None), P("sp", "tp", None), P("sp", "tp", None), P("sp", "tp")),
        check_vma=False,
    )
```
